32 devices in a mesh: ep: 8 (over z, y), tp: 4 (over x, core).
Axes of the slice: x: 2, y: 2, z: 4, core: 2. Of those that a mesh axis runs over, the one named last changes fastest.
Arguments:
- queries: bfloat16 [16384, 1024], P('ep', 'tp'), may hold values from -6 to 6
- keys_values: bfloat16 [16384, 512], P('ep', 'tp'), may hold values from -6 to 6
- sink_logits: float32 [16], replicated, may hold values from 4 to 8
- out_weight: bfloat16 [1024, 2048], replicated, may hold values from -4 to 4
- expert_tokens: bfloat16 [8192, 2048], P(('ep', 'tp')), may hold values from -6 to 6
- norm_gain: float32 [2048], replicated, may hold values from 0.1 to 1.9
- routes: int32 [8192, 2], P(('ep', 'tp')), may hold values from 0 to 7, all different within a row; in each aligned block of 256 rows (0 to 255, 256 to 511, ...) at most 96 rows name the same one
- route_weights: float32 [8192, 2], P(('ep', 'tp')), may hold values from 0.1 to 1
- gate_weight: bfloat16 [8, 2048, 1024], P('ep', None, 'tp'), may hold values from -0.125 to 0.125
- up_weight: bfloat16 [8, 2048, 1024], P('ep', None, 'tp'), may hold values from -0.125 to 0.125
- down_weight: bfloat16 [8, 1024, 2048], P('ep', 'tp'), may hold values from -0.1875 to 0.1875
Outputs:
- mixer_out: bfloat16 [16384, 2048], P(('ep', 'tp'))
- expert_out: bfloat16 [8192, 2048], P(('ep', 'tp'))
The draws below stay inside these ranges and needn't reach their ends.
Inputs may be any that keep to these rules, and one draw needn't show every extreme that they name: `routes`: each row names 2 different experts. In each aligned block of 256 rows, no expert is named by more than 96 rows, and in some block an expert is named by exactly 96 rows.
All inputs are finite; a program needn't handle non-finite values.
Results may differ from the reference program's by a relative error of at most 0.012.
Values may be sent and summed in bfloat16 or wider, within the bound.
A program may use at most 128 MiB of HBM per device.

```python
import math
import jax
import jax.numpy as jnp
import numpy as np
from jax import lax

D = 2048
HEADS = 16
KV_HEADS = 4
GROUP = 4
HEAD_DIM = 64
WINDOW = 128
FE = 1024
TOPK = 2
MOE_ROWS = 256
SEQ = 16384
MOE_TOKENS = 8192
EXPERTS = 8
CAP = 96
N_TP = 4


def draw_queries(key, part):
    noise_key = jax.random.fold_in(key, 11)
    return jax.random.truncated_normal(noise_key, -6.0, 6.0, (SEQ, HEADS * HEAD_DIM)).astype(jnp.bfloat16)


def draw_keys_values(key, part):
    noise_key = jax.random.fold_in(key, 17)
    return jax.random.truncated_normal(noise_key, -6.0, 6.0, (SEQ, KV_HEADS * 2 * HEAD_DIM)).astype(jnp.bfloat16)


def block_scale(key, shape, split, least, high):
    level = 1.0
    for axis_at, shards_of in split:
        draws = jax.random.uniform(jax.random.fold_in(jax.random.fold_in(key, 6), axis_at), (shards_of,), jnp.float32, least / len(split), high / len(split))
        level = level * jnp.repeat(jnp.exp(draws), shape[axis_at] // shards_of).reshape((-1,) + (1,) * (len(shape) - 1 - axis_at))
    return level


def routed_block(own_key, own, number, rows, number_of, top, most, lean):
    order = jax.random.permutation(own_key, number_of)
    crowded, usual = portions_of(number_of, rows * top, most, lean, True), portions_of(number_of, rows * top, most, lean, False)
    places = jnp.arange(number_of)

    def named(lengths, rotation):
        used = int((lengths > 0).sum())
        fixed = max(1, used // 4)
        moved = fixed + (places - fixed + rotation * (used - fixed)) % max(1, number_of - fixed)
        return jnp.zeros((number_of,), jnp.int32).at[order[jnp.where(places < fixed, places, moved)]].set(jnp.asarray(lengths, jnp.int32))

    lengths = jnp.where(number % 4 == 0, named(crowded, number // 4), named(usual, number - number // 4 - 1))
    mixed = jax.random.permutation(jax.random.fold_in(own, 3), number_of)
    giver, taker = mixed[0:number_of // 2 * 2:2], mixed[1:number_of // 2 * 2:2]
    margin = jnp.minimum(lengths[giver] - 1, most - lengths[taker]) // 2
    margin = jnp.where((giver == order[0]) | (taker == order[0]) | (lengths[taker] == 0), 0, jnp.maximum(margin, 0))
    moved = jax.random.randint(jax.random.fold_in(own, 4), (number_of // 2,), 0, 1 << 20) % (margin + 1)
    lengths = lengths.at[giver].add(-moved).at[taker].add(moved)
    items = jnp.searchsorted(jnp.cumsum(lengths), jnp.arange(rows * top), side="right").astype(jnp.int32)
    table = items.reshape(top, rows).T
    table = table[jax.random.permutation(jax.random.fold_in(own, 1), rows)]
    rotation = jax.random.randint(jax.random.fold_in(own, 2), (rows, 1), 0, top)
    return jnp.take_along_axis(table, (jnp.arange(top)[None, :] + rotation) % top, axis=1)


def portions_of(number_of, total, most, skew, full):
    portions = [(1 << 20) // math.isqrt(grade ** skew) + 1 for grade in range(1, number_of + 1)]
    largest = most if full else min(most, max(-(-total // number_of), total * portions[0] // sum(portions)))
    least = 1 if total - largest >= number_of - 1 else 0
    counts, surplus = [largest] + [least] * (number_of - 1), total - largest - least * (number_of - 1)
    while surplus > 0:
        candidates = [i for i in range(1, number_of) if counts[i] < largest] or [i for i in range(1, number_of) if counts[i] < most]
        whole, left = sum([portions[i] for i in candidates]), surplus
        for i in candidates:
            addition = min(most - counts[i], max(1, left * portions[i] // whole), surplus)
            counts[i] = counts[i] + addition
            surplus = surplus - addition
    return np.array(counts)


def normal_values(rng, dims, width, limit, cuts=(), kind=jnp.bfloat16):
    result = width * jax.random.normal(rng, dims, jnp.float32)
    if cuts:
        result = result * block_scale(rng, dims, cuts, -0.22, 0.18)
    return jnp.clip(result, -limit, limit).astype(kind)


def setup_inputs(seed: int = 0) -> dict:
    keys = jax.random.split(jax.random.key(seed), 12)
    queries = draw_queries(jax.random.fold_in(keys[11], 71), 0)
    keys_values = draw_keys_values(jax.random.fold_in(keys[11], 71), 0)
    sink_logits = jnp.clip(jax.random.uniform(keys[2], (HEADS,), jnp.float32, 4.0, 8.0), 4.0, 8.0)
    out_weight = normal_values(keys[3], (HEADS * HEAD_DIM, D), 0.8, 4.0)
    expert_tokens = normal_values(keys[4], (MOE_TOKENS, D), 1.0, 6.0, ((0, 32),))
    norm_gain = jnp.clip(1.0 + 0.18 * jax.random.normal(keys[5], (D,), jnp.float32), 0.1, 1.9)
    routes_keys = jax.random.split(jax.random.fold_in(keys[6], 1), MOE_TOKENS // MOE_ROWS)
    routes_turns = jax.random.permutation(jax.random.fold_in(keys[6], 3), MOE_TOKENS // MOE_ROWS)
    routes = jax.vmap(lambda own, number: routed_block(jax.random.fold_in(keys[6], 2), own, number, MOE_ROWS, EXPERTS, TOPK, CAP, 2))(routes_keys, routes_turns).reshape((MOE_TOKENS, TOPK))
    route_weights = jnp.clip(0.1 + 0.9 * jax.random.uniform(keys[7], (MOE_TOKENS, TOPK), jnp.float32) ** block_scale(keys[7], (MOE_TOKENS, TOPK), ((0, 32),), -0.2, 0.2), 0.1, 1.0)
    gate_weight = normal_values(keys[8], (EXPERTS, D, FE), D ** -0.5, 0.125, ((0, 8), (2, 4)))
    up_weight = normal_values(keys[9], (EXPERTS, D, FE), D ** -0.5, 0.125, ((0, 8), (2, 4)))
    down_weight = normal_values(keys[10], (EXPERTS, FE, D), FE ** -0.5, 0.1875, ((0, 8), (1, 4)))
    return dict(queries=queries, keys_values=keys_values, sink_logits=sink_logits, out_weight=out_weight, expert_tokens=expert_tokens, norm_gain=norm_gain, routes=routes, route_weights=route_weights, gate_weight=gate_weight, up_weight=up_weight, down_weight=down_weight)


NEG_FILL = -1e+30

def attend_all(queries, keys_values, sink_logits):
    seq_total = queries.shape[0]
    block_rows = min(512, seq_total)
    key_span = block_rows + 2 * WINDOW
    query_all = queries.astype(jnp.float32).reshape(seq_total, KV_HEADS, GROUP, HEAD_DIM)
    pair_all = keys_values.astype(jnp.float32).reshape(seq_total, KV_HEADS, 2, HEAD_DIM)
    padded = jnp.pad(pair_all, ((WINDOW, WINDOW), (0, 0), (0, 0), (0, 0)))
    sink_grid = sink_logits.astype(jnp.float32).reshape(KV_HEADS, GROUP, 1, 1)

    def one_block(block_index):
        first_row = block_index * block_rows
        query_block = lax.dynamic_slice_in_dim(query_all, first_row, block_rows, 0)
        pair_block = lax.dynamic_slice_in_dim(padded, first_row, key_span, 0)
        scores = jnp.einsum('qhgd,khd->hgqk', query_block, pair_block[:, :, 0]) * HEAD_DIM ** (-0.5)
        query_pos = first_row + jnp.arange(block_rows, dtype=jnp.int32)
        key_pos = first_row - WINDOW + jnp.arange(key_span, dtype=jnp.int32)
        allowed = (jnp.abs(query_pos[:, None] - key_pos[None, :]) <= WINDOW) & (key_pos >= 0)[None, :] & (key_pos < seq_total)[None, :]
        scores = jnp.where(allowed, scores, NEG_FILL)
        top_score = jnp.maximum(lax.optimization_barrier(jnp.max(scores, -1, keepdims=True)), sink_grid)
        exp_scores = jnp.exp(scores - top_score)
        denominator = lax.optimization_barrier(jnp.sum(exp_scores, -1, keepdims=True)) + jnp.exp(sink_grid - top_score)
        attn_weights = lax.optimization_barrier((exp_scores / denominator).astype(jnp.bfloat16)).astype(jnp.float32)
        head_values = jnp.einsum('hgqk,khd->qhgd', attn_weights, pair_block[:, :, 1])
        return head_values.astype(jnp.bfloat16).reshape(block_rows, HEADS * HEAD_DIM)
    blocks = lax.map(one_block, jnp.arange(seq_total // block_rows, dtype=jnp.int32))
    return blocks.reshape(seq_total, HEADS * HEAD_DIM)

def reference(queries, keys_values, sink_logits, out_weight, expert_tokens, norm_gain, routes, route_weights, gate_weight, up_weight, down_weight):
    attended = attend_all(queries, keys_values, sink_logits)
    mixer_out = jnp.dot(attended, out_weight, preferred_element_type=jnp.float32).astype(jnp.bfloat16)
    token_total = expert_tokens.shape[0]
    block_count = token_total // MOE_ROWS
    rows_float = expert_tokens.astype(jnp.float32)
    centred = rows_float - lax.optimization_barrier(jnp.mean(rows_float, -1, keepdims=True))
    normed = (centred * lax.rsqrt(lax.optimization_barrier(jnp.mean(centred * centred, -1, keepdims=True)) + 1e-06) * norm_gain).astype(jnp.bfloat16)
    flat_routes = routes.reshape(block_count, MOE_ROWS * TOPK).astype(jnp.int32)
    one_hot = (flat_routes[:, :, None] == jnp.arange(EXPERTS, dtype=jnp.int32)[None, None, :]).astype(jnp.int32)
    slot_rank = lax.optimization_barrier(jnp.sum((jnp.cumsum(one_hot, 1) - 1) * one_hot, -1))
    block_ids = jnp.arange(block_count, dtype=jnp.int32)[:, None]
    expert_slot = (flat_routes * (block_count * CAP) + block_ids * CAP + slot_rank).reshape(-1)
    copy_token = (block_ids * MOE_ROWS + jnp.arange(MOE_ROWS * TOPK, dtype=jnp.int32)[None, :] // TOPK).reshape(-1)
    slot_table = jnp.full((EXPERTS * block_count * CAP,), token_total, jnp.int32).at[expert_slot].set(copy_token)
    slot_table = slot_table.reshape(EXPERTS, block_count * CAP)
    weight_table = jnp.zeros((EXPERTS * block_count * CAP,), jnp.float32).at[expert_slot].set(route_weights.reshape(-1))
    weight_table = weight_table.reshape(EXPERTS, block_count * CAP)
    quarter = FE // N_TP

    def add_expert(running, expert_index):
        token_index = slot_table[expert_index]
        chosen = jnp.take(normed, token_index, axis=0, mode='fill', fill_value=0)
        gate_value = jnp.dot(chosen, gate_weight[expert_index], preferred_element_type=jnp.float32)
        up_value = jnp.dot(chosen, up_weight[expert_index], preferred_element_type=jnp.float32)
        hidden = (jax.nn.silu(gate_value) * up_value).astype(jnp.bfloat16)
        hidden_parts = hidden.astype(jnp.float32).reshape(-1, N_TP, quarter)
        down_parts = down_weight[expert_index].astype(jnp.float32).reshape(N_TP, quarter, -1)
        partial_value = jnp.einsum('rqf,qfd->qrd', hidden_parts, down_parts)
        partial_value = lax.optimization_barrier(partial_value.astype(jnp.bfloat16)).astype(jnp.float32)
        copy_result = lax.optimization_barrier(jnp.sum(partial_value, 0)).astype(jnp.bfloat16)
        update = lax.optimization_barrier(copy_result).astype(jnp.float32) * weight_table[expert_index][:, None]
        return (running.at[token_index].add(update, mode='drop'), None)
    total_out, unused = lax.scan(add_expert, jnp.zeros((token_total, expert_tokens.shape[1]), jnp.float32), jnp.arange(EXPERTS, dtype=jnp.int32))
    expert_out = total_out.astype(jnp.bfloat16)
    return (mixer_out, expert_out)
```

```python
import functools

import jax
import jax.numpy as jnp
from jax import lax
from jax.experimental import pallas as pl
from jax.experimental.pallas import tpu as pltpu
from jax.sharding import PartitionSpec as P

HEAD_DIM = 64
WINDOW = 128
TOPK = 2
PLANES = 4
CHUNKS = 4
STEP_ROWS = 128
NEG_FILL = -1e30
MESH = pl.DeviceIdType.MESH


def div(a, b):
    return lax.div(a, jnp.int32(b))


def rem(a, b):
    return lax.rem(a, jnp.int32(b))


def layer_kernel(n, tp, cap, stride, *refs):
    (
        sink, q_hbm, kv_hbm, ow_hbm, tok_hbm, gain, routes, rweights, gate_hbm, up_hbm, down_hbm,
        mix_hbm, out_hbm,
        tok_v, norm_v, info, info_in, block_in, x_in, near_out, relay_out, sel,
        gate_s, up_s, down_s, hid, res, relay_in, merged, near_in, far_in,
        mix_hi, mix_lo, out_v,
        q_v, kv_s, vk_s, att, att_in, ow_v, mo_v,
        load_sem, w_recv, w_near_send, w_far_send, w_fwd_send,
        halo_recv, halo_send, info_recv, info_send, block_recv, block_send,
        near_recv, near_send, pack_recv, pack_send,
        back_near_recv, back_near_send, back_far_send, back_own_send,
        relay_recv, merged_send, far_recv, att_recv, att_send, store_sem,
    ) = refs
    count, width = tok_v.shape
    wide = width // CHUNKS
    half_count = n // 2
    members = n // PLANES
    rows = half_count * stride
    group = members * stride
    side = tp // 2
    shard = gate_s.shape[2]
    seq_rows, q_width = q_v.shape
    heads = q_width // HEAD_DIM
    kv_heads = kv_s.shape[1] // (2 * HEAD_DIM)
    fan = heads // kv_heads
    own_count = seq_rows // tp

    e = lax.axis_index("ep")
    t = lax.axis_index("tp")
    plane = div(e, members)
    member = rem(e, members)
    half = div(e, half_count)
    local = rem(e, half_count)
    other = 1 - half
    is_relay = jnp.logical_or(plane == 1, plane == 2)
    own_relay_plane = 1 + half
    far_relay = (1 + other) * members + member
    tp_base = t - rem(t, side)
    tp_far = rem(t + side, tp)

    def near_tp(k):
        return tp_base + rem(t - tp_base + k, side)

    def near_ep(j):
        return rem(local + j, half_count)

    def far_source(s, k):
        return (other * 2 + s) * members + rem(member + k, members)

    def at(start, size):
        return pl.ds(pl.multiple_of(start, 16), size)

    def cols(c):
        return pl.ds(c * wide, wide)

    def remote(src, dst, send, recv, **where):
        return pltpu.make_async_remote_copy(
            src_ref=src, dst_ref=dst, send_sem=send, recv_sem=recv,
            device_id=where, device_id_type=MESH,
        )

    def arrived(ref, sem):
        pltpu.make_async_copy(ref, ref, sem).wait()

    kv_own = kv_s.at[pl.ds(WINDOW, seq_rows), :]
    loads = [
        pltpu.make_async_copy(tok_hbm, tok_v, load_sem.at[0]),
        pltpu.make_async_copy(kv_hbm, kv_own, load_sem.at[1]),
        pltpu.make_async_copy(q_hbm, q_v, load_sem.at[2]),
        pltpu.make_async_copy(ow_hbm, ow_v, load_sem.at[3]),
    ]
    items = 2 + CHUNKS

    def w_source(item):
        if item == 0:
            return gate_hbm
        if item == 1:
            return up_hbm
        return down_hbm.at[:, cols(item - 2)]

    def w_place(item, slot):
        if item == 0:
            return gate_s.at[slot]
        if item == 1:
            return up_s.at[slot]
        return down_s.at[item - 2, pl.ds(slot * shard, shard), :]

    own_weights = [
        pltpu.make_async_copy(w_source(i), w_place(i, 0), w_recv.at[i, 0]) for i in range(items)
    ]
    for copy in loads:
        copy.start()

    barrier = pltpu.get_barrier_semaphore()

    def greet(**where):
        pl.semaphore_signal(barrier, inc=1, device_id=where, device_id_type=MESH)

    for j in range(1, half_count):
        greet(ep=half * half_count + near_ep(j))
    for k in range(1, tp):
        greet(tp=rem(t + k, tp))

    @pl.when(e > 0)
    def greet_before():
        greet(ep=e - 1)

    @pl.when(e < n - 1)
    def greet_after():
        greet(ep=e + 1)

    @pl.when(is_relay)
    def greet_sources():
        for s in range(2):
            greet(ep=far_source(s, 0))

    @pl.when(jnp.logical_not(is_relay))
    def greet_relay():
        greet(ep=far_relay)

    def one(flag):
        return jnp.where(flag, 1, 0).astype(jnp.int32)

    pl.semaphore_wait(
        barrier, half_count - 1 + tp - 1 + one(e > 0) + one(e < n - 1) + 1 + one(is_relay)
    )

    halo_after = remote(
        kv_hbm.at[pl.ds(seq_rows - WINDOW, WINDOW), :], kv_s.at[pl.ds(0, WINDOW), :],
        halo_send.at[0], halo_recv.at[0], ep=rem(e + 1, n),
    )
    halo_before = remote(
        kv_hbm.at[pl.ds(0, WINDOW), :], kv_s.at[pl.ds(seq_rows + WINDOW, WINDOW), :],
        halo_send.at[1], halo_recv.at[1], ep=rem(e + n - 1, n),
    )

    @pl.when(e < n - 1)
    def send_after():
        halo_after.start()

    @pl.when(e > 0)
    def send_before():
        halo_before.start()

    w_far = [
        remote(w_source(i), w_place(i, side), w_far_send.at[i], w_recv.at[i, side], tp=tp_far)
        for i in range(items)
    ]
    w_near = [
        remote(
            w_source(i), w_place(i, (side - k) % side), w_near_send.at[i, k],
            w_recv.at[i, (side - k) % side], tp=near_tp(k),
        )
        for i in range(items)
        for k in range(1, side)
    ]
    w_fwd = {
        i: [
            remote(
                w_place(i, side), w_place(i, side + (side - k) % side), w_fwd_send.at[i, k],
                w_recv.at[i, side + (side - k) % side], tp=near_tp(k),
            )
            for k in range(1, side)
        ]
        for i in range(items)
    }
    for copy in w_far:
        copy.start()

    loads[0].wait()
    tokens = tok_v[...].astype(jnp.float32)
    centred = tokens - jnp.mean(tokens, -1, keepdims=True)
    scale = lax.rsqrt(jnp.mean(centred * centred, -1, keepdims=True) + 1e-06)
    normed = (centred * scale * gain[...]).astype(jnp.bfloat16)
    for c in range(CHUNKS):
        norm_v[c] = normed[:, c * wide : (c + 1) * wide]

    expert = lax.broadcasted_iota(jnp.int32, (n, count), 0)
    named = [expert == routes[k : k + 1, :] for k in range(TOPK)]
    member_of = functools.reduce(jnp.logical_or, named)
    earlier = lax.broadcasted_iota(jnp.int32, (count, count), 0) < lax.broadcasted_iota(
        jnp.int32, (count, count), 1
    )
    rank = jnp.dot(
        jnp.where(member_of, 1.0, 0.0).astype(jnp.bfloat16),
        jnp.where(earlier, 1.0, 0.0).astype(jnp.bfloat16),
        preferred_element_type=jnp.float32,
    )
    place = expert.astype(jnp.float32) * float(stride) + rank
    info[...] = jnp.zeros_like(info)
    for k in range(TOPK):
        info[k : k + 1, :] = jnp.sum(jnp.where(named[k], place, 0.0), 0, keepdims=True)
        info[TOPK + k : TOPK + k + 1, :] = rweights[k : k + 1, :]

    slot_of = rem(plane, 2)
    send_info = remote(info, info_in.at[slot_of], info_send, info_recv.at[slot_of], ep=far_relay)
    send_info.start()
    send_blocks = [
        remote(
            norm_v.at[c], block_in.at[slot_of, c], block_send.at[c], block_recv.at[slot_of, c],
            ep=far_relay,
        )
        for c in range(CHUNKS)
    ]
    for copy in send_blocks:
        copy.start()
    for copy in w_near:
        copy.start()
    for copy in own_weights:
        copy.start()

    base = half * rows

    def hits(table, k):
        slot = lax.broadcasted_iota(jnp.int32, (rows, count), 0) + base
        return slot.astype(jnp.float32) == table[k : k + 1, :]

    def pick(table):
        hit = functools.reduce(jnp.logical_or, [hits(table, k) for k in range(TOPK)])
        return jnp.where(hit, 1.0, 0.0).astype(jnp.bfloat16)

    def mixture(table, where):
        mix = sum(
            jnp.where(hits(table, k), table[TOPK + k : TOPK + k + 1, :], 0.0)
            for k in range(TOPK)
        ).T
        high = mix.astype(jnp.bfloat16)
        mix_hi[where] = high
        mix_lo[where] = (mix - high.astype(jnp.float32)).astype(jnp.bfloat16)

    own_table = info[...]
    sel[2] = pick(own_table)
    for c in range(CHUNKS):
        near_out[:, cols(c)] = jnp.dot(
            sel[2], norm_v[c], preferred_element_type=jnp.float32
        ).astype(jnp.bfloat16)
    own_rows = at(e * stride, stride)
    near_self = pltpu.make_async_copy(
        near_out.at[at(local * stride, stride), :], x_in.at[own_rows, :], near_recv
    )
    near_self.start()
    for j in range(1, half_count):
        remote(
            near_out.at[at(near_ep(j) * stride, stride), :], x_in.at[own_rows, :],
            near_send, near_recv, ep=half * half_count + near_ep(j),
        ).start()
    mixture(own_table, 2)

    loads[1].wait()

    @pl.when(e == 0)
    def no_before():
        kv_s[0:WINDOW, :] = jnp.zeros((WINDOW, kv_s.shape[1]), kv_s.dtype)

    @pl.when(e > 0)
    def got_before():
        halo_after.wait_recv()

    @pl.when(e == n - 1)
    def no_after():
        kv_s[seq_rows + WINDOW : seq_rows + 2 * WINDOW, :] = jnp.zeros(
            (WINDOW, kv_s.shape[1]), kv_s.dtype
        )

    @pl.when(e < n - 1)
    def got_after():
        halo_before.wait_recv()

    for kv_head in range(kv_heads):
        lanes = slice(kv_head * 2 * HEAD_DIM, (kv_head + 1) * 2 * HEAD_DIM)
        both = kv_s[:, lanes]
        vk_s[:, lanes] = jnp.concatenate([both[:, HEAD_DIM:], both[:, :HEAD_DIM]], 1)
    loads[2].wait()

    span = STEP_ROWS + 2 * WINDOW
    seq_total = seq_rows * n
    lower = lax.broadcasted_iota(jnp.int32, (STEP_ROWS, 2 * HEAD_DIM), 1) < HEAD_DIM

    def attend_step(start):
        start = pl.multiple_of(start, STEP_ROWS)
        row = lax.broadcasted_iota(jnp.int32, (STEP_ROWS, span), 0)
        column = lax.broadcasted_iota(jnp.int32, (STEP_ROWS, span), 1)
        key_pos = e * seq_rows + start - WINDOW + column
        allowed = (
            (column >= row) & (column <= row + 2 * WINDOW)
            & (key_pos >= 0) & (key_pos < seq_total)
        )
        for kv_head in range(kv_heads):
            lanes = slice(kv_head * 2 * HEAD_DIM, (kv_head + 1) * 2 * HEAD_DIM)
            kv = kv_s[pl.ds(start, span), lanes]
            vk = vk_s[pl.ds(start, span), lanes]
            for pair in range(fan // 2):
                head = kv_head * fan + 2 * pair
                places = slice(head * HEAD_DIM, (head + 2) * HEAD_DIM)
                q_pair = q_v[pl.ds(start, STEP_ROWS), places] * jnp.bfloat16(HEAD_DIM ** -0.5)
                results = []
                for odd in range(2):
                    q_one = jnp.where(lower != bool(odd), q_pair, jnp.zeros_like(q_pair))
                    key_side, value_side = (vk, kv) if odd else (kv, vk)
                    scores = lax.dot_general(
                        q_one, key_side, (((1,), (1,)), ((), ())),
                        preferred_element_type=jnp.float32,
                    )
                    scores = jnp.where(allowed, scores, NEG_FILL)
                    bound = sink[t * heads + head + odd]
                    top = jnp.maximum(jnp.max(scores, 1, keepdims=True), bound)
                    expo = jnp.exp(scores - top)
                    denom = jnp.sum(expo, 1, keepdims=True) + jnp.exp(bound - top)
                    value = jnp.dot(
                        expo.astype(jnp.bfloat16), value_side, preferred_element_type=jnp.float32
                    )
                    results.append(value / denom)
                att[pl.ds(start, STEP_ROWS), places] = jnp.where(
                    lower, results[0], results[1]
                ).astype(jnp.bfloat16)

    def attend_block(k):
        owner = rem(t + k, tp)

        def step(i, carry):
            attend_step(owner * own_count + i * STEP_ROWS)
            return carry

        lax.fori_loop(0, own_count // STEP_ROWS, step, 0)
        block = att.at[at(owner * own_count, own_count), :]
        if k == 0:
            pltpu.make_async_copy(block, att_in.at[t], att_recv.at[0]).start()
        else:
            remote(block, att_in.at[t], att_send.at[k], att_recv.at[k], tp=owner).start()

    def relay_tables():
        for s in range(2):
            arrived(info_in.at[s], info_recv.at[s])
            table = info_in[s]
            sel[s] = pick(table)
            mixture(table, s)

    def relay_forward(c):
        for s in (1, 0):
            arrived(block_in.at[s, c], block_recv.at[s, c])
            relay_out[s, c] = jnp.dot(
                sel[s], block_in[s, c], preferred_element_type=jnp.float32
            ).astype(jnp.bfloat16)
            landing = x_in.at[at(far_source(s, 0) * stride, stride), cols(c)]
            for j in list(range(1, half_count)):
                remote(
                    relay_out.at[s, c, at(near_ep(j) * stride, stride), :], landing,
                    pack_send.at[s, c], pack_recv.at[s], ep=half * half_count + near_ep(j),
                ).start()
            pltpu.make_async_copy(
                relay_out.at[s, c, at(local * stride, stride), :], landing, pack_recv.at[s]
            ).start()

    def on_relay(task, *args):
        pl.when(is_relay)(lambda: task(*args))

    def forward_weights(i):
        arrived(w_place(i, side), w_recv.at[i, side])
        for copy in w_fwd[i]:
            copy.start()

    def hidden_rows(start, size, slot):
        x = x_in[at(start, size), :]
        gate = jnp.dot(x, gate_s[slot], preferred_element_type=jnp.float32)
        up = jnp.dot(x, up_s[slot], preferred_element_type=jnp.float32)
        hid[at(start, size), pl.ds(slot * shard, shard)] = (
            gate / (1.0 + jnp.exp(-gate)) * up
        ).astype(jnp.bfloat16)

    def got_weights(item, slot):
        arrived(w_place(item, slot), w_recv.at[item, slot])

    def project():
        arrived(att_in.at[0], att_recv.at[0])
        for k in range(1, tp):
            arrived(att_in.at[0], att_recv.at[k])
        loads[3].wait()
        total = jnp.zeros(mo_v.shape, jnp.float32)
        for c in range(CHUNKS):
            total = sum(
                jnp.dot(
                    att_in[k], ow_v[k * q_width : (k + 1) * q_width, cols(c)],
                    preferred_element_type=jnp.float32,
                )
                for k in range(tp)
            )
            mo_v[:, cols(c)] = total.astype(jnp.bfloat16)
        pltpu.make_async_copy(mo_v, mix_hbm, store_sem.at[CHUNKS]).start()

    on_relay(relay_tables)
    for k in range(1, 3):
        attend_block(k)
    on_relay(relay_forward, 0)
    for k in range(3, tp):
        attend_block(k)
    forward_weights(0)
    on_relay(relay_forward, 1)
    attend_block(0)
    for slot in range(side):
        for item in range(2):
            got_weights(item, slot)
    on_relay(relay_forward, 2)
    project()
    arrived(x_in.at[at(half * rows, rows), :], near_recv)
    for slot in range(side):
        hidden_rows(half * rows, rows, slot)
    forward_weights(1)
    on_relay(relay_forward, 3)
    for c in range(4, CHUNKS):
        on_relay(relay_forward, c)
    for slot in range(side, tp):
        for item in range(2):
            if slot > side:
                got_weights(item, slot)
        hidden_rows(half * rows, rows, slot)
    forward_weights(2)
    for s in (1, 0):
        arrived(x_in.at[at((other * 2 + s) * group, group), :], pack_recv.at[s])
    for slot in range(tp):
        hidden_rows(other * rows, rows, slot)

    def results(c):
        for slot in range(tp):
            if slot != side:
                got_weights(2 + c, slot)
        res[c] = jnp.dot(hid[...], down_s[c], preferred_element_type=jnp.float32).astype(
            jnp.bfloat16
        )
        for s in range(2):
            for k in range(members):
                block = res.at[c, at(far_source(s, k) * stride, stride), :]
                landing = relay_in.at[s, c, at(local * stride, stride), :]
                relay = own_relay_plane * members + rem(member + k, members)
                if k:
                    remote(
                        block, landing, back_far_send.at[c], relay_recv.at[s, c], ep=relay
                    ).start()
                else:

                    @pl.when(is_relay)
                    def keep():
                        pltpu.make_async_copy(block, landing, relay_recv.at[s, c]).start()

                    @pl.when(jnp.logical_not(is_relay))
                    def send():
                        remote(
                            block, landing, back_own_send.at[c], relay_recv.at[s, c], ep=relay
                        ).start()

        landing = near_in.at[c, at(local * stride, stride), :]
        for j in range(1, half_count):
            target = half * half_count + near_ep(j)
            remote(
                res.at[c, at(target * stride, stride), :], landing,
                back_near_send.at[c], back_near_recv.at[c], ep=target,
            ).start()
        pltpu.make_async_copy(
            res.at[c, own_rows, :], landing, back_near_recv.at[c]
        ).start()

    def mixed(where, values):
        return jnp.dot(
            mix_hi[where], values, preferred_element_type=jnp.float32
        ) + jnp.dot(mix_lo[where], values, preferred_element_type=jnp.float32)

    def relay_merge(c):
        for s in range(2):
            arrived(relay_in.at[s, c], relay_recv.at[s, c])
            merged[s, c] = mixed(s, relay_in[s, c]).astype(jnp.bfloat16)
            remote(
                merged.at[s, c], far_in.at[c], merged_send.at[s, c], far_recv.at[c],
                ep=far_source(s, 0),
            ).start()

    def finish(c):
        arrived(near_in.at[c], back_near_recv.at[c])
        total = mixed(2, near_in[c])
        arrived(far_in.at[c], far_recv.at[c])
        out_v[:, cols(c)] = (total + far_in[c].astype(jnp.float32)).astype(jnp.bfloat16)
        pltpu.make_async_copy(
            out_v.at[:, cols(c)], out_hbm.at[:, cols(c)], store_sem.at[c]
        ).start()

    for step in range(CHUNKS + 4):
        if step < CHUNKS:
            results(step)
        if step + 1 < CHUNKS:
            forward_weights(2 + step + 1)
        if 1 <= step <= CHUNKS:
            on_relay(relay_merge, step - 1)
        if 3 <= step < CHUNKS + 3:
            finish(step - 3)

    for c in range(CHUNKS):
        pltpu.make_async_copy(
            out_v.at[:, cols(c)], out_hbm.at[:, cols(c)], store_sem.at[c]
        ).wait()
    pltpu.make_async_copy(mo_v, mix_hbm, store_sem.at[CHUNKS]).wait()

    def sent(ref, sem):
        pltpu.make_async_copy(ref, ref, sem).wait()

    @pl.when(e < n - 1)
    def sent_after():
        halo_after.wait_send()

    @pl.when(e > 0)
    def sent_before():
        halo_before.wait_send()

    for copy in w_far + w_near + [c for i in range(items) for c in w_fwd[i]]:
        copy.wait_send()
    send_info.wait_send()
    for copy in send_blocks:
        copy.wait_send()
    others = half_count - 1
    sent(near_out.at[pl.ds(0, others * stride), :], near_send)
    for k in range(1, tp):
        sent(att_in.at[0], att_send.at[k])
    for c in range(CHUNKS):
        sent(near_in.at[c, pl.ds(0, others * stride), :], back_near_send.at[c])
        sent(res.at[c, pl.ds(0, 2 * (members - 1) * stride), :], back_far_send.at[c])

        @pl.when(is_relay)
        def sent_relay():
            for s in range(2):
                sent(relay_out.at[s, c, pl.ds(0, others * stride), :], pack_send.at[s, c])
                sent(merged.at[s, c], merged_send.at[s, c])

        @pl.when(jnp.logical_not(is_relay))
        def sent_own():
            sent(res.at[c, pl.ds(0, 2 * stride), :], back_own_send.at[c])


def body(
    queries,
    keys_values,
    sink_logits,
    out_weight,
    expert_tokens,
    norm_gain,
    routes,
    route_weights,
    gate_weight,
    up_weight,
    down_weight,
):
    n, tp = lax.axis_size("ep"), lax.axis_size("tp")
    count, width = expert_tokens.shape
    cap = 3 * count * TOPK // (2 * n)
    stride = -(-cap // 16) * 16
    rows = n // 2 * stride
    wide = width // CHUNKS
    shard = gate_weight.shape[2]
    seq_rows, q_width = queries.shape
    kv_width = keys_values.shape[1]
    items = 2 + CHUNKS
    side = tp // 2
    bf16, f32 = jnp.bfloat16, jnp.float32
    dma = pltpu.SemaphoreType.DMA

    def vmem(*shape, dtype=bf16):
        return pltpu.VMEM(shape, dtype)

    scratch = [
        vmem(count, width),
        vmem(CHUNKS, count, wide),
        vmem(8, count, dtype=f32),
        vmem(2, 8, count, dtype=f32),
        vmem(2, CHUNKS, count, wide),
        vmem(n * stride, width),
        vmem(rows, width),
        vmem(2, CHUNKS, rows, wide),
        vmem(3, rows, count),
        vmem(tp, width, shard),
        vmem(tp, width, shard),
        vmem(CHUNKS, tp * shard, wide),
        vmem(n * stride, tp * shard),
        vmem(CHUNKS, n * stride, wide),
        vmem(2, CHUNKS, rows, wide),
        vmem(2, CHUNKS, count, wide),
        vmem(CHUNKS, rows, wide),
        vmem(CHUNKS, count, wide),
        vmem(3, count, rows),
        vmem(3, count, rows),
        vmem(count, width),
        vmem(seq_rows, q_width),
        vmem(seq_rows + 2 * WINDOW, kv_width),
        vmem(seq_rows + 2 * WINDOW, kv_width),
        vmem(seq_rows, q_width),
        vmem(tp, seq_rows // tp, q_width),
        vmem(*out_weight.shape),
        vmem(seq_rows // tp, width),
        dma((4,)),
        dma((items, tp)),
        dma((items, side)),
        dma((items,)),
        dma((items, side)),
        dma((2,)),
        dma((2,)),
        dma((2,)),
        dma,
        dma((2, CHUNKS)),
        dma((CHUNKS,)),
        dma,
        dma,
        dma((2,)),
        dma((2, CHUNKS)),
        dma((CHUNKS,)),
        dma((CHUNKS,)),
        dma((CHUNKS,)),
        dma((CHUNKS,)),
        dma((2, CHUNKS)),
        dma((2, CHUNKS)),
        dma((CHUNKS,)),
        dma((tp,)),
        dma((tp,)),
        dma((CHUNKS + 1,)),
    ]
    anywhere = pl.BlockSpec(memory_space=pl.ANY)
    small = pl.BlockSpec(memory_space=pltpu.VMEM)
    return pl.pallas_call(
        functools.partial(layer_kernel, n, tp, cap, stride),
        out_shape=(
            jax.ShapeDtypeStruct((seq_rows // tp, width), bf16),
            jax.ShapeDtypeStruct((count, width), bf16),
        ),
        in_specs=[
            pl.BlockSpec(memory_space=pltpu.SMEM), anywhere, anywhere, anywhere, anywhere,
            small, small, small, anywhere, anywhere, anywhere,
        ],
        out_specs=(anywhere, anywhere),
        scratch_shapes=scratch,
        compiler_params=pltpu.CompilerParams(
            collective_id=0, has_side_effects=True, vmem_limit_bytes=67043328
        ),
        name="layer",
    )(
        sink_logits, queries, keys_values, out_weight, expert_tokens,
        norm_gain.reshape(1, width), routes.T, route_weights.T,
        gate_weight[0], up_weight[0], down_weight[0],
    )


def solution(mesh):
    return jax.shard_map(
        body,
        mesh=mesh,
        in_specs=(
            P("ep", "tp"),
            P("ep", "tp"),
            P(),
            P(),
            P(("ep", "tp"), None),
            P(),
            P(("ep", "tp"), None),
            P(("ep", "tp"), None),
            P("ep", None, "tp"),
            P("ep", None, "tp"),
            P("ep", "tp", None),
        ),
        out_specs=(P(("ep", "tp"), None), P(("ep", "tp"), None)),
        check_vma=False,
    )
```

```python
import functools

import jax
import jax.numpy as jnp
from jax import lax
from jax.experimental import pallas as pl
from jax.experimental.pallas import tpu as pltpu
from jax.sharding import PartitionSpec as P

HEAD_DIM = 64
WINDOW = 128
TOPK = 2
PLANES = 4
CHUNKS = 8
STEP_ROWS = 128
NEG_FILL = -1e30
MESH = pl.DeviceIdType.MESH


def div(a, b):
    return lax.div(a, jnp.int32(b))


def rem(a, b):
    return lax.rem(a, jnp.int32(b))


def layer_kernel(n, tp, cap, stride, *refs):
    (
        sink, q_hbm, kv_hbm, ow_hbm, tok_hbm, gain, routes, rweights, gate_hbm, up_hbm, down_hbm,
        mix_hbm, out_hbm,
        tok_v, norm_v, info, info_in, block_in, x_in, near_out, relay_out, sel,
        gate_s, up_s, down_s, hid, res, relay_in, merged, near_in, far_in,
        mix_hi, mix_lo, out_v,
        q_v, kv_s, vk_s, att, att_in, ow_v, mo_v,
        load_sem, w_recv, w_near_send, w_far_send, w_fwd_send,
        halo_recv, halo_send, info_recv, info_send, block_recv, block_send,
        near_recv, near_send, pack_recv, pack_send,
        back_near_recv, back_near_send, back_far_send, back_own_send,
        relay_recv, merged_send, far_recv, att_recv, att_send, store_sem,
    ) = refs
    count, width = tok_v.shape
    wide = width // CHUNKS
    half_count = n // 2
    members = n // PLANES
    rows = half_count * stride
    group = members * stride
    side = tp // 2
    shard = gate_s.shape[2]
    seq_rows, q_width = q_v.shape
    heads = q_width // HEAD_DIM
    kv_heads = kv_s.shape[1] // (2 * HEAD_DIM)
    fan = heads // kv_heads
    own_count = seq_rows // tp

    e = lax.axis_index("ep")
    t = lax.axis_index("tp")
    plane = div(e, members)
    member = rem(e, members)
    half = div(e, half_count)
    local = rem(e, half_count)
    other = 1 - half
    is_relay = jnp.logical_or(plane == 1, plane == 2)
    own_relay_plane = 1 + half
    far_relay = (1 + other) * members + member
    tp_base = t - rem(t, side)
    tp_far = rem(t + side, tp)

    def near_tp(k):
        return tp_base + rem(t - tp_base + k, side)

    def near_ep(j):
        return rem(local + j, half_count)

    def far_plane(s):
        return 1 + other if s else 3 * other

    def far_source(s, k):
        return far_plane(s) * members + rem(member + k, members)

    def at(start, size):
        return pl.ds(pl.multiple_of(start, 16), size)

    def cols(c):
        return pl.ds(c * wide, wide)

    def remote(src, dst, send, recv, **where):
        return pltpu.make_async_remote_copy(
            src_ref=src, dst_ref=dst, send_sem=send, recv_sem=recv,
            device_id=where, device_id_type=MESH,
        )

    def arrived(ref, sem):
        pltpu.make_async_copy(ref, ref, sem).wait()

    kv_own = kv_s.at[pl.ds(WINDOW, seq_rows), :]
    loads = [
        pltpu.make_async_copy(tok_hbm, tok_v, load_sem.at[0]),
        pltpu.make_async_copy(kv_hbm, kv_own, load_sem.at[1]),
        pltpu.make_async_copy(q_hbm, q_v, load_sem.at[2]),
        pltpu.make_async_copy(ow_hbm, ow_v, load_sem.at[3]),
    ]
    items = 2 + CHUNKS

    def w_source(item):
        if item == 0:
            return gate_hbm
        if item == 1:
            return up_hbm
        return down_hbm.at[:, cols(item - 2)]

    def w_place(item, slot):
        if item == 0:
            return gate_s.at[slot]
        if item == 1:
            return up_s.at[slot]
        return down_s.at[item - 2, pl.ds(slot * shard, shard), :]

    own_weights = [
        pltpu.make_async_copy(w_source(i), w_place(i, 0), w_recv.at[i, 0]) for i in range(items)
    ]
    for copy in loads:
        copy.start()

    barrier = pltpu.get_barrier_semaphore()

    def greet(**where):
        pl.semaphore_signal(barrier, inc=1, device_id=where, device_id_type=MESH)

    for j in range(1, half_count):
        greet(ep=half * half_count + near_ep(j))
    for k in range(1, tp):
        greet(tp=rem(t + k, tp))

    @pl.when(e > 0)
    def greet_before():
        greet(ep=e - 1)

    @pl.when(e < n - 1)
    def greet_after():
        greet(ep=e + 1)

    @pl.when(is_relay)
    def greet_sources():
        for s in range(2):
            greet(ep=far_source(s, 0))

    @pl.when(jnp.logical_not(is_relay))
    def greet_relay():
        greet(ep=far_relay)

    def one(flag):
        return jnp.where(flag, 1, 0).astype(jnp.int32)

    pl.semaphore_wait(
        barrier, half_count - 1 + tp - 1 + one(e > 0) + one(e < n - 1) + 1 + one(is_relay)
    )

    halo_after = remote(
        kv_hbm.at[pl.ds(seq_rows - WINDOW, WINDOW), :], kv_s.at[pl.ds(0, WINDOW), :],
        halo_send.at[0], halo_recv.at[0], ep=rem(e + 1, n),
    )
    halo_before = remote(
        kv_hbm.at[pl.ds(0, WINDOW), :], kv_s.at[pl.ds(seq_rows + WINDOW, WINDOW), :],
        halo_send.at[1], halo_recv.at[1], ep=rem(e + n - 1, n),
    )

    @pl.when(e < n - 1)
    def send_after():
        halo_after.start()

    @pl.when(e > 0)
    def send_before():
        halo_before.start()

    w_far = [
        remote(w_source(i), w_place(i, side), w_far_send.at[i], w_recv.at[i, side], tp=tp_far)
        for i in range(items)
    ]
    w_near = [
        remote(
            w_source(i), w_place(i, (side - k) % side), w_near_send.at[i, k],
            w_recv.at[i, (side - k) % side], tp=near_tp(k),
        )
        for i in range(items)
        for k in range(1, side)
    ]
    w_fwd = {
        i: [
            remote(
                w_place(i, side), w_place(i, side + (side - k) % side), w_fwd_send.at[i, k],
                w_recv.at[i, side + (side - k) % side], tp=near_tp(k),
            )
            for k in range(1, side)
        ]
        for i in range(items)
    }
    for copy in w_far:
        copy.start()

    loads[0].wait()
    tokens = tok_v[...].astype(jnp.float32)
    centred = tokens - jnp.mean(tokens, -1, keepdims=True)
    scale = lax.rsqrt(jnp.mean(centred * centred, -1, keepdims=True) + 1e-06)
    normed = (centred * scale * gain[...]).astype(jnp.bfloat16)
    for c in range(CHUNKS):
        norm_v[c] = normed[:, c * wide : (c + 1) * wide]

    expert = lax.broadcasted_iota(jnp.int32, (n, count), 0)
    named = [expert == routes[k : k + 1, :] for k in range(TOPK)]
    member_of = functools.reduce(jnp.logical_or, named)
    earlier = lax.broadcasted_iota(jnp.int32, (count, count), 0) < lax.broadcasted_iota(
        jnp.int32, (count, count), 1
    )
    rank = jnp.dot(
        jnp.where(member_of, 1.0, 0.0).astype(jnp.bfloat16),
        jnp.where(earlier, 1.0, 0.0).astype(jnp.bfloat16),
        preferred_element_type=jnp.float32,
    )
    place = expert.astype(jnp.float32) * float(stride) + rank
    info[...] = jnp.zeros_like(info)
    for k in range(TOPK):
        info[k : k + 1, :] = jnp.sum(jnp.where(named[k], place, 0.0), 0, keepdims=True)
        info[TOPK + k : TOPK + k + 1, :] = rweights[k : k + 1, :]

    slot_of = one(is_relay)
    send_info = remote(info, info_in.at[slot_of], info_send, info_recv.at[slot_of], ep=far_relay)
    send_info.start()
    send_blocks = [
        remote(
            norm_v.at[c], block_in.at[slot_of, c], block_send.at[c], block_recv.at[slot_of, c],
            ep=far_relay,
        )
        for c in range(CHUNKS)
    ]
    for copy in send_blocks:
        copy.start()
    for copy in w_near:
        copy.start()
    for copy in own_weights:
        copy.start()

    base = half * rows

    def hits(table, k):
        slot = lax.broadcasted_iota(jnp.int32, (rows, count), 0) + base
        return slot.astype(jnp.float32) == table[k : k + 1, :]

    def pick(table):
        hit = functools.reduce(jnp.logical_or, [hits(table, k) for k in range(TOPK)])
        return jnp.where(hit, 1.0, 0.0).astype(jnp.bfloat16)

    def mixture(table, where):
        mix = sum(
            jnp.where(hits(table, k), table[TOPK + k : TOPK + k + 1, :], 0.0)
            for k in range(TOPK)
        ).T
        high = mix.astype(jnp.bfloat16)
        mix_hi[where] = high
        mix_lo[where] = (mix - high.astype(jnp.float32)).astype(jnp.bfloat16)

    own_table = info[...]
    sel[2] = pick(own_table)
    for c in range(CHUNKS):
        near_out[:, cols(c)] = jnp.dot(
            sel[2], norm_v[c], preferred_element_type=jnp.float32
        ).astype(jnp.bfloat16)
    own_rows = at(e * stride, stride)
    near_self = pltpu.make_async_copy(
        near_out.at[at(local * stride, stride), :], x_in.at[own_rows, :], near_recv
    )
    near_self.start()
    for j in range(1, half_count):
        remote(
            near_out.at[at(near_ep(j) * stride, stride), :], x_in.at[own_rows, :],
            near_send, near_recv, ep=half * half_count + near_ep(j),
        ).start()
    mixture(own_table, 2)

    loads[1].wait()

    @pl.when(e == 0)
    def no_before():
        kv_s[0:WINDOW, :] = jnp.zeros((WINDOW, kv_s.shape[1]), kv_s.dtype)

    @pl.when(e > 0)
    def got_before():
        halo_after.wait_recv()

    @pl.when(e == n - 1)
    def no_after():
        kv_s[seq_rows + WINDOW : seq_rows + 2 * WINDOW, :] = jnp.zeros(
            (WINDOW, kv_s.shape[1]), kv_s.dtype
        )

    @pl.when(e < n - 1)
    def got_after():
        halo_before.wait_recv()

    for kv_head in range(kv_heads):
        lanes = slice(kv_head * 2 * HEAD_DIM, (kv_head + 1) * 2 * HEAD_DIM)
        both = kv_s[:, lanes]
        vk_s[:, lanes] = jnp.concatenate([both[:, HEAD_DIM:], both[:, :HEAD_DIM]], 1)
    loads[2].wait()

    span = STEP_ROWS + 2 * WINDOW
    seq_total = seq_rows * n
    lower = lax.broadcasted_iota(jnp.int32, (STEP_ROWS, 2 * HEAD_DIM), 1) < HEAD_DIM

    def attend_step(start):
        start = pl.multiple_of(start, STEP_ROWS)
        row = lax.broadcasted_iota(jnp.int32, (STEP_ROWS, span), 0)
        column = lax.broadcasted_iota(jnp.int32, (STEP_ROWS, span), 1)
        key_pos = e * seq_rows + start - WINDOW + column
        allowed = (
            (column >= row) & (column <= row + 2 * WINDOW)
            & (key_pos >= 0) & (key_pos < seq_total)
        )
        for kv_head in range(kv_heads):
            lanes = slice(kv_head * 2 * HEAD_DIM, (kv_head + 1) * 2 * HEAD_DIM)
            kv = kv_s[pl.ds(start, span), lanes]
            vk = vk_s[pl.ds(start, span), lanes]
            for pair in range(fan // 2):
                head = kv_head * fan + 2 * pair
                places = slice(head * HEAD_DIM, (head + 2) * HEAD_DIM)
                q_pair = q_v[pl.ds(start, STEP_ROWS), places] * jnp.bfloat16(HEAD_DIM ** -0.5)
                results = []
                for odd in range(2):
                    q_one = jnp.where(lower != bool(odd), q_pair, jnp.zeros_like(q_pair))
                    key_side, value_side = (vk, kv) if odd else (kv, vk)
                    scores = lax.dot_general(
                        q_one, key_side, (((1,), (1,)), ((), ())),
                        preferred_element_type=jnp.float32,
                    )
                    scores = jnp.where(allowed, scores, NEG_FILL)
                    bound = sink[t * heads + head + odd]
                    top = jnp.maximum(jnp.max(scores, 1, keepdims=True), bound)
                    expo = jnp.exp(scores - top)
                    denom = jnp.sum(expo, 1, keepdims=True) + jnp.exp(bound - top)
                    value = jnp.dot(
                        expo.astype(jnp.bfloat16), value_side, preferred_element_type=jnp.float32
                    )
                    results.append(value / denom)
                att[pl.ds(start, STEP_ROWS), places] = jnp.where(
                    lower, results[0], results[1]
                ).astype(jnp.bfloat16)

    def attend_block(k):
        owner = rem(t + k, tp)

        def step(i, carry):
            attend_step(owner * own_count + i * STEP_ROWS)
            return carry

        lax.fori_loop(0, own_count // STEP_ROWS, step, 0)
        block = att.at[at(owner * own_count, own_count), :]
        if k == 0:
            pltpu.make_async_copy(block, att_in.at[t], att_recv.at[0]).start()
        else:
            remote(block, att_in.at[t], att_send.at[k], att_recv.at[k], tp=owner).start()

    def relay_tables():
        for s in range(2):
            arrived(info_in.at[s], info_recv.at[s])
            table = info_in[s]
            sel[s] = pick(table)
            mixture(table, s)

    def relay_forward(s, c):
        arrived(block_in.at[s, c], block_recv.at[s, c])
        relay_out[s, c] = jnp.dot(
            sel[s], block_in[s, c], preferred_element_type=jnp.float32
        ).astype(jnp.bfloat16)
        landing = x_in.at[at(far_source(s, 0) * stride, stride), cols(c)]
        for j in range(1, half_count):
            remote(
                relay_out.at[s, c, at(near_ep(j) * stride, stride), :], landing,
                pack_send.at[s, c], pack_recv.at[s], ep=half * half_count + near_ep(j),
            ).start()
        pltpu.make_async_copy(
            relay_out.at[s, c, at(local * stride, stride), :], landing, pack_recv.at[s]
        ).start()

    def on_relay(task, *args):
        pl.when(is_relay)(lambda: task(*args))

    def forward_weights(i):
        arrived(w_place(i, side), w_recv.at[i, side])
        for copy in w_fwd[i]:
            copy.start()

    def hidden_rows(start, size, slot):
        x = x_in[at(start, size), :]
        gate = jnp.dot(x, gate_s[slot], preferred_element_type=jnp.float32)
        up = jnp.dot(x, up_s[slot], preferred_element_type=jnp.float32)
        hid[at(start, size), pl.ds(slot * shard, shard)] = (
            gate / (1.0 + jnp.exp(-gate)) * up
        ).astype(jnp.bfloat16)

    def got_weights(item, slot):
        arrived(w_place(item, slot), w_recv.at[item, slot])

    def project():
        arrived(att_in.at[0], att_recv.at[0])
        for k in range(1, tp):
            arrived(att_in.at[0], att_recv.at[k])
        loads[3].wait()
        total = jnp.zeros(mo_v.shape, jnp.float32)
        for c in range(CHUNKS):
            total = sum(
                jnp.dot(
                    att_in[k], ow_v[k * q_width : (k + 1) * q_width, cols(c)],
                    preferred_element_type=jnp.float32,
                )
                for k in range(tp)
            )
            mo_v[:, cols(c)] = total.astype(jnp.bfloat16)
        pltpu.make_async_copy(mo_v, mix_hbm, store_sem.at[CHUNKS]).start()

    def results(s, c):
        first = far_plane(s) * group
        res[c, at(first, group), :] = jnp.dot(
            hid[at(first, group), :], down_s[c], preferred_element_type=jnp.float32
        ).astype(jnp.bfloat16)
        for k in range(members):
            block = res.at[c, at(far_source(s, k) * stride, stride), :]
            landing = relay_in.at[s, c, at(local * stride, stride), :]
            relay = own_relay_plane * members + rem(member + k, members)
            if k:
                remote(
                    block, landing, back_far_send.at[s, c], relay_recv.at[s, c], ep=relay
                ).start()
            else:

                @pl.when(is_relay)
                def keep():
                    pltpu.make_async_copy(block, landing, relay_recv.at[s, c]).start()

                @pl.when(jnp.logical_not(is_relay))
                def send():
                    remote(
                        block, landing, back_own_send.at[s, c], relay_recv.at[s, c], ep=relay
                    ).start()

    def near_results(c):
        first = half * rows
        res[c, at(first, rows), :] = jnp.dot(
            hid[at(first, rows), :], down_s[c], preferred_element_type=jnp.float32
        ).astype(jnp.bfloat16)
        landing = near_in.at[c, at(local * stride, stride), :]
        for j in range(1, half_count):
            target = half * half_count + near_ep(j)
            remote(
                res.at[c, at(target * stride, stride), :], landing,
                back_near_send.at[c], back_near_recv.at[c], ep=target,
            ).start()
        pltpu.make_async_copy(
            res.at[c, own_rows, :], landing, back_near_recv.at[c]
        ).start()

    def mixed(where, values):
        return jnp.dot(
            mix_hi[where], values, preferred_element_type=jnp.float32
        ) + jnp.dot(mix_lo[where], values, preferred_element_type=jnp.float32)

    def relay_merge(s, c):
        arrived(relay_in.at[s, c], relay_recv.at[s, c])
        merged[s, c] = mixed(s, relay_in[s, c]).astype(jnp.bfloat16)
        remote(
            merged.at[s, c], far_in.at[c], merged_send.at[s, c], far_recv.at[c],
            ep=far_source(s, 0),
        ).start()

    def finish(c):
        arrived(near_in.at[c], back_near_recv.at[c])
        total = mixed(2, near_in[c])
        arrived(far_in.at[c], far_recv.at[c])
        out_v[:, cols(c)] = (total + far_in[c].astype(jnp.float32)).astype(jnp.bfloat16)
        pltpu.make_async_copy(
            out_v.at[:, cols(c)], out_hbm.at[:, cols(c)], store_sem.at[c]
        ).start()

    on_relay(relay_tables)
    attend_block(1)
    for c in range(0, 2):
        on_relay(relay_forward, 0, c)
    attend_block(2)
    for c in range(2, 4):
        on_relay(relay_forward, 0, c)
    for k in range(3, tp):
        attend_block(k)
    on_relay(relay_forward, 0, 4)
    attend_block(0)
    for c in range(5, CHUNKS):
        on_relay(relay_forward, 0, c)
    forward_weights(0)
    for slot in range(side):
        for item in range(2):
            got_weights(item, slot)
    for c in range(0, 4):
        on_relay(relay_forward, 1, c)
    first_rows, last_rows = far_plane(0) * group, far_plane(1) * group
    arrived(x_in.at[at(first_rows, group), :], pack_recv.at[0])
    for slot in range(side):
        hidden_rows(first_rows, group, slot)
    for c in range(4, 6):
        on_relay(relay_forward, 1, c)
    arrived(x_in.at[at(half * rows, rows), :], near_recv)
    for slot in range(side):
        hidden_rows(half * rows, rows, slot)
    on_relay(relay_forward, 1, 6)
    forward_weights(1)
    hidden_rows(first_rows, group, side)
    for c in range(7, CHUNKS):
        on_relay(relay_forward, 1, c)
    for slot in range(side + 1, tp):
        for item in range(2):
            got_weights(item, slot)
        hidden_rows(first_rows, group, slot)

    def got_down(c):
        for slot in range(tp):
            if slot != side:
                got_weights(2 + c, slot)

    forward_weights(2)
    hidden_rows(half * rows, rows, side)
    got_down(0)
    results(0, 0)
    forward_weights(3)
    for slot in range(side + 1, tp):
        hidden_rows(half * rows, rows, slot)
    got_down(1)
    results(0, 1)
    arrived(x_in.at[at(last_rows, group), :], pack_recv.at[1])
    for slot in range(tp):
        hidden_rows(last_rows, group, slot)
    results(1, 0)
    results(1, 1)
    merges = [(0, 0), (0, 1), (1, 0), (1, 1)] + [
        (s, c) for c in range(2, CHUNKS) for s in range(2)
    ]
    due = {3: 3, 4: 1, 5: 1, 6: 2, 7: 1}
    for c in range(2, CHUNKS):
        forward_weights(2 + c)
        got_down(c)
        results(0, c)
        results(1, c)
        for _ in range(due.get(c, 0)):
            on_relay(relay_merge, *merges.pop(0))
    for c in range(0, CHUNKS, 2):
        near_results(c)
        near_results(c + 1)
        on_relay(relay_merge, *merges.pop(0))
    project()
    for item in merges:
        on_relay(relay_merge, *item)
    for c in range(CHUNKS):
        finish(c)

    for c in range(CHUNKS):
        pltpu.make_async_copy(
            out_v.at[:, cols(c)], out_hbm.at[:, cols(c)], store_sem.at[c]
        ).wait()
    pltpu.make_async_copy(mo_v, mix_hbm, store_sem.at[CHUNKS]).wait()

    def sent(ref, sem):
        pltpu.make_async_copy(ref, ref, sem).wait()

    @pl.when(e < n - 1)
    def sent_after():
        halo_after.wait_send()

    @pl.when(e > 0)
    def sent_before():
        halo_before.wait_send()

    for copy in w_far + w_near + [c for i in range(items) for c in w_fwd[i]]:
        copy.wait_send()
    send_info.wait_send()
    for copy in send_blocks:
        copy.wait_send()
    others = half_count - 1
    sent(near_out.at[pl.ds(0, others * stride), :], near_send)
    for k in range(1, tp):
        sent(att_in.at[0], att_send.at[k])
    for c in range(CHUNKS):
        sent(near_in.at[c, pl.ds(0, others * stride), :], back_near_send.at[c])
        for s in range(2):
            sent(res.at[c, pl.ds(0, (members - 1) * stride), :], back_far_send.at[s, c])

        @pl.when(is_relay)
        def sent_relay():
            for s in range(2):
                sent(relay_out.at[s, c, pl.ds(0, others * stride), :], pack_send.at[s, c])
                sent(merged.at[s, c], merged_send.at[s, c])

        @pl.when(jnp.logical_not(is_relay))
        def sent_own():
            for s in range(2):
                sent(res.at[c, pl.ds(0, stride), :], back_own_send.at[s, c])


def body(
    queries,
    keys_values,
    sink_logits,
    out_weight,
    expert_tokens,
    norm_gain,
    routes,
    route_weights,
    gate_weight,
    up_weight,
    down_weight,
):
    n, tp = lax.axis_size("ep"), lax.axis_size("tp")
    count, width = expert_tokens.shape
    cap = 3 * count * TOPK // (2 * n)
    stride = -(-cap // 16) * 16
    rows = n // 2 * stride
    wide = width // CHUNKS
    shard = gate_weight.shape[2]
    seq_rows, q_width = queries.shape
    kv_width = keys_values.shape[1]
    items = 2 + CHUNKS
    side = tp // 2
    bf16, f32 = jnp.bfloat16, jnp.float32
    dma = pltpu.SemaphoreType.DMA

    def vmem(*shape, dtype=bf16):
        return pltpu.VMEM(shape, dtype)

    scratch = [
        vmem(count, width),
        vmem(CHUNKS, count, wide),
        vmem(8, count, dtype=f32),
        vmem(2, 8, count, dtype=f32),
        vmem(2, CHUNKS, count, wide),
        vmem(n * stride, width),
        vmem(rows, width),
        vmem(2, CHUNKS, rows, wide),
        vmem(3, rows, count),
        vmem(tp, width, shard),
        vmem(tp, width, shard),
        vmem(CHUNKS, tp * shard, wide),
        vmem(n * stride, tp * shard),
        vmem(CHUNKS, n * stride, wide),
        vmem(2, CHUNKS, rows, wide),
        vmem(2, CHUNKS, count, wide),
        vmem(CHUNKS, rows, wide),
        vmem(CHUNKS, count, wide),
        vmem(3, count, rows),
        vmem(3, count, rows),
        vmem(count, width),
        vmem(seq_rows, q_width),
        vmem(seq_rows + 2 * WINDOW, kv_width),
        vmem(seq_rows + 2 * WINDOW, kv_width),
        vmem(seq_rows, q_width),
        vmem(tp, seq_rows // tp, q_width),
        vmem(*out_weight.shape),
        vmem(seq_rows // tp, width),
        dma((4,)),
        dma((items, tp)),
        dma((items, side)),
        dma((items,)),
        dma((items, side)),
        dma((2,)),
        dma((2,)),
        dma((2,)),
        dma,
        dma((2, CHUNKS)),
        dma((CHUNKS,)),
        dma,
        dma,
        dma((2,)),
        dma((2, CHUNKS)),
        dma((CHUNKS,)),
        dma((CHUNKS,)),
        dma((2, CHUNKS)),
        dma((2, CHUNKS)),
        dma((2, CHUNKS)),
        dma((2, CHUNKS)),
        dma((CHUNKS,)),
        dma((tp,)),
        dma((tp,)),
        dma((CHUNKS + 1,)),
    ]
    anywhere = pl.BlockSpec(memory_space=pl.ANY)
    small = pl.BlockSpec(memory_space=pltpu.VMEM)
    return pl.pallas_call(
        functools.partial(layer_kernel, n, tp, cap, stride),
        out_shape=(
            jax.ShapeDtypeStruct((seq_rows // tp, width), bf16),
            jax.ShapeDtypeStruct((count, width), bf16),
        ),
        in_specs=[
            pl.BlockSpec(memory_space=pltpu.SMEM), anywhere, anywhere, anywhere, anywhere,
            small, small, small, anywhere, anywhere, anywhere,
        ],
        out_specs=(anywhere, anywhere),
        scratch_shapes=scratch,
        compiler_params=pltpu.CompilerParams(
            collective_id=0, has_side_effects=True, vmem_limit_bytes=67043328
        ),
        name="layer",
    )(
        sink_logits, queries, keys_values, out_weight, expert_tokens,
        norm_gain.reshape(1, width), routes.T, route_weights.T,
        gate_weight[0], up_weight[0], down_weight[0],
    )


def solution(mesh):
    return jax.shard_map(
        body,
        mesh=mesh,
        in_specs=(
            P("ep", "tp"),
            P("ep", "tp"),
            P(),
            P(),
            P(("ep", "tp"), None),
            P(),
            P(("ep", "tp"), None),
            P(("ep", "tp"), None),
            P("ep", None, "tp"),
            P("ep", None, "tp"),
            P("ep", "tp", None),
        ),
        out_specs=(P(("ep", "tp"), None), P(("ep", "tp"), None)),
        check_vma=False,
    )
```

```python
import functools

import jax
import jax.numpy as jnp
from jax import lax
from jax.experimental import pallas as pl
from jax.experimental.pallas import tpu as pltpu
from jax.sharding import PartitionSpec as P

HEAD_DIM = 64
WINDOW = 128
TOPK = 2
PLANES = 4
CHUNKS = 8
STEP_ROWS = 128
NEG_FILL = -1e30
MESH = pl.DeviceIdType.MESH


def div(a, b):
    return lax.div(a, jnp.int32(b))


def rem(a, b):
    return lax.rem(a, jnp.int32(b))


def layer_kernel(n, tp, cap, stride, *refs):
    (
        sink, q_hbm, kv_hbm, ow_hbm, tok_hbm, gain, routes, rweights, gate_hbm, up_hbm, down_hbm,
        mix_hbm, out_hbm,
        tok_v, norm_v, info, info_in, block_in, x_in, near_out, relay_out, sel,
        gate_s, up_s, down_s, hid, res, relay_in, merged, near_in, far_in,
        mix_hi, mix_lo, out_v,
        q_v, kv_s, vk_s, att, att_in, ow_v, mo_v,
        load_sem, w_recv, w_near_send, w_far_send, w_fwd_send,
        halo_recv, halo_send, info_recv, info_send, block_recv, block_send,
        near_recv, near_send, pack_recv, pack_send,
        back_near_recv, back_near_send, back_far_send, edge_send,
        relay_recv, merged_send, far_recv, att_recv, att_send, store_sem,
    ) = refs
    count, width = tok_v.shape
    wide = width // CHUNKS
    half_count = n // 2
    members = n // PLANES
    rows = half_count * stride
    group = members * stride
    side = tp // 2
    shard = gate_s.shape[2]
    seq_rows, q_width = q_v.shape
    heads = q_width // HEAD_DIM
    kv_heads = kv_s.shape[1] // (2 * HEAD_DIM)
    fan = heads // kv_heads
    own_count = seq_rows // tp

    e = lax.axis_index("ep")
    t = lax.axis_index("tp")
    plane = div(e, members)
    member = rem(e, members)
    half = div(e, half_count)
    local = rem(e, half_count)
    other = 1 - half
    is_relay = jnp.logical_or(plane == 1, plane == 2)
    own_relay_plane = 1 + half
    far_relay = (1 + other) * members + member
    tp_base = t - rem(t, side)
    tp_far = rem(t + side, tp)

    def near_tp(k):
        return tp_base + rem(t - tp_base + k, side)

    def near_ep(j):
        return rem(local + j, half_count)

    def far_plane(s):
        return 1 + other if s else 3 * other

    def far_source(s, k):
        return far_plane(s) * members + rem(member + k, members)

    def at(start, size):
        return pl.ds(pl.multiple_of(start, 16), size)

    def cols(c):
        return pl.ds(c * wide, wide)

    def remote(src, dst, send, recv, **where):
        return pltpu.make_async_remote_copy(
            src_ref=src, dst_ref=dst, send_sem=send, recv_sem=recv,
            device_id=where, device_id_type=MESH,
        )

    def arrived(ref, sem):
        pltpu.make_async_copy(ref, ref, sem).wait()

    kv_own = kv_s.at[pl.ds(WINDOW, seq_rows), :]
    loads = [
        pltpu.make_async_copy(tok_hbm, tok_v, load_sem.at[0]),
        pltpu.make_async_copy(kv_hbm, kv_own, load_sem.at[1]),
        pltpu.make_async_copy(q_hbm, q_v, load_sem.at[2]),
        pltpu.make_async_copy(ow_hbm, ow_v, load_sem.at[3]),
    ]
    items = 2 + CHUNKS

    def w_source(item):
        if item == 0:
            return gate_hbm
        if item == 1:
            return up_hbm
        return down_hbm.at[:, cols(item - 2)]

    def w_place(item, slot):
        if item == 0:
            return gate_s.at[slot]
        if item == 1:
            return up_s.at[slot]
        return down_s.at[item - 2, pl.ds(slot * shard, shard), :]

    own_weights = [
        pltpu.make_async_copy(w_source(i), w_place(i, 0), w_recv.at[i, 0]) for i in range(items)
    ]
    for copy in loads:
        copy.start()

    barrier = pltpu.get_barrier_semaphore()

    def greet(**where):
        pl.semaphore_signal(barrier, inc=1, device_id=where, device_id_type=MESH)

    for j in range(1, half_count):
        greet(ep=half * half_count + near_ep(j))
    for k in range(1, tp):
        greet(tp=rem(t + k, tp))

    @pl.when(e > 0)
    def greet_before():
        greet(ep=e - 1)

    @pl.when(e < n - 1)
    def greet_after():
        greet(ep=e + 1)

    @pl.when(is_relay)
    def greet_sources():
        for s in range(2):
            greet(ep=far_source(s, 0))

    @pl.when(jnp.logical_not(is_relay))
    def greet_relay():
        greet(ep=far_relay)

    def one(flag):
        return jnp.where(flag, 1, 0).astype(jnp.int32)

    pl.semaphore_wait(
        barrier, half_count - 1 + tp - 1 + one(e > 0) + one(e < n - 1) + 1 + one(is_relay)
    )

    halo_after = remote(
        kv_hbm.at[pl.ds(seq_rows - WINDOW, WINDOW), :], kv_s.at[pl.ds(0, WINDOW), :],
        halo_send.at[0], halo_recv.at[0], ep=rem(e + 1, n),
    )
    halo_before = remote(
        kv_hbm.at[pl.ds(0, WINDOW), :], kv_s.at[pl.ds(seq_rows + WINDOW, WINDOW), :],
        halo_send.at[1], halo_recv.at[1], ep=rem(e + n - 1, n),
    )

    @pl.when(e < n - 1)
    def send_after():
        halo_after.start()

    @pl.when(e > 0)
    def send_before():
        halo_before.start()

    w_far = [
        remote(w_source(i), w_place(i, side), w_far_send.at[i], w_recv.at[i, side], tp=tp_far)
        for i in range(items)
    ]
    w_near = [
        remote(
            w_source(i), w_place(i, (side - k) % side), w_near_send.at[i, k],
            w_recv.at[i, (side - k) % side], tp=near_tp(k),
        )
        for i in range(items)
        for k in range(1, side)
    ]
    w_fwd = {
        i: [
            remote(
                w_place(i, side), w_place(i, side + (side - k) % side), w_fwd_send.at[i, k],
                w_recv.at[i, side + (side - k) % side], tp=near_tp(k),
            )
            for k in range(1, side)
        ]
        for i in range(items)
    }
    for copy in w_far:
        copy.start()

    loads[0].wait()
    tokens = tok_v[...].astype(jnp.float32)
    centred = tokens - jnp.mean(tokens, -1, keepdims=True)
    scale = lax.rsqrt(jnp.mean(centred * centred, -1, keepdims=True) + 1e-06)
    normed = (centred * scale * gain[...]).astype(jnp.bfloat16)
    for c in range(CHUNKS):
        norm_v[c] = normed[:, c * wide : (c + 1) * wide]

    expert = lax.broadcasted_iota(jnp.int32, (n, count), 0)
    named = [expert == routes[k : k + 1, :] for k in range(TOPK)]
    member_of = functools.reduce(jnp.logical_or, named)
    earlier = lax.broadcasted_iota(jnp.int32, (count, count), 0) < lax.broadcasted_iota(
        jnp.int32, (count, count), 1
    )
    rank = jnp.dot(
        jnp.where(member_of, 1.0, 0.0).astype(jnp.bfloat16),
        jnp.where(earlier, 1.0, 0.0).astype(jnp.bfloat16),
        preferred_element_type=jnp.float32,
    )
    place = expert.astype(jnp.float32) * float(stride) + rank
    info[...] = jnp.zeros_like(info)
    for k in range(TOPK):
        info[k : k + 1, :] = jnp.sum(jnp.where(named[k], place, 0.0), 0, keepdims=True)
        info[TOPK + k : TOPK + k + 1, :] = rweights[k : k + 1, :]

    slot_of = one(is_relay)
    send_info = remote(info, info_in.at[slot_of], info_send, info_recv.at[slot_of], ep=far_relay)
    send_info.start()
    send_blocks = [
        remote(
            norm_v.at[c], block_in.at[slot_of, c], block_send.at[c], block_recv.at[slot_of, c],
            ep=far_relay,
        )
        for c in range(CHUNKS)
    ]
    for copy in send_blocks:
        copy.start()
    for copy in w_near:
        copy.start()
    for copy in own_weights:
        copy.start()

    base = half * rows

    def hits(table, k):
        slot = lax.broadcasted_iota(jnp.int32, (rows, count), 0) + base
        return slot.astype(jnp.float32) == table[k : k + 1, :]

    def pick(table):
        hit = functools.reduce(jnp.logical_or, [hits(table, k) for k in range(TOPK)])
        return jnp.where(hit, 1.0, 0.0).astype(jnp.bfloat16)

    def mixture(table, where):
        mix = sum(
            jnp.where(hits(table, k), table[TOPK + k : TOPK + k + 1, :], 0.0)
            for k in range(TOPK)
        ).T
        high = mix.astype(jnp.bfloat16)
        mix_hi[where] = high
        mix_lo[where] = (mix - high.astype(jnp.float32)).astype(jnp.bfloat16)

    own_table = info[...]
    sel[2] = pick(own_table)
    for c in range(CHUNKS):
        near_out[:, cols(c)] = jnp.dot(
            sel[2], norm_v[c], preferred_element_type=jnp.float32
        ).astype(jnp.bfloat16)
    own_rows = at(e * stride, stride)
    near_self = pltpu.make_async_copy(
        near_out.at[at(local * stride, stride), :], x_in.at[own_rows, :], near_recv
    )
    near_self.start()
    for j in range(1, half_count):
        remote(
            near_out.at[at(near_ep(j) * stride, stride), :], x_in.at[own_rows, :],
            near_send, near_recv, ep=half * half_count + near_ep(j),
        ).start()
    mixture(own_table, 2)

    def both_orders(first, size):
        for kv_head in range(kv_heads):
            lanes = slice(kv_head * 2 * HEAD_DIM, (kv_head + 1) * 2 * HEAD_DIM)
            both = kv_s[first : first + size, lanes]
            vk_s[first : first + size, lanes] = jnp.concatenate(
                [both[:, HEAD_DIM:], both[:, :HEAD_DIM]], 1
            )

    def got_halo():
        @pl.when(e == 0)
        def no_before():
            kv_s[0:WINDOW, :] = jnp.zeros((WINDOW, kv_s.shape[1]), kv_s.dtype)

        @pl.when(e > 0)
        def got_before():
            halo_after.wait_recv()

        @pl.when(e == n - 1)
        def no_after():
            kv_s[seq_rows + WINDOW : seq_rows + 2 * WINDOW, :] = jnp.zeros(
                (WINDOW, kv_s.shape[1]), kv_s.dtype
            )

        @pl.when(e < n - 1)
        def got_after():
            halo_before.wait_recv()

        both_orders(0, WINDOW)
        both_orders(seq_rows + WINDOW, WINDOW)

    loads[1].wait()
    both_orders(WINDOW, seq_rows)
    loads[2].wait()

    span = STEP_ROWS + 2 * WINDOW
    seq_total = seq_rows * n
    lower = lax.broadcasted_iota(jnp.int32, (STEP_ROWS, 2 * HEAD_DIM), 1) < HEAD_DIM

    def attend_step(start):
        start = pl.multiple_of(start, STEP_ROWS)
        row = lax.broadcasted_iota(jnp.int32, (STEP_ROWS, span), 0)
        column = lax.broadcasted_iota(jnp.int32, (STEP_ROWS, span), 1)
        key_pos = e * seq_rows + start - WINDOW + column
        allowed = (
            (column >= row) & (column <= row + 2 * WINDOW)
            & (key_pos >= 0) & (key_pos < seq_total)
        )
        for kv_head in range(kv_heads):
            lanes = slice(kv_head * 2 * HEAD_DIM, (kv_head + 1) * 2 * HEAD_DIM)
            kv = kv_s[pl.ds(start, span), lanes]
            vk = vk_s[pl.ds(start, span), lanes]
            for pair in range(fan // 2):
                head = kv_head * fan + 2 * pair
                places = slice(head * HEAD_DIM, (head + 2) * HEAD_DIM)
                q_pair = q_v[pl.ds(start, STEP_ROWS), places] * jnp.bfloat16(HEAD_DIM ** -0.5)
                results = []
                for odd in range(2):
                    q_one = jnp.where(lower != bool(odd), q_pair, jnp.zeros_like(q_pair))
                    key_side, value_side = (vk, kv) if odd else (kv, vk)
                    scores = lax.dot_general(
                        q_one, key_side, (((1,), (1,)), ((), ())),
                        preferred_element_type=jnp.float32,
                    )
                    scores = jnp.where(allowed, scores, NEG_FILL)
                    bound = sink[t * heads + head + odd]
                    top = jnp.maximum(jnp.max(scores, 1, keepdims=True), bound)
                    expo = jnp.exp(scores - top)
                    denom = jnp.sum(expo, 1, keepdims=True) + jnp.exp(bound - top)
                    value = jnp.dot(
                        expo.astype(jnp.bfloat16), value_side, preferred_element_type=jnp.float32
                    )
                    results.append(value / denom)
                att[pl.ds(start, STEP_ROWS), places] = jnp.where(
                    lower, results[0], results[1]
                ).astype(jnp.bfloat16)

    def attend_inner(first, last):
        def step(i, carry):
            attend_step(i * STEP_ROWS)
            return carry

        lax.fori_loop(first, last, step, 0)

    def attend_edges():
        def step(i, carry):
            attend_step(i * (seq_rows - STEP_ROWS))
            return carry

        lax.fori_loop(0, 2, step, 0)
        for k in range(tp):
            owner = rem(t + k, tp)
            block = att.at[at(owner * own_count, own_count), :]
            if k:
                remote(block, att_in.at[t], att_send.at[k], att_recv.at[k], tp=owner).start()
            else:
                pltpu.make_async_copy(block, att_in.at[t], att_recv.at[0]).start()

    def relay_tables(s):
        arrived(info_in.at[s], info_recv.at[s])
        table = info_in[s]
        sel[s] = pick(table)
        mixture(table, s)

    def relay_forward(s, c):
        arrived(block_in.at[s, c], block_recv.at[s, c])
        relay_out[s, c] = jnp.dot(
            sel[s], block_in[s, c], preferred_element_type=jnp.float32
        ).astype(jnp.bfloat16)
        landing = x_in.at[at(far_source(s, 0) * stride, stride), cols(c)]
        for j in range(1, half_count):
            remote(
                relay_out.at[s, c, at(near_ep(j) * stride, stride), :], landing,
                pack_send.at[s, c], pack_recv.at[s], ep=half * half_count + near_ep(j),
            ).start()
        pltpu.make_async_copy(
            relay_out.at[s, c, at(local * stride, stride), :], landing, pack_recv.at[s]
        ).start()

    def on_relay(task, *args):
        pl.when(is_relay)(lambda: task(*args))

    def off_relay(task, *args):
        pl.when(jnp.logical_not(is_relay))(lambda: task(*args))

    def forward_weights(i):
        arrived(w_place(i, side), w_recv.at[i, side])
        for copy in w_fwd[i]:
            copy.start()

    def hidden_rows(start, size, slot):
        x = x_in[at(start, size), :]
        gate = jnp.dot(x, gate_s[slot], preferred_element_type=jnp.float32)
        up = jnp.dot(x, up_s[slot], preferred_element_type=jnp.float32)
        hid[at(start, size), pl.ds(slot * shard, shard)] = (
            gate / (1.0 + jnp.exp(-gate)) * up
        ).astype(jnp.bfloat16)

    def got_weights(item, slot):
        arrived(w_place(item, slot), w_recv.at[item, slot])

    def project():
        arrived(att_in.at[0], att_recv.at[0])
        for k in range(1, tp):
            arrived(att_in.at[0], att_recv.at[k])
        loads[3].wait()
        total = jnp.zeros(mo_v.shape, jnp.float32)
        for c in range(CHUNKS):
            total = sum(
                jnp.dot(
                    att_in[k], ow_v[k * q_width : (k + 1) * q_width, cols(c)],
                    preferred_element_type=jnp.float32,
                )
                for k in range(tp)
            )
            mo_v[:, cols(c)] = total.astype(jnp.bfloat16)
        pltpu.make_async_copy(mo_v, mix_hbm, store_sem.at[CHUNKS]).start()

    def results(s, c):
        first = far_plane(s) * group
        res[c, at(first, group), :] = jnp.dot(
            hid[at(first, group), :], down_s[c], preferred_element_type=jnp.float32
        ).astype(jnp.bfloat16)
        landing = relay_in.at[s, c, at(local * stride, stride), :]
        for k in range(members):
            block = res.at[c, at(far_source(s, k) * stride, stride), :]
            if k:
                remote(
                    block, landing, back_far_send.at[s, c], relay_recv.at[s, c],
                    ep=plane * members + rem(member + k, members),
                ).start()
            else:
                pltpu.make_async_copy(block, landing, relay_recv.at[s, c]).start()

    def edge_block(s, c):
        return relay_in.at[s, c, at(rem(plane, 2) * group, group), :]

    def edge_forward(s, c):
        arrived(edge_block(s, c), relay_recv.at[s, c])
        remote(
            edge_block(s, c), edge_block(s, c), edge_send.at[s, c], relay_recv.at[s, c],
            ep=own_relay_plane * members + member,
        ).start()

    def near_results(c):
        first = half * rows
        res[c, at(first, rows), :] = jnp.dot(
            hid[at(first, rows), :], down_s[c], preferred_element_type=jnp.float32
        ).astype(jnp.bfloat16)
        landing = near_in.at[c, at(local * stride, stride), :]
        for j in range(1, half_count):
            target = half * half_count + near_ep(j)
            remote(
                res.at[c, at(target * stride, stride), :], landing,
                back_near_send.at[c], back_near_recv.at[c], ep=target,
            ).start()
        pltpu.make_async_copy(
            res.at[c, own_rows, :], landing, back_near_recv.at[c]
        ).start()

    def mixed(where, values):
        return jnp.dot(
            mix_hi[where], values, preferred_element_type=jnp.float32
        ) + jnp.dot(mix_lo[where], values, preferred_element_type=jnp.float32)

    def relay_merge(s, c):
        arrived(relay_in.at[s, c], relay_recv.at[s, c])
        merged[s, c] = mixed(s, relay_in[s, c]).astype(jnp.bfloat16)
        remote(
            merged.at[s, c], far_in.at[c], merged_send.at[s, c], far_recv.at[c],
            ep=far_source(s, 0),
        ).start()

    def finish(c):
        arrived(near_in.at[c], back_near_recv.at[c])
        total = mixed(2, near_in[c])
        arrived(far_in.at[c], far_recv.at[c])
        out_v[:, cols(c)] = (total + far_in[c].astype(jnp.float32)).astype(jnp.bfloat16)
        pltpu.make_async_copy(
            out_v.at[:, cols(c)], out_hbm.at[:, cols(c)], store_sem.at[c]
        ).start()

    on_relay(relay_tables, 0)
    steps = seq_rows // STEP_ROWS
    quarter = max(steps // 4, 1)
    bounds = [1] + [min(1 + quarter * (i + 1), steps - 1) for i in range(4)]
    plan = [range(0, 2), range(2, 4), range(4, 6), range(6, CHUNKS)]
    for i in range(4):
        attend_inner(bounds[i], bounds[i + 1])
        for c in plan[i]:
            on_relay(relay_forward, 0, c)
    forward_weights(0)
    on_relay(relay_tables, 1)
    on_relay(relay_forward, 1, 0)
    got_halo()
    attend_edges()
    for c in range(1, 4):
        on_relay(relay_forward, 1, c)
    for slot in range(side):
        for item in range(2):
            got_weights(item, slot)
    first_rows, last_rows = far_plane(0) * group, far_plane(1) * group
    arrived(x_in.at[at(first_rows, group), :], pack_recv.at[0])
    for slot in range(side):
        hidden_rows(first_rows, group, slot)
    for c in range(4, 6):
        on_relay(relay_forward, 1, c)
    arrived(x_in.at[at(half * rows, rows), :], near_recv)
    for slot in range(side):
        hidden_rows(half * rows, rows, slot)
    on_relay(relay_forward, 1, 6)
    forward_weights(1)
    hidden_rows(first_rows, group, side)
    for c in range(7, CHUNKS):
        on_relay(relay_forward, 1, c)
    hidden_rows(half * rows, rows, side)
    for slot in range(side + 1, tp):
        for item in range(2):
            got_weights(item, slot)
        hidden_rows(first_rows, group, slot)

    def got_down(c):
        for slot in range(tp):
            if slot != side:
                got_weights(2 + c, slot)

    forward_weights(2)
    for slot in range(side + 1, tp):
        hidden_rows(half * rows, rows, slot)
    got_down(0)
    results(0, 0)
    on_relay(near_results, 0)
    forward_weights(3)
    got_down(1)
    results(0, 1)
    on_relay(near_results, 1)
    edges = [(0, 0), (0, 1), (1, 0), (1, 1)] + [
        (s, c) for c in range(2, CHUNKS) for s in range(2)
    ]
    off_relay(edge_forward, *edges.pop(0))
    arrived(x_in.at[at(last_rows, group), :], pack_recv.at[1])
    for slot in range(tp):
        hidden_rows(last_rows, group, slot)
    results(1, 0)
    results(1, 1)
    off_relay(edge_forward, *edges.pop(0))
    merges = [(0, 0), (0, 1), (1, 0), (1, 1)] + [
        (s, c) for c in range(2, CHUNKS) for s in range(2)
    ]
    due = {3: 3, 4: 1, 5: 1, 6: 2, 7: 1}
    for c in range(2, CHUNKS):
        forward_weights(2 + c)
        got_down(c)
        results(0, c)
        results(1, c)
        for _ in range(2):
            off_relay(edge_forward, *edges.pop(0))
        on_relay(near_results, c)
        for _ in range(due.get(c, 0)):
            on_relay(relay_merge, *merges.pop(0))
    for item in edges:
        off_relay(edge_forward, *item)
    for c in range(0, CHUNKS, 2):
        off_relay(near_results, c)
        off_relay(near_results, c + 1)
        on_relay(relay_merge, *merges.pop(0))
    project()
    for item in merges:
        on_relay(relay_merge, *item)
    for c in range(CHUNKS):
        finish(c)

    for c in range(CHUNKS):
        pltpu.make_async_copy(
            out_v.at[:, cols(c)], out_hbm.at[:, cols(c)], store_sem.at[c]
        ).wait()
    pltpu.make_async_copy(mo_v, mix_hbm, store_sem.at[CHUNKS]).wait()

    def sent(ref, sem):
        pltpu.make_async_copy(ref, ref, sem).wait()

    @pl.when(e < n - 1)
    def sent_after():
        halo_after.wait_send()

    @pl.when(e > 0)
    def sent_before():
        halo_before.wait_send()

    for copy in w_far + w_near + [c for i in range(items) for c in w_fwd[i]]:
        copy.wait_send()
    send_info.wait_send()
    for copy in send_blocks:
        copy.wait_send()
    others = half_count - 1
    sent(near_out.at[pl.ds(0, others * stride), :], near_send)
    for k in range(1, tp):
        sent(att_in.at[0], att_send.at[k])
    for c in range(CHUNKS):
        sent(near_in.at[c, pl.ds(0, others * stride), :], back_near_send.at[c])
        for s in range(2):
            sent(res.at[c, pl.ds(0, (members - 1) * stride), :], back_far_send.at[s, c])

        @pl.when(is_relay)
        def sent_relay():
            for s in range(2):
                sent(relay_out.at[s, c, pl.ds(0, others * stride), :], pack_send.at[s, c])
                sent(merged.at[s, c], merged_send.at[s, c])

        @pl.when(jnp.logical_not(is_relay))
        def sent_own():
            for s in range(2):
                sent(relay_in.at[s, c, pl.ds(0, group), :], edge_send.at[s, c])


def body(
    queries,
    keys_values,
    sink_logits,
    out_weight,
    expert_tokens,
    norm_gain,
    routes,
    route_weights,
    gate_weight,
    up_weight,
    down_weight,
):
    n, tp = lax.axis_size("ep"), lax.axis_size("tp")
    count, width = expert_tokens.shape
    cap = 3 * count * TOPK // (2 * n)
    stride = -(-cap // 16) * 16
    rows = n // 2 * stride
    wide = width // CHUNKS
    shard = gate_weight.shape[2]
    seq_rows, q_width = queries.shape
    kv_width = keys_values.shape[1]
    items = 2 + CHUNKS
    side = tp // 2
    bf16, f32 = jnp.bfloat16, jnp.float32
    dma = pltpu.SemaphoreType.DMA

    def vmem(*shape, dtype=bf16):
        return pltpu.VMEM(shape, dtype)

    scratch = [
        vmem(count, width),
        vmem(CHUNKS, count, wide),
        vmem(8, count, dtype=f32),
        vmem(2, 8, count, dtype=f32),
        vmem(2, CHUNKS, count, wide),
        vmem(n * stride, width),
        vmem(rows, width),
        vmem(2, CHUNKS, rows, wide),
        vmem(3, rows, count),
        vmem(tp, width, shard),
        vmem(tp, width, shard),
        vmem(CHUNKS, tp * shard, wide),
        vmem(n * stride, tp * shard),
        vmem(CHUNKS, n * stride, wide),
        vmem(2, CHUNKS, rows, wide),
        vmem(2, CHUNKS, count, wide),
        vmem(CHUNKS, rows, wide),
        vmem(CHUNKS, count, wide),
        vmem(3, count, rows),
        vmem(3, count, rows),
        vmem(count, width),
        vmem(seq_rows, q_width),
        vmem(seq_rows + 2 * WINDOW, kv_width),
        vmem(seq_rows + 2 * WINDOW, kv_width),
        vmem(seq_rows, q_width),
        vmem(tp, seq_rows // tp, q_width),
        vmem(*out_weight.shape),
        vmem(seq_rows // tp, width),
        dma((4,)),
        dma((items, tp)),
        dma((items, side)),
        dma((items,)),
        dma((items, side)),
        dma((2,)),
        dma((2,)),
        dma((2,)),
        dma,
        dma((2, CHUNKS)),
        dma((CHUNKS,)),
        dma,
        dma,
        dma((2,)),
        dma((2, CHUNKS)),
        dma((CHUNKS,)),
        dma((CHUNKS,)),
        dma((2, CHUNKS)),
        dma((2, CHUNKS)),
        dma((2, CHUNKS)),
        dma((2, CHUNKS)),
        dma((CHUNKS,)),
        dma((tp,)),
        dma((tp,)),
        dma((CHUNKS + 1,)),
    ]
    anywhere = pl.BlockSpec(memory_space=pl.ANY)
    small = pl.BlockSpec(memory_space=pltpu.VMEM)
    return pl.pallas_call(
        functools.partial(layer_kernel, n, tp, cap, stride),
        out_shape=(
            jax.ShapeDtypeStruct((seq_rows // tp, width), bf16),
            jax.ShapeDtypeStruct((count, width), bf16),
        ),
        in_specs=[
            pl.BlockSpec(memory_space=pltpu.SMEM), anywhere, anywhere, anywhere, anywhere,
            small, small, small, anywhere, anywhere, anywhere,
        ],
        out_specs=(anywhere, anywhere),
        scratch_shapes=scratch,
        compiler_params=pltpu.CompilerParams(
            collective_id=0, has_side_effects=True, vmem_limit_bytes=67043328
        ),
        name="layer",
    )(
        sink_logits, queries, keys_values, out_weight, expert_tokens,
        norm_gain.reshape(1, width), routes.T, route_weights.T,
        gate_weight[0], up_weight[0], down_weight[0],
    )


def solution(mesh):
    return jax.shard_map(
        body,
        mesh=mesh,
        in_specs=(
            P("ep", "tp"),
            P("ep", "tp"),
            P(),
            P(),
            P(("ep", "tp"), None),
            P(),
            P(("ep", "tp"), None),
            P(("ep", "tp"), None),
            P("ep", None, "tp"),
            P("ep", None, "tp"),
            P("ep", "tp", None),
        ),
        out_specs=(P(("ep", "tp"), None), P(("ep", "tp"), None)),
        check_vma=False,
    )
```

```python
import functools

import jax
import jax.numpy as jnp
from jax import lax
from jax.experimental import pallas as pl
from jax.experimental.pallas import tpu as pltpu
from jax.sharding import PartitionSpec as P

HEAD_DIM = 64
WINDOW = 128
TOPK = 2
PLANES = 4
CHUNKS = 8
STEP_ROWS = 128
NEG_FILL = -1e30
MESH = pl.DeviceIdType.MESH


def div(a, b):
    return lax.div(a, jnp.int32(b))


def rem(a, b):
    return lax.rem(a, jnp.int32(b))


def layer_kernel(n, tp, cap, stride, *refs):
    (
        sink, q_hbm, kv_hbm, ow_hbm, tok_hbm, gain, routes, rweights, gate_hbm, up_hbm, down_hbm,
        mo_v, out_v,
        tok_v, norm_v, info, info_in, block_in, x_in, near_out, relay_out, sel,
        gate_s, up_s, down_s, hid, res, relay_in, merged, near_in, far_in,
        mix_hi, mix_lo,
        q_v, kv_s, vk_s, att, att_in, ow_v,
        load_sem, w_recv, w_near_send, w_far_send, w_fwd_send,
        halo_recv, halo_send, info_recv, info_send, block_recv, block_send,
        near_recv, near_send, pack_recv, pack_send,
        back_near_recv, back_near_send, back_far_send, edge_send,
        relay_recv, merged_send, far_recv, att_recv, att_send,
    ) = refs
    count, width = tok_v.shape
    wide = width // CHUNKS
    half_count = n // 2
    members = n // PLANES
    rows = half_count * stride
    group = members * stride
    side = tp // 2
    shard = gate_s.shape[2]
    seq_rows, q_width = q_v.shape
    heads = q_width // HEAD_DIM
    kv_heads = kv_s.shape[1] // (2 * HEAD_DIM)
    fan = heads // kv_heads
    own_count = seq_rows // tp

    e = lax.axis_index("ep")
    t = lax.axis_index("tp")
    plane = div(e, members)
    member = rem(e, members)
    half = div(e, half_count)
    local = rem(e, half_count)
    other = 1 - half
    is_relay = jnp.logical_or(plane == 1, plane == 2)
    own_relay_plane = 1 + half
    far_relay = (1 + other) * members + member
    tp_base = t - rem(t, side)
    tp_far = rem(t + side, tp)

    def near_tp(k):
        return tp_base + rem(t - tp_base + k, side)

    def near_ep(j):
        return rem(local + j, half_count)

    def far_plane(s):
        return 1 + other if s else 3 * other

    def far_source(s, k):
        return far_plane(s) * members + rem(member + k, members)

    def at(start, size):
        return pl.ds(pl.multiple_of(start, 16), size)

    def cols(c):
        return pl.ds(c * wide, wide)

    def remote(src, dst, send, recv, **where):
        return pltpu.make_async_remote_copy(
            src_ref=src, dst_ref=dst, send_sem=send, recv_sem=recv,
            device_id=where, device_id_type=MESH,
        )

    def arrived(ref, sem):
        pltpu.make_async_copy(ref, ref, sem).wait()

    kv_own = kv_s.at[pl.ds(WINDOW, seq_rows), :]
    loads = [
        pltpu.make_async_copy(tok_hbm, tok_v, load_sem.at[0]),
        pltpu.make_async_copy(kv_hbm, kv_own, load_sem.at[1]),
        pltpu.make_async_copy(q_hbm, q_v, load_sem.at[2]),
        pltpu.make_async_copy(ow_hbm, ow_v, load_sem.at[3]),
    ]
    items = 2 + CHUNKS

    def w_source(item):
        if item == 0:
            return gate_hbm
        if item == 1:
            return up_hbm
        return down_hbm.at[:, cols(item - 2)]

    def w_place(item, slot):
        if item == 0:
            return gate_s.at[slot]
        if item == 1:
            return up_s.at[slot]
        return down_s.at[item - 2, pl.ds(slot * shard, shard), :]

    own_weights = [
        pltpu.make_async_copy(w_source(i), w_place(i, 0), w_recv.at[i, 0]) for i in range(items)
    ]
    for copy in loads:
        copy.start()

    barrier = pltpu.get_barrier_semaphore()

    def greet(**where):
        pl.semaphore_signal(barrier, inc=1, device_id=where, device_id_type=MESH)

    for j in range(1, half_count):
        greet(ep=half * half_count + near_ep(j))
    for k in range(1, tp):
        greet(tp=rem(t + k, tp))

    @pl.when(e > 0)
    def greet_before():
        greet(ep=e - 1)

    @pl.when(e < n - 1)
    def greet_after():
        greet(ep=e + 1)

    @pl.when(is_relay)
    def greet_sources():
        for s in range(2):
            greet(ep=far_source(s, 0))

    @pl.when(jnp.logical_not(is_relay))
    def greet_relay():
        greet(ep=far_relay)

    def one(flag):
        return jnp.where(flag, 1, 0).astype(jnp.int32)

    pl.semaphore_wait(
        barrier, half_count - 1 + tp - 1 + one(e > 0) + one(e < n - 1) + 1 + one(is_relay)
    )

    halo_after = remote(
        kv_hbm.at[pl.ds(seq_rows - WINDOW, WINDOW), :], kv_s.at[pl.ds(0, WINDOW), :],
        halo_send.at[0], halo_recv.at[0], ep=rem(e + 1, n),
    )
    halo_before = remote(
        kv_hbm.at[pl.ds(0, WINDOW), :], kv_s.at[pl.ds(seq_rows + WINDOW, WINDOW), :],
        halo_send.at[1], halo_recv.at[1], ep=rem(e + n - 1, n),
    )

    @pl.when(e < n - 1)
    def send_after():
        halo_after.start()

    @pl.when(e > 0)
    def send_before():
        halo_before.start()

    w_far = [
        remote(w_source(i), w_place(i, side), w_far_send.at[i], w_recv.at[i, side], tp=tp_far)
        for i in range(items)
    ]
    w_near = [
        remote(
            w_source(i), w_place(i, (side - k) % side), w_near_send.at[i, k],
            w_recv.at[i, (side - k) % side], tp=near_tp(k),
        )
        for i in range(items)
        for k in range(1, side)
    ]
    w_fwd = {
        i: [
            remote(
                w_place(i, side), w_place(i, side + (side - k) % side), w_fwd_send.at[i, k],
                w_recv.at[i, side + (side - k) % side], tp=near_tp(k),
            )
            for k in range(1, side)
        ]
        for i in range(items)
    }
    for copy in w_far:
        copy.start()

    loads[0].wait()
    tokens = tok_v[...].astype(jnp.float32)
    centred = tokens - jnp.mean(tokens, -1, keepdims=True)
    scale = lax.rsqrt(jnp.mean(centred * centred, -1, keepdims=True) + 1e-06)
    normed = (centred * scale * gain[...]).astype(jnp.bfloat16)
    for c in range(CHUNKS):
        norm_v[c] = normed[:, c * wide : (c + 1) * wide]

    expert = lax.broadcasted_iota(jnp.int32, (n, count), 0)
    named = [expert == routes[k : k + 1, :] for k in range(TOPK)]
    member_of = functools.reduce(jnp.logical_or, named)
    earlier = lax.broadcasted_iota(jnp.int32, (count, count), 0) < lax.broadcasted_iota(
        jnp.int32, (count, count), 1
    )
    rank = jnp.dot(
        jnp.where(member_of, 1.0, 0.0).astype(jnp.bfloat16),
        jnp.where(earlier, 1.0, 0.0).astype(jnp.bfloat16),
        preferred_element_type=jnp.float32,
    )
    place = expert.astype(jnp.float32) * float(stride) + rank
    info[...] = jnp.zeros_like(info)
    for k in range(TOPK):
        info[k : k + 1, :] = jnp.sum(jnp.where(named[k], place, 0.0), 0, keepdims=True)
        info[TOPK + k : TOPK + k + 1, :] = rweights[k : k + 1, :]

    slot_of = one(is_relay)
    send_info = remote(info, info_in.at[slot_of], info_send, info_recv.at[slot_of], ep=far_relay)
    send_info.start()
    send_blocks = [
        remote(
            norm_v.at[c], block_in.at[slot_of, c], block_send.at[c], block_recv.at[slot_of, c],
            ep=far_relay,
        )
        for c in range(CHUNKS)
    ]
    for copy in send_blocks:
        copy.start()
    for copy in w_near:
        copy.start()
    for copy in own_weights:
        copy.start()

    base = half * rows

    def hits(table, k):
        slot = lax.broadcasted_iota(jnp.int32, (rows, count), 0) + base
        return slot.astype(jnp.float32) == table[k : k + 1, :]

    def pick(table):
        hit = functools.reduce(jnp.logical_or, [hits(table, k) for k in range(TOPK)])
        return jnp.where(hit, 1.0, 0.0).astype(jnp.bfloat16)

    def mixture(table, where):
        mix = sum(
            jnp.where(hits(table, k), table[TOPK + k : TOPK + k + 1, :], 0.0)
            for k in range(TOPK)
        ).T
        high = mix.astype(jnp.bfloat16)
        mix_hi[where] = high
        mix_lo[where] = (mix - high.astype(jnp.float32)).astype(jnp.bfloat16)

    own_table = info[...]
    sel[2] = pick(own_table)
    for c in range(CHUNKS):
        near_out[:, cols(c)] = jnp.dot(
            sel[2], norm_v[c], preferred_element_type=jnp.float32
        ).astype(jnp.bfloat16)
    own_rows = at(e * stride, stride)
    near_self = pltpu.make_async_copy(
        near_out.at[at(local * stride, stride), :], x_in.at[own_rows, :], near_recv
    )
    near_self.start()
    for j in range(1, half_count):
        remote(
            near_out.at[at(near_ep(j) * stride, stride), :], x_in.at[own_rows, :],
            near_send, near_recv, ep=half * half_count + near_ep(j),
        ).start()
    mixture(own_table, 2)

    def both_orders(first, size):
        for kv_head in range(kv_heads):
            lanes = slice(kv_head * 2 * HEAD_DIM, (kv_head + 1) * 2 * HEAD_DIM)
            both = kv_s[first : first + size, lanes]
            vk_s[first : first + size, lanes] = jnp.concatenate(
                [both[:, HEAD_DIM:], both[:, :HEAD_DIM]], 1
            )

    def got_halo():
        @pl.when(e == 0)
        def no_before():
            kv_s[0:WINDOW, :] = jnp.zeros((WINDOW, kv_s.shape[1]), kv_s.dtype)

        @pl.when(e > 0)
        def got_before():
            halo_after.wait_recv()

        @pl.when(e == n - 1)
        def no_after():
            kv_s[seq_rows + WINDOW : seq_rows + 2 * WINDOW, :] = jnp.zeros(
                (WINDOW, kv_s.shape[1]), kv_s.dtype
            )

        @pl.when(e < n - 1)
        def got_after():
            halo_before.wait_recv()

        both_orders(0, WINDOW)
        both_orders(seq_rows + WINDOW, WINDOW)

    loads[1].wait()
    both_orders(WINDOW, seq_rows)
    loads[2].wait()

    span = STEP_ROWS + 2 * WINDOW
    seq_total = seq_rows * n
    lower = lax.broadcasted_iota(jnp.int32, (STEP_ROWS, 2 * HEAD_DIM), 1) < HEAD_DIM

    def attend_step(start):
        start = pl.multiple_of(start, STEP_ROWS)
        row = lax.broadcasted_iota(jnp.int32, (STEP_ROWS, span), 0)
        column = lax.broadcasted_iota(jnp.int32, (STEP_ROWS, span), 1)
        key_pos = e * seq_rows + start - WINDOW + column
        allowed = (
            (column >= row) & (column <= row + 2 * WINDOW)
            & (key_pos >= 0) & (key_pos < seq_total)
        )
        for kv_head in range(kv_heads):
            lanes = slice(kv_head * 2 * HEAD_DIM, (kv_head + 1) * 2 * HEAD_DIM)
            kv = kv_s[pl.ds(start, span), lanes]
            vk = vk_s[pl.ds(start, span), lanes]
            for pair in range(fan // 2):
                head = kv_head * fan + 2 * pair
                places = slice(head * HEAD_DIM, (head + 2) * HEAD_DIM)
                q_pair = q_v[pl.ds(start, STEP_ROWS), places] * jnp.bfloat16(HEAD_DIM ** -0.5)
                results = []
                for odd in range(2):
                    q_one = jnp.where(lower != bool(odd), q_pair, jnp.zeros_like(q_pair))
                    key_side, value_side = (vk, kv) if odd else (kv, vk)
                    scores = lax.dot_general(
                        q_one, key_side, (((1,), (1,)), ((), ())),
                        preferred_element_type=jnp.float32,
                    )
                    scores = jnp.where(allowed, scores, NEG_FILL)
                    bound = sink[t * heads + head + odd]
                    top = jnp.maximum(jnp.max(scores, 1, keepdims=True), bound)
                    expo = jnp.exp(scores - top)
                    denom = jnp.sum(expo, 1, keepdims=True) + jnp.exp(bound - top)
                    value = jnp.dot(
                        expo.astype(jnp.bfloat16), value_side, preferred_element_type=jnp.float32
                    )
                    results.append(value / denom)
                att[pl.ds(start, STEP_ROWS), places] = jnp.where(
                    lower, results[0], results[1]
                ).astype(jnp.bfloat16)

    def attend_inner(first, last):
        def step(i, carry):
            attend_step(i * STEP_ROWS)
            return carry

        lax.fori_loop(first, last, step, 0)

    def attend_edges():
        def step(i, carry):
            attend_step(i * (seq_rows - STEP_ROWS))
            return carry

        lax.fori_loop(0, 2, step, 0)
        for k in range(tp):
            owner = rem(t + k, tp)
            block = att.at[at(owner * own_count, own_count), :]
            if k:
                remote(block, att_in.at[t], att_send.at[k], att_recv.at[k], tp=owner).start()
            else:
                pltpu.make_async_copy(block, att_in.at[t], att_recv.at[0]).start()

    def relay_tables(s):
        arrived(info_in.at[s], info_recv.at[s])
        table = info_in[s]
        sel[s] = pick(table)
        mixture(table, s)

    def relay_forward(s, c):
        arrived(block_in.at[s, c], block_recv.at[s, c])
        relay_out[s, c] = jnp.dot(
            sel[s], block_in[s, c], preferred_element_type=jnp.float32
        ).astype(jnp.bfloat16)
        landing = x_in.at[at(far_source(s, 0) * stride, stride), cols(c)]
        for j in range(1, half_count):
            remote(
                relay_out.at[s, c, at(near_ep(j) * stride, stride), :], landing,
                pack_send.at[s, c], pack_recv.at[s], ep=half * half_count + near_ep(j),
            ).start()
        pltpu.make_async_copy(
            relay_out.at[s, c, at(local * stride, stride), :], landing, pack_recv.at[s]
        ).start()

    def on_relay(task, *args):
        pl.when(is_relay)(lambda: task(*args))

    def off_relay(task, *args):
        pl.when(jnp.logical_not(is_relay))(lambda: task(*args))

    def forward_weights(i):
        arrived(w_place(i, side), w_recv.at[i, side])
        for copy in w_fwd[i]:
            copy.start()

    def hidden_rows(start, size, slot):
        x = x_in[at(start, size), :]
        gate = jnp.dot(x, gate_s[slot], preferred_element_type=jnp.float32)
        up = jnp.dot(x, up_s[slot], preferred_element_type=jnp.float32)
        hid[at(start, size), pl.ds(slot * shard, shard)] = (
            gate / (1.0 + jnp.exp(-gate)) * up
        ).astype(jnp.bfloat16)

    def got_weights(item, slot):
        arrived(w_place(item, slot), w_recv.at[item, slot])

    def project():
        arrived(att_in.at[0], att_recv.at[0])
        for k in range(1, tp):
            arrived(att_in.at[0], att_recv.at[k])
        loads[3].wait()
        total = jnp.zeros(mo_v.shape, jnp.float32)
        for c in range(CHUNKS):
            total = sum(
                jnp.dot(
                    att_in[k], ow_v[k * q_width : (k + 1) * q_width, cols(c)],
                    preferred_element_type=jnp.float32,
                )
                for k in range(tp)
            )
            mo_v[:, cols(c)] = total.astype(jnp.bfloat16)

    def results(s, c):
        first = far_plane(s) * group
        res[c, at(first, group), :] = jnp.dot(
            hid[at(first, group), :], down_s[c], preferred_element_type=jnp.float32
        ).astype(jnp.bfloat16)
        landing = relay_in.at[s, c, at(local * stride, stride), :]
        for k in range(members):
            block = res.at[c, at(far_source(s, k) * stride, stride), :]
            if k:
                remote(
                    block, landing, back_far_send.at[s, c], relay_recv.at[s, c],
                    ep=plane * members + rem(member + k, members),
                ).start()
            else:
                pltpu.make_async_copy(block, landing, relay_recv.at[s, c]).start()

    def edge_block(s, c):
        return relay_in.at[s, c, at(rem(plane, 2) * group, group), :]

    def edge_forward(s, c):
        arrived(edge_block(s, c), relay_recv.at[s, c])
        remote(
            edge_block(s, c), edge_block(s, c), edge_send.at[s, c], relay_recv.at[s, c],
            ep=own_relay_plane * members + member,
        ).start()

    def near_results(c):
        first = half * rows
        res[c, at(first, rows), :] = jnp.dot(
            hid[at(first, rows), :], down_s[c], preferred_element_type=jnp.float32
        ).astype(jnp.bfloat16)
        landing = near_in.at[c, at(local * stride, stride), :]
        for j in range(1, half_count):
            target = half * half_count + near_ep(j)
            remote(
                res.at[c, at(target * stride, stride), :], landing,
                back_near_send.at[c], back_near_recv.at[c], ep=target,
            ).start()
        pltpu.make_async_copy(
            res.at[c, own_rows, :], landing, back_near_recv.at[c]
        ).start()

    def mixed(where, values):
        return jnp.dot(
            mix_hi[where], values, preferred_element_type=jnp.float32
        ) + jnp.dot(mix_lo[where], values, preferred_element_type=jnp.float32)

    def relay_merge(s, c):
        arrived(relay_in.at[s, c], relay_recv.at[s, c])
        merged[s, c] = mixed(s, relay_in[s, c]).astype(jnp.bfloat16)
        remote(
            merged.at[s, c], far_in.at[c], merged_send.at[s, c], far_recv.at[c],
            ep=far_source(s, 0),
        ).start()

    def finish(c):
        arrived(near_in.at[c], back_near_recv.at[c])
        total = mixed(2, near_in[c])
        arrived(far_in.at[c], far_recv.at[c])
        out_v[:, cols(c)] = (total + far_in[c].astype(jnp.float32)).astype(jnp.bfloat16)

    on_relay(relay_tables, 0)
    steps = seq_rows // STEP_ROWS
    quarter = max(steps // 4, 1)
    bounds = [1] + [min(1 + quarter * (i + 1), steps - 1) for i in range(4)]
    plan = [range(0, 2), range(2, 4), range(4, 6), range(6, CHUNKS)]
    for i in range(4):
        attend_inner(bounds[i], bounds[i + 1])
        for c in plan[i]:
            on_relay(relay_forward, 0, c)
    forward_weights(0)
    on_relay(relay_tables, 1)
    on_relay(relay_forward, 1, 0)
    got_halo()
    attend_edges()
    for c in range(1, 4):
        on_relay(relay_forward, 1, c)
    for slot in range(side):
        for item in range(2):
            got_weights(item, slot)
    first_rows, last_rows = far_plane(0) * group, far_plane(1) * group
    arrived(x_in.at[at(first_rows, group), :], pack_recv.at[0])
    for slot in range(side):
        hidden_rows(first_rows, group, slot)
    for c in range(4, 6):
        on_relay(relay_forward, 1, c)
    arrived(x_in.at[at(half * rows, rows), :], near_recv)
    for slot in range(side):
        hidden_rows(half * rows, rows, slot)
    on_relay(relay_forward, 1, 6)
    forward_weights(1)
    hidden_rows(first_rows, group, side)
    for c in range(7, CHUNKS):
        on_relay(relay_forward, 1, c)
    hidden_rows(half * rows, rows, side)
    for slot in range(side + 1, tp):
        for item in range(2):
            got_weights(item, slot)
        hidden_rows(first_rows, group, slot)

    def got_down(c):
        for slot in range(tp):
            if slot != side:
                got_weights(2 + c, slot)

    forward_weights(2)
    for slot in range(side + 1, tp):
        hidden_rows(half * rows, rows, slot)
    got_down(0)
    results(0, 0)
    on_relay(near_results, 0)
    forward_weights(3)
    got_down(1)
    results(0, 1)
    on_relay(near_results, 1)
    edges = [(0, 0), (0, 1), (1, 0), (1, 1)] + [
        (s, c) for c in range(2, CHUNKS) for s in range(2)
    ]
    off_relay(near_results, 0)
    off_relay(edge_forward, *edges.pop(0))
    arrived(x_in.at[at(last_rows, group), :], pack_recv.at[1])
    for slot in range(tp):
        hidden_rows(last_rows, group, slot)
    results(1, 0)
    results(1, 1)
    off_relay(edge_forward, *edges.pop(0))
    merges = [(0, 0), (0, 1), (1, 0), (1, 1)] + [
        (s, c) for c in range(2, CHUNKS) for s in range(2)
    ]
    on_relay(relay_merge, *merges.pop(0))
    for c in range(2, CHUNKS):
        forward_weights(2 + c)
        got_down(c)
        results(0, c)
        results(1, c)
        for _ in range(1 + c % 2):
            off_relay(edge_forward, *edges.pop(0))
        on_relay(near_results, c)
        on_relay(relay_merge, *merges.pop(0))
    for item in edges:
        off_relay(edge_forward, *item)
    for c in range(1, CHUNKS):
        off_relay(near_results, c)
    while len(merges) > 4:
        on_relay(relay_merge, *merges.pop(0))
    project()
    for item in merges:
        on_relay(relay_merge, *item)
    for c in range(CHUNKS):
        finish(c)

    def sent(ref, sem):
        pltpu.make_async_copy(ref, ref, sem).wait()

    @pl.when(e < n - 1)
    def sent_after():
        halo_after.wait_send()

    @pl.when(e > 0)
    def sent_before():
        halo_before.wait_send()

    for copy in w_far + w_near + [c for i in range(items) for c in w_fwd[i]]:
        copy.wait_send()
    send_info.wait_send()
    for copy in send_blocks:
        copy.wait_send()
    others = half_count - 1
    sent(near_out.at[pl.ds(0, others * stride), :], near_send)
    for k in range(1, tp):
        sent(att_in.at[0], att_send.at[k])
    for c in range(CHUNKS):
        sent(near_in.at[c, pl.ds(0, others * stride), :], back_near_send.at[c])
        for s in range(2):
            sent(res.at[c, pl.ds(0, (members - 1) * stride), :], back_far_send.at[s, c])

        @pl.when(is_relay)
        def sent_relay():
            for s in range(2):
                sent(relay_out.at[s, c, pl.ds(0, others * stride), :], pack_send.at[s, c])
                sent(merged.at[s, c], merged_send.at[s, c])

        @pl.when(jnp.logical_not(is_relay))
        def sent_own():
            for s in range(2):
                sent(relay_in.at[s, c, pl.ds(0, group), :], edge_send.at[s, c])


def body(
    queries,
    keys_values,
    sink_logits,
    out_weight,
    expert_tokens,
    norm_gain,
    routes,
    route_weights,
    gate_weight,
    up_weight,
    down_weight,
):
    n, tp = lax.axis_size("ep"), lax.axis_size("tp")
    count, width = expert_tokens.shape
    cap = 3 * count * TOPK // (2 * n)
    stride = -(-cap // 16) * 16
    rows = n // 2 * stride
    wide = width // CHUNKS
    shard = gate_weight.shape[2]
    seq_rows, q_width = queries.shape
    kv_width = keys_values.shape[1]
    items = 2 + CHUNKS
    side = tp // 2
    bf16, f32 = jnp.bfloat16, jnp.float32
    dma = pltpu.SemaphoreType.DMA

    def vmem(*shape, dtype=bf16):
        return pltpu.VMEM(shape, dtype)

    scratch = [
        vmem(count, width),
        vmem(CHUNKS, count, wide),
        vmem(8, count, dtype=f32),
        vmem(2, 8, count, dtype=f32),
        vmem(2, CHUNKS, count, wide),
        vmem(n * stride, width),
        vmem(rows, width),
        vmem(2, CHUNKS, rows, wide),
        vmem(3, rows, count),
        vmem(tp, width, shard),
        vmem(tp, width, shard),
        vmem(CHUNKS, tp * shard, wide),
        vmem(n * stride, tp * shard),
        vmem(CHUNKS, n * stride, wide),
        vmem(2, CHUNKS, rows, wide),
        vmem(2, CHUNKS, count, wide),
        vmem(CHUNKS, rows, wide),
        vmem(CHUNKS, count, wide),
        vmem(3, count, rows),
        vmem(3, count, rows),
        vmem(seq_rows, q_width),
        vmem(seq_rows + 2 * WINDOW, kv_width),
        vmem(seq_rows + 2 * WINDOW, kv_width),
        vmem(seq_rows, q_width),
        vmem(tp, seq_rows // tp, q_width),
        vmem(*out_weight.shape),
        dma((4,)),
        dma((items, tp)),
        dma((items, side)),
        dma((items,)),
        dma((items, side)),
        dma((2,)),
        dma((2,)),
        dma((2,)),
        dma,
        dma((2, CHUNKS)),
        dma((CHUNKS,)),
        dma,
        dma,
        dma((2,)),
        dma((2, CHUNKS)),
        dma((CHUNKS,)),
        dma((CHUNKS,)),
        dma((2, CHUNKS)),
        dma((2, CHUNKS)),
        dma((2, CHUNKS)),
        dma((2, CHUNKS)),
        dma((CHUNKS,)),
        dma((tp,)),
        dma((tp,)),
    ]
    anywhere = pl.BlockSpec(memory_space=pl.ANY)
    small = pl.BlockSpec(memory_space=pltpu.VMEM)
    return pl.pallas_call(
        functools.partial(layer_kernel, n, tp, cap, stride),
        out_shape=(
            pltpu.VMEM((seq_rows // tp, width), bf16),
            pltpu.VMEM((count, width), bf16),
        ),
        in_specs=[
            pl.BlockSpec(memory_space=pltpu.SMEM), anywhere, anywhere, anywhere, anywhere,
            small, small, small, anywhere, anywhere, anywhere,
        ],
        out_specs=(small, small),
        scratch_shapes=scratch,
        compiler_params=pltpu.CompilerParams(
            collective_id=0, has_side_effects=True, vmem_limit_bytes=62000000
        ),
        name="layer",
    )(
        sink_logits, queries, keys_values, out_weight, expert_tokens,
        norm_gain.reshape(1, width), routes.T, route_weights.T,
        gate_weight[0], up_weight[0], down_weight[0],
    )


def solution(mesh):
    return jax.shard_map(
        body,
        mesh=mesh,
        in_specs=(
            P("ep", "tp"),
            P("ep", "tp"),
            P(),
            P(),
            P(("ep", "tp"), None),
            P(),
            P(("ep", "tp"), None),
            P(("ep", "tp"), None),
            P("ep", None, "tp"),
            P("ep", None, "tp"),
            P("ep", "tp", None),
        ),
        out_specs=(P(("ep", "tp"), None), P(("ep", "tp"), None)),
        check_vma=False,
    )
```

```python
import functools

import jax
import jax.numpy as jnp
from jax import lax
from jax.experimental import pallas as pl
from jax.experimental.pallas import tpu as pltpu
from jax.sharding import PartitionSpec as P

HEAD_DIM = 64
WINDOW = 128
TOPK = 2
PLANES = 4
CHUNKS = 8
STEP_ROWS = 128
NEG_FILL = -1e30
MESH = pl.DeviceIdType.MESH


def div(a, b):
    return lax.div(a, jnp.int32(b))


def rem(a, b):
    return lax.rem(a, jnp.int32(b))


def layer_kernel(n, tp, cap, stride, *refs):
    (
        sink_hbm, q_hbm, kv_hbm, ow_hbm, tok_hbm, gain_hbm, routes_hbm, rweights_hbm,
        gate_hbm, up_hbm, down_hbm,
        mo_v, out_v,
        sink, gain, routes, rweights, tok_v, norm_v, info, info_in, block_in, x_in, near_out, relay_out, sel,
        gate_s, up_s, down_s, hid, res, relay_in, merged, near_in, far_in,
        mix_hi, mix_lo,
        q_v, kv_s, vk_s, att, att_in, ow_v,
        load_sem, w_near_recv, w_recv, w_near_send, w_far_send, w_fwd_send,
        halo_recv, halo_send, info_recv, info_send, block_recv, block_send,
        near_recv, near_send, pack_recv, pack_send,
        back_near_recv, back_near_send, back_far_send, direct_send, edge_send,
        relay_recv, merged_send, far_recv, att_recv, att_send,
    ) = refs
    count, width = tok_v.shape
    wide = width // CHUNKS
    half_count = n // 2
    members = n // PLANES
    rows = half_count * stride
    group = members * stride
    side = tp // 2
    shard = gate_s.shape[2]
    seq_rows, q_width = q_v.shape
    heads = q_width // HEAD_DIM
    kv_heads = kv_s.shape[1] // (2 * HEAD_DIM)
    fan = heads // kv_heads
    own_count = seq_rows // tp

    e = lax.axis_index("ep")
    t = lax.axis_index("tp")
    plane = div(e, members)
    member = rem(e, members)
    half = div(e, half_count)
    local = rem(e, half_count)
    other = 1 - half
    is_relay = jnp.logical_or(plane == 1, plane == 2)
    own_relay_plane = 1 + half
    far_relay = (1 + other) * members + member
    tp_base = t - rem(t, side)
    tp_far = rem(t + side, tp)

    def near_tp(k):
        return tp_base + rem(t - tp_base + k, side)

    def near_ep(j):
        return rem(local + j, half_count)

    def far_plane(s):
        return 1 + other if s else 3 * other

    def far_source(s, k):
        return far_plane(s) * members + rem(member + k, members)

    def at(start, size):
        return pl.ds(pl.multiple_of(start, 16), size)

    def cols(c):
        return pl.ds(c * wide, wide)

    def remote(src, dst, send, recv, **where):
        return pltpu.make_async_remote_copy(
            src_ref=src, dst_ref=dst, send_sem=send, recv_sem=recv,
            device_id=where, device_id_type=MESH,
        )

    def arrived(ref, sem):
        pltpu.make_async_copy(ref, ref, sem).wait()

    kv_own = kv_s.at[pl.ds(WINDOW, seq_rows), :]
    loads = [
        pltpu.make_async_copy(tok_hbm, tok_v, load_sem.at[0]),
        pltpu.make_async_copy(kv_hbm, kv_own, load_sem.at[1]),
        pltpu.make_async_copy(q_hbm, q_v, load_sem.at[2]),
        pltpu.make_async_copy(ow_hbm, ow_v, load_sem.at[3]),
        pltpu.make_async_copy(gain_hbm, gain, load_sem.at[4]),
        pltpu.make_async_copy(routes_hbm, routes, load_sem.at[5]),
        pltpu.make_async_copy(rweights_hbm, rweights, load_sem.at[6]),
        pltpu.make_async_copy(sink_hbm, sink, load_sem.at[7]),
    ]
    items = 2 + CHUNKS

    def w_source(item):
        if item == 0:
            return gate_hbm
        if item == 1:
            return up_hbm
        return down_hbm.at[:, cols(item - 2)]

    def w_place(item, slot):
        if item == 0:
            return gate_s.at[slot]
        if item == 1:
            return up_s.at[slot]
        return down_s.at[item - 2, pl.ds(slot * shard, shard), :]

    def w_sem(item, slot):
        if slot < side:
            return w_near_recv.at[slot, 0 if item < 2 else 1]
        return w_recv.at[item, slot - side]

    own_weights = [
        pltpu.make_async_copy(w_source(i), w_place(i, 0), w_sem(i, 0)) for i in range(items)
    ]
    barrier = pltpu.get_barrier_semaphore()

    def greet(**where):
        pl.semaphore_signal(barrier, inc=1, device_id=where, device_id_type=MESH)

    for j in range(1, half_count):
        greet(ep=half * half_count + near_ep(j))
    for k in range(1, tp):
        greet(tp=rem(t + k, tp))

    @pl.when(e > 0)
    def greet_before():
        greet(ep=e - 1)

    @pl.when(e < n - 1)
    def greet_after():
        greet(ep=e + 1)

    @pl.when(is_relay)
    def greet_sources():
        for s in range(2):
            greet(ep=far_source(s, 0))

    @pl.when(jnp.logical_not(is_relay))
    def greet_relay():
        greet(ep=far_relay)

    for copy in loads:
        copy.start()

    def one(flag):
        return jnp.where(flag, 1, 0).astype(jnp.int32)

    pl.semaphore_wait(
        barrier, half_count - 1 + tp - 1 + one(e > 0) + one(e < n - 1) + 1 + one(is_relay)
    )

    halo_after = remote(
        kv_hbm.at[pl.ds(seq_rows - WINDOW, WINDOW), :], kv_s.at[pl.ds(0, WINDOW), :],
        halo_send.at[0], halo_recv.at[0], ep=rem(e + 1, n),
    )
    halo_before = remote(
        kv_hbm.at[pl.ds(0, WINDOW), :], kv_s.at[pl.ds(seq_rows + WINDOW, WINDOW), :],
        halo_send.at[1], halo_recv.at[1], ep=rem(e + n - 1, n),
    )

    @pl.when(e < n - 1)
    def send_after():
        halo_after.start()

    @pl.when(e > 0)
    def send_before():
        halo_before.start()

    w_far = [
        remote(w_source(i), w_place(i, side), w_far_send, w_sem(i, side), tp=tp_far)
        for i in range(items)
    ]
    w_near = [
        remote(
            w_source(i), w_place(i, (side - k) % side), w_near_send.at[k],
            w_sem(i, (side - k) % side), tp=near_tp(k),
        )
        for i in range(items)
        for k in range(1, side)
    ]
    w_fwd = {
        i: [
            remote(
                w_place(i, side), w_place(i, side + (side - k) % side), w_fwd_send.at[k],
                w_sem(i, side + (side - k) % side), tp=near_tp(k),
            )
            for k in range(1, side)
        ]
        for i in range(items)
    }
    for copy in w_far:
        copy.start()

    loads[0].wait()
    for copy in loads[4:]:
        copy.wait()
    tokens = tok_v[...].astype(jnp.float32)
    centred = tokens - jnp.mean(tokens, -1, keepdims=True)
    scale = lax.rsqrt(jnp.mean(centred * centred, -1, keepdims=True) + 1e-06)
    normed = (centred * scale * gain[...]).astype(jnp.bfloat16)
    for c in range(CHUNKS):
        norm_v[c] = normed[:, c * wide : (c + 1) * wide]

    expert = lax.broadcasted_iota(jnp.int32, (n, count), 0)
    named = [expert == routes[k : k + 1, :] for k in range(TOPK)]
    member_of = functools.reduce(jnp.logical_or, named)
    earlier = lax.broadcasted_iota(jnp.int32, (count, count), 0) < lax.broadcasted_iota(
        jnp.int32, (count, count), 1
    )
    rank = jnp.dot(
        jnp.where(member_of, 1.0, 0.0).astype(jnp.bfloat16),
        jnp.where(earlier, 1.0, 0.0).astype(jnp.bfloat16),
        preferred_element_type=jnp.float32,
    )
    place = expert.astype(jnp.float32) * float(stride) + rank
    info[...] = jnp.zeros_like(info)
    for k in range(TOPK):
        info[k : k + 1, :] = jnp.sum(jnp.where(named[k], place, 0.0), 0, keepdims=True)
        info[TOPK + k : TOPK + k + 1, :] = rweights[k : k + 1, :]

    slot_of = one(is_relay)
    send_info = remote(info, info_in.at[slot_of], info_send, info_recv.at[slot_of], ep=far_relay)
    send_info.start()
    send_blocks = [
        remote(
            norm_v.at[c], block_in.at[slot_of, c], block_send, block_recv.at[slot_of, c],
            ep=far_relay,
        )
        for c in range(CHUNKS)
    ]
    for copy in send_blocks:
        copy.start()
    for copy in w_near:
        copy.start()
    for copy in own_weights:
        copy.start()

    base = half * rows

    def hits(table, k):
        slot = lax.broadcasted_iota(jnp.int32, (rows, count), 0) + base
        return slot.astype(jnp.float32) == table[k : k + 1, :]

    def pick(table):
        hit = functools.reduce(jnp.logical_or, [hits(table, k) for k in range(TOPK)])
        return jnp.where(hit, 1.0, 0.0).astype(jnp.bfloat16)

    def mixture(table, where):
        mix = sum(
            jnp.where(hits(table, k), table[TOPK + k : TOPK + k + 1, :], 0.0)
            for k in range(TOPK)
        ).T
        high = mix.astype(jnp.bfloat16)
        mix_hi[where] = high
        mix_lo[where] = (mix - high.astype(jnp.float32)).astype(jnp.bfloat16)

    own_table = info[...]
    sel[2] = pick(own_table)
    for c in range(CHUNKS):
        near_out[:, cols(c)] = jnp.dot(
            sel[2], norm_v[c], preferred_element_type=jnp.float32
        ).astype(jnp.bfloat16)
    own_rows = at(e * stride, stride)
    near_self = pltpu.make_async_copy(
        near_out.at[at(local * stride, stride), :], x_in.at[own_rows, :], near_recv
    )
    near_self.start()
    for j in range(1, half_count):
        remote(
            near_out.at[at(near_ep(j) * stride, stride), :], x_in.at[own_rows, :],
            near_send, near_recv, ep=half * half_count + near_ep(j),
        ).start()
    mixture(own_table, 2)

    def both_orders(first, size):
        for kv_head in range(kv_heads):
            lanes = slice(kv_head * 2 * HEAD_DIM, (kv_head + 1) * 2 * HEAD_DIM)
            both = kv_s[first : first + size, lanes]
            vk_s[first : first + size, lanes] = jnp.concatenate(
                [both[:, HEAD_DIM:], both[:, :HEAD_DIM]], 1
            )

    def got_halo():
        @pl.when(e == 0)
        def no_before():
            kv_s[0:WINDOW, :] = jnp.zeros((WINDOW, kv_s.shape[1]), kv_s.dtype)

        @pl.when(e > 0)
        def got_before():
            halo_after.wait_recv()

        @pl.when(e == n - 1)
        def no_after():
            kv_s[seq_rows + WINDOW : seq_rows + 2 * WINDOW, :] = jnp.zeros(
                (WINDOW, kv_s.shape[1]), kv_s.dtype
            )

        @pl.when(e < n - 1)
        def got_after():
            halo_before.wait_recv()

        both_orders(0, WINDOW)
        both_orders(seq_rows + WINDOW, WINDOW)

    loads[1].wait()
    both_orders(WINDOW, seq_rows)
    loads[2].wait()

    span = STEP_ROWS + 2 * WINDOW
    seq_total = seq_rows * n
    lower = lax.broadcasted_iota(jnp.int32, (STEP_ROWS, 2 * HEAD_DIM), 1) < HEAD_DIM

    def attend_step(start):
        start = pl.multiple_of(start, STEP_ROWS)
        row = lax.broadcasted_iota(jnp.int32, (STEP_ROWS, span), 0)
        column = lax.broadcasted_iota(jnp.int32, (STEP_ROWS, span), 1)
        key_pos = e * seq_rows + start - WINDOW + column
        allowed = (
            (column >= row) & (column <= row + 2 * WINDOW)
            & (key_pos >= 0) & (key_pos < seq_total)
        )
        for kv_head in range(kv_heads):
            lanes = slice(kv_head * 2 * HEAD_DIM, (kv_head + 1) * 2 * HEAD_DIM)
            kv = kv_s[pl.ds(start, span), lanes]
            vk = vk_s[pl.ds(start, span), lanes]
            for pair in range(fan // 2):
                head = kv_head * fan + 2 * pair
                places = slice(head * HEAD_DIM, (head + 2) * HEAD_DIM)
                q_pair = q_v[pl.ds(start, STEP_ROWS), places] * jnp.bfloat16(HEAD_DIM ** -0.5)
                results = []
                for odd in range(2):
                    q_one = jnp.where(lower != bool(odd), q_pair, jnp.zeros_like(q_pair))
                    key_side, value_side = (vk, kv) if odd else (kv, vk)
                    scores = lax.dot_general(
                        q_one, key_side, (((1,), (1,)), ((), ())),
                        preferred_element_type=jnp.float32,
                    )
                    scores = jnp.where(allowed, scores, NEG_FILL)
                    bound = sink[t * heads + head + odd]
                    top = jnp.maximum(jnp.max(scores, 1, keepdims=True), bound)
                    expo = jnp.exp(scores - top)
                    denom = jnp.sum(expo, 1, keepdims=True) + jnp.exp(bound - top)
                    value = jnp.dot(
                        expo.astype(jnp.bfloat16), value_side, preferred_element_type=jnp.float32
                    )
                    results.append(value / denom)
                att[pl.ds(start, STEP_ROWS), places] = jnp.where(
                    lower, results[0], results[1]
                ).astype(jnp.bfloat16)

    def attend_inner(first, last):
        def step(i, carry):
            attend_step(i * STEP_ROWS)
            return carry

        lax.fori_loop(first, last, step, 0)

    def attend_edges():
        def step(i, carry):
            attend_step(i * (seq_rows - STEP_ROWS))
            return carry

        lax.fori_loop(0, 2, step, 0)
        for k in range(tp):
            owner = rem(t + k, tp)
            block = att.at[at(owner * own_count, own_count), :]
            if k:
                remote(block, att_in.at[t], att_send, att_recv, tp=owner).start()
            else:
                pltpu.make_async_copy(block, att_in.at[t], att_recv).start()

    def relay_tables(s):
        arrived(info_in.at[s], info_recv.at[s])
        table = info_in[s]
        sel[s] = pick(table)
        mixture(table, s)

    def relay_forward(s, c):
        arrived(block_in.at[s, c], block_recv.at[s, c])
        relay_out[s, c] = jnp.dot(
            sel[s], block_in[s, c], preferred_element_type=jnp.float32
        ).astype(jnp.bfloat16)
        landing = x_in.at[at(far_source(s, 0) * stride, stride), cols(c)]
        for j in range(1, half_count):
            remote(
                relay_out.at[s, c, at(near_ep(j) * stride, stride), :], landing,
                pack_send, pack_recv.at[s], ep=half * half_count + near_ep(j),
            ).start()
        pltpu.make_async_copy(
            relay_out.at[s, c, at(local * stride, stride), :], landing, pack_recv.at[s]
        ).start()

    def on_relay(task, *args):
        pl.when(is_relay)(lambda: task(*args))

    def off_relay(task, *args):
        pl.when(jnp.logical_not(is_relay))(lambda: task(*args))

    def forward_weights(i):
        arrived(w_place(i, side), w_sem(i, side))
        for copy in w_fwd[i]:
            copy.start()

    def hidden_rows(start, size, slot):
        x = x_in[at(start, size), :]
        gate = jnp.dot(x, gate_s[slot], preferred_element_type=jnp.float32)
        up = jnp.dot(x, up_s[slot], preferred_element_type=jnp.float32)
        hid[at(start, size), pl.ds(slot * shard, shard)] = (
            gate / (1.0 + jnp.exp(-gate)) * up
        ).astype(jnp.bfloat16)

    def got_weights(item, slot):
        arrived(w_place(item, slot), w_sem(item, slot))

    def project():
        arrived(att_in, att_recv)
        loads[3].wait()
        total = jnp.zeros(mo_v.shape, jnp.float32)
        for c in range(CHUNKS):
            total = sum(
                jnp.dot(
                    att_in[k], ow_v[k * q_width : (k + 1) * q_width, cols(c)],
                    preferred_element_type=jnp.float32,
                )
                for k in range(tp)
            )
            mo_v[:, cols(c)] = total.astype(jnp.bfloat16)

    def results(s, c, direct=False):
        first = far_plane(s) * group
        res[c, at(first, group), :] = jnp.dot(
            hid[at(first, group), :], down_s[c], preferred_element_type=jnp.float32
        ).astype(jnp.bfloat16)
        landing = relay_in.at[s, c, at(local * stride, stride), :]
        for k in range(members):
            block = res.at[c, at(far_source(s, k) * stride, stride), :]
            near_plane = own_relay_plane if direct else plane
            if k:
                remote(
                    block, landing, back_far_send, relay_recv.at[s, c],
                    ep=near_plane * members + rem(member + k, members),
                ).start()
            else:
                keep = pltpu.make_async_copy(block, landing, relay_recv.at[s, c])
            if not k and direct:
                hand = remote(
                    block, landing, direct_send, relay_recv.at[s, c],
                    ep=own_relay_plane * members + member,
                )
                pl.when(is_relay)(keep.start)
                pl.when(jnp.logical_not(is_relay))(hand.start)
            elif not k:
                keep.start()

    def edge_block(s, c):
        return relay_in.at[s, c, at(rem(plane, 2) * group, group), :]

    def edge_forward(s, c):
        arrived(edge_block(s, c), relay_recv.at[s, c])
        remote(
            edge_block(s, c), edge_block(s, c), edge_send, relay_recv.at[s, c],
            ep=own_relay_plane * members + member,
        ).start()

    def near_results(c):
        first = half * rows
        res[c, at(first, rows), :] = jnp.dot(
            hid[at(first, rows), :], down_s[c], preferred_element_type=jnp.float32
        ).astype(jnp.bfloat16)
        landing = near_in.at[c, at(local * stride, stride), :]
        for j in range(1, half_count):
            target = half * half_count + near_ep(j)
            remote(
                res.at[c, at(target * stride, stride), :], landing,
                back_near_send, back_near_recv.at[c], ep=target,
            ).start()
        pltpu.make_async_copy(
            res.at[c, own_rows, :], landing, back_near_recv.at[c]
        ).start()

    def mixed(where, values):
        return jnp.dot(
            mix_hi[where], values, preferred_element_type=jnp.float32
        ) + jnp.dot(mix_lo[where], values, preferred_element_type=jnp.float32)

    def relay_merge(s, c):
        arrived(relay_in.at[s, c], relay_recv.at[s, c])
        merged[s, c] = mixed(s, relay_in[s, c]).astype(jnp.bfloat16)
        remote(
            merged.at[s, c], far_in.at[c], merged_send, far_recv.at[c],
            ep=far_source(s, 0),
        ).start()

    def finish(c):
        arrived(near_in.at[c], back_near_recv.at[c])
        total = mixed(2, near_in[c])
        arrived(far_in.at[c], far_recv.at[c])
        out_v[:, cols(c)] = (total + far_in[c].astype(jnp.float32)).astype(jnp.bfloat16)

    on_relay(relay_tables, 0)
    steps = seq_rows // STEP_ROWS
    quarter = max(steps // 4, 1)
    bounds = [1] + [min(1 + quarter * (i + 1), steps - 1) for i in range(4)]
    plan = [range(0, 2), range(2, 4), range(4, 6), range(6, CHUNKS)]
    for i in range(4):
        attend_inner(bounds[i], bounds[i + 1])
        for c in plan[i]:
            on_relay(relay_forward, 0, c)
    forward_weights(0)
    on_relay(relay_tables, 1)
    on_relay(relay_forward, 1, 0)
    got_halo()
    attend_edges()
    for c in range(1, 4):
        on_relay(relay_forward, 1, c)
    for slot in range(side):
        arrived(gate_s.at[pl.ds(0, 2)], w_near_recv.at[slot, 0])
    first_rows, last_rows = far_plane(0) * group, far_plane(1) * group
    arrived(x_in.at[at(first_rows, group), :], pack_recv.at[0])
    for slot in range(side):
        hidden_rows(first_rows, group, slot)
    for c in range(4, 6):
        on_relay(relay_forward, 1, c)
    arrived(x_in.at[at(half * rows, rows), :], near_recv)
    for slot in range(side):
        hidden_rows(half * rows, rows, slot)
    on_relay(relay_forward, 1, 6)
    forward_weights(1)
    hidden_rows(first_rows, group, side)
    for c in range(7, CHUNKS):
        on_relay(relay_forward, 1, c)
    hidden_rows(half * rows, rows, side)
    for slot in range(side + 1, tp):
        for item in range(2):
            got_weights(item, slot)
        hidden_rows(first_rows, group, slot)

    def got_down(c):
        for slot in range(tp):
            if slot < side and c == 0:
                arrived(gate_s.at[0], w_near_recv.at[slot, 1])
            if slot > side:
                got_weights(2 + c, slot)

    directs = ((0, 0), (0, 1), (1, 0), (1, 1))
    order = [(0, 0), (0, 1), (1, 0), (1, 1)] + [(s, c) for c in range(2, CHUNKS) for s in range(2)]
    merges, edges = list(order), [item for item in order if item not in directs]
    forward_weights(2)
    got_down(0)
    results(0, 0, True)
    forward_weights(3)
    for slot in range(side + 1, tp):
        hidden_rows(half * rows, rows, slot)
    got_down(1)
    results(0, 1, True)
    near_results(0)
    arrived(x_in.at[at(last_rows, group), :], pack_recv.at[1])
    for slot in range(tp):
        hidden_rows(last_rows, group, slot)
        if slot == side - 1:
            on_relay(relay_merge, *merges.pop(0))
    results(1, 0, True)
    results(1, 1, True)
    on_relay(near_results, 1)
    on_relay(relay_merge, *merges.pop(0))
    for c in range(2, CHUNKS):
        forward_weights(2 + c)
        got_down(c)
        results(0, c)
        results(1, c)
        for _ in range((0, 1, 2, 1, 2, 2)[min(c - 2, 5)]):
            off_relay(edge_forward, *edges.pop(0))
        on_relay(near_results, c)
        on_relay(relay_merge, *merges.pop(0))
    for item in edges:
        off_relay(edge_forward, *item)
    for c in range(1, CHUNKS):
        off_relay(near_results, c)
    while len(merges) > 4:
        on_relay(relay_merge, *merges.pop(0))
    project()
    for item in merges:
        on_relay(relay_merge, *item)
    for c in range(CHUNKS):
        finish(c)

    def sent(ref, sem):
        pltpu.make_async_copy(ref, ref, sem).wait()

    @pl.when(e < n - 1)
    def sent_after():
        halo_after.wait_send()

    @pl.when(e > 0)
    def sent_before():
        halo_before.wait_send()

    whole_shard = gate_s.at[pl.ds(0, 3)]
    sent(whole_shard, w_far_send)
    for k in range(1, side):
        sent(whole_shard, w_near_send.at[k])
        sent(whole_shard, w_fwd_send.at[k])
    send_info.wait_send()
    sent(norm_v, block_send)
    others = half_count - 1
    sent(near_out.at[pl.ds(0, others * stride), :], near_send)
    sent(att_in.at[pl.ds(0, tp - 1)], att_send)
    sent(near_in.at[:, pl.ds(0, others * stride), :], back_near_send)
    sent(relay_in.at[:, :, pl.ds(0, (members - 1) * stride), :], back_far_send)

    @pl.when(is_relay)
    def sent_relay():
        sent(relay_out.at[:, :, pl.ds(0, others * stride), :], pack_send)
        sent(merged, merged_send)

    @pl.when(jnp.logical_not(is_relay))
    def sent_edge():
        sent(relay_in.at[:, pl.ds(0, 2), pl.ds(0, stride), :], direct_send)
        sent(relay_in.at[:, pl.ds(0, CHUNKS - 2), pl.ds(0, group), :], edge_send)


def body(
    queries,
    keys_values,
    sink_logits,
    out_weight,
    expert_tokens,
    norm_gain,
    routes,
    route_weights,
    gate_weight,
    up_weight,
    down_weight,
):
    n, tp = lax.axis_size("ep"), lax.axis_size("tp")
    count, width = expert_tokens.shape
    cap = 3 * count * TOPK // (2 * n)
    stride = -(-cap // 16) * 16
    rows = n // 2 * stride
    wide = width // CHUNKS
    shard = gate_weight.shape[2]
    seq_rows, q_width = queries.shape
    kv_width = keys_values.shape[1]
    items = 2 + CHUNKS
    side = tp // 2
    bf16, f32 = jnp.bfloat16, jnp.float32
    dma = pltpu.SemaphoreType.DMA

    def vmem(*shape, dtype=bf16):
        return pltpu.VMEM(shape, dtype)

    scratch = [
        pltpu.SMEM(sink_logits.shape, f32),
        vmem(1, width, dtype=f32),
        vmem(TOPK, count, dtype=jnp.int32),
        vmem(TOPK, count, dtype=f32),
        vmem(count, width),
        vmem(CHUNKS, count, wide),
        vmem(8, count, dtype=f32),
        vmem(2, 8, count, dtype=f32),
        vmem(2, CHUNKS, count, wide),
        vmem(n * stride, width),
        vmem(rows, width),
        vmem(2, CHUNKS, rows, wide),
        vmem(3, rows, count),
        vmem(tp, width, shard),
        vmem(tp, width, shard),
        vmem(CHUNKS, tp * shard, wide),
        vmem(n * stride, tp * shard),
        vmem(CHUNKS, n * stride, wide),
        vmem(2, CHUNKS, rows, wide),
        vmem(2, CHUNKS, count, wide),
        vmem(CHUNKS, rows, wide),
        vmem(CHUNKS, count, wide),
        vmem(3, count, rows),
        vmem(3, count, rows),
        vmem(seq_rows, q_width),
        vmem(seq_rows + 2 * WINDOW, kv_width),
        vmem(seq_rows + 2 * WINDOW, kv_width),
        vmem(seq_rows, q_width),
        vmem(tp, seq_rows // tp, q_width),
        vmem(*out_weight.shape),
        dma((8,)),
        dma((side, 2)),
        dma((items, side)),
        dma((side,)),
        dma,
        dma((side,)),
        dma((2,)),
        dma((2,)),
        dma((2,)),
        dma,
        dma((2, CHUNKS)),
        dma,
        dma,
        dma,
        dma((2,)),
        dma,
        dma((CHUNKS,)),
        dma,
        dma,
        dma,
        dma,
        dma((2, CHUNKS)),
        dma,
        dma((CHUNKS,)),
        dma,
        dma,
    ]
    anywhere = pl.BlockSpec(memory_space=pl.ANY)
    small = pl.BlockSpec(memory_space=pltpu.VMEM)
    return pl.pallas_call(
        functools.partial(layer_kernel, n, tp, cap, stride),
        out_shape=(
            pltpu.VMEM((seq_rows // tp, width), bf16),
            pltpu.VMEM((count, width), bf16),
        ),
        in_specs=[anywhere] * 11,
        out_specs=(small, small),
        scratch_shapes=scratch,
        compiler_params=pltpu.CompilerParams(
            collective_id=0, has_side_effects=True, vmem_limit_bytes=62000000
        ),
        name="layer",
    )(
        sink_logits, queries, keys_values, out_weight, expert_tokens,
        norm_gain.reshape(1, width), routes.T, route_weights.T,
        gate_weight[0], up_weight[0], down_weight[0],
    )


def solution(mesh):
    return jax.shard_map(
        body,
        mesh=mesh,
        in_specs=(
            P("ep", "tp"),
            P("ep", "tp"),
            P(),
            P(),
            P(("ep", "tp"), None),
            P(),
            P(("ep", "tp"), None),
            P(("ep", "tp"), None),
            P("ep", None, "tp"),
            P("ep", None, "tp"),
            P("ep", "tp", None),
        ),
        out_specs=(P(("ep", "tp"), None), P(("ep", "tp"), None)),
        check_vma=False,
    )
```

```python
import functools

import jax
import jax.numpy as jnp
from jax import lax
from jax.experimental import pallas as pl
from jax.experimental.pallas import tpu as pltpu
from jax.sharding import PartitionSpec as P

HEAD_DIM = 64
WINDOW = 128
TOPK = 2
PLANES = 4
CHUNKS = 8
STEP_ROWS = 128
NEG_FILL = -1e30
MESH = pl.DeviceIdType.MESH


def div(a, b):
    return lax.div(a, jnp.int32(b))


def rem(a, b):
    return lax.rem(a, jnp.int32(b))


def layer_kernel(n, tp, cap, stride, *refs):
    (
        sink_hbm, q_hbm, kv_hbm, ow_hbm, tok_hbm, gain_hbm, routes_hbm, rweights_hbm,
        gate_hbm, up_hbm, down_hbm,
        mo_v, out_v,
        sink, gain, routes, rweights, tok_v, norm_v, info, info_in, block_in, x_in, near_out, relay_out, sel,
        gate_s, up_s, down_s, hid, res, relay_in, merged, near_in, far_in,
        mix_hi, mix_lo,
        q_v, kv_s, vk_s, att, att_in, ow_v,
        load_sem, w_near_recv, w_recv, w_near_send, w_far_send, w_fwd_send,
        halo_recv, halo_send, info_recv, info_send, block_recv, block_send,
        near_recv, near_send, pack_recv, pack_send,
        back_near_recv, back_near_send, back_far_send, direct_send, edge_send,
        relay_recv, merged_send, far_recv, att_recv, att_send,
    ) = refs
    count, width = tok_v.shape
    wide = width // CHUNKS
    half_count = n // 2
    members = n // PLANES
    rows = half_count * stride
    group = members * stride
    side = tp // 2
    shard = gate_s.shape[2]
    seq_rows, q_width = q_v.shape
    heads = q_width // HEAD_DIM
    kv_heads = kv_s.shape[1] // (2 * HEAD_DIM)
    fan = heads // kv_heads
    own_count = seq_rows // tp

    e = lax.axis_index("ep")
    t = lax.axis_index("tp")
    plane = div(e, members)
    member = rem(e, members)
    half = div(e, half_count)
    local = rem(e, half_count)
    other = 1 - half
    is_relay = jnp.logical_or(plane == 1, plane == 2)
    own_relay_plane = 1 + half
    far_relay = (1 + other) * members + member
    tp_base = t - rem(t, side)
    tp_far = rem(t + side, tp)

    def near_tp(k):
        return tp_base + rem(t - tp_base + k, side)

    def near_ep(j):
        return rem(local + j, half_count)

    def far_plane(s):
        return 1 + other if s else 3 * other

    def far_source(s, k):
        return far_plane(s) * members + rem(member + k, members)

    def at(start, size):
        return pl.ds(pl.multiple_of(start, 16), size)

    def cols(c):
        return pl.ds(c * wide, wide)

    def remote(src, dst, send, recv, **where):
        return pltpu.make_async_remote_copy(
            src_ref=src, dst_ref=dst, send_sem=send, recv_sem=recv,
            device_id=where, device_id_type=MESH,
        )

    def arrived(ref, sem):
        pltpu.make_async_copy(ref, ref, sem).wait()

    kv_own = kv_s.at[pl.ds(WINDOW, seq_rows), :]
    loads = [
        pltpu.make_async_copy(tok_hbm, tok_v, load_sem.at[0]),
        pltpu.make_async_copy(kv_hbm, kv_own, load_sem.at[1]),
        pltpu.make_async_copy(q_hbm, q_v, load_sem.at[2]),
        pltpu.make_async_copy(ow_hbm, ow_v, load_sem.at[3]),
        pltpu.make_async_copy(gain_hbm, gain, load_sem.at[4]),
        pltpu.make_async_copy(routes_hbm, routes, load_sem.at[5]),
        pltpu.make_async_copy(rweights_hbm, rweights, load_sem.at[6]),
        pltpu.make_async_copy(sink_hbm, sink, load_sem.at[7]),
    ]
    items = 2 + CHUNKS

    def w_source(item):
        if item == 0:
            return gate_hbm
        if item == 1:
            return up_hbm
        return down_hbm.at[:, cols(item - 2)]

    def w_place(item, slot):
        if item == 0:
            return gate_s.at[slot]
        if item == 1:
            return up_s.at[slot]
        return down_s.at[item - 2, pl.ds(slot * shard, shard), :]

    def w_sem(item, slot):
        if slot < side:
            return w_near_recv.at[slot, 0 if item < 2 else 1]
        return w_recv.at[item, slot - side]

    own_weights = [
        pltpu.make_async_copy(w_source(i), w_place(i, 0), w_sem(i, 0)) for i in range(items)
    ]
    barrier = pltpu.get_barrier_semaphore()

    def greet(**where):
        pl.semaphore_signal(barrier, inc=1, device_id=where, device_id_type=MESH)

    for j in range(1, half_count):
        greet(ep=half * half_count + near_ep(j))
    for k in range(1, tp):
        greet(tp=rem(t + k, tp))

    @pl.when(e > 0)
    def greet_before():
        greet(ep=e - 1)

    @pl.when(e < n - 1)
    def greet_after():
        greet(ep=e + 1)

    @pl.when(is_relay)
    def greet_sources():
        for s in range(2):
            greet(ep=far_source(s, 0))

    @pl.when(jnp.logical_not(is_relay))
    def greet_relay():
        greet(ep=far_relay)

    for copy in loads:
        copy.start()

    def one(flag):
        return jnp.where(flag, 1, 0).astype(jnp.int32)

    pl.semaphore_wait(
        barrier, half_count - 1 + tp - 1 + one(e > 0) + one(e < n - 1) + 1 + one(is_relay)
    )

    halo_after = remote(
        kv_hbm.at[pl.ds(seq_rows - WINDOW, WINDOW), :], kv_s.at[pl.ds(0, WINDOW), :],
        halo_send.at[0], halo_recv.at[0], ep=rem(e + 1, n),
    )
    halo_before = remote(
        kv_hbm.at[pl.ds(0, WINDOW), :], kv_s.at[pl.ds(seq_rows + WINDOW, WINDOW), :],
        halo_send.at[1], halo_recv.at[1], ep=rem(e + n - 1, n),
    )

    @pl.when(e < n - 1)
    def send_after():
        halo_after.start()

    @pl.when(e > 0)
    def send_before():
        halo_before.start()

    w_far = [
        remote(w_source(i), w_place(i, side), w_far_send, w_sem(i, side), tp=tp_far)
        for i in range(items)
    ]
    w_near = [
        remote(
            w_source(i), w_place(i, (side - k) % side), w_near_send.at[k],
            w_sem(i, (side - k) % side), tp=near_tp(k),
        )
        for i in range(items)
        for k in range(1, side)
    ]
    w_fwd = {
        i: [
            remote(
                w_place(i, side), w_place(i, side + (side - k) % side), w_fwd_send.at[k],
                w_sem(i, side + (side - k) % side), tp=near_tp(k),
            )
            for k in range(1, side)
        ]
        for i in range(items)
    }
    for copy in w_far:
        copy.start()

    loads[0].wait()
    for copy in loads[4:]:
        copy.wait()
    tokens = tok_v[...].astype(jnp.float32)
    centred = tokens - jnp.mean(tokens, -1, keepdims=True)
    scale = lax.rsqrt(jnp.mean(centred * centred, -1, keepdims=True) + 1e-06)
    normed = (centred * scale * gain[...]).astype(jnp.bfloat16)
    for c in range(CHUNKS):
        norm_v[c] = normed[:, c * wide : (c + 1) * wide]

    expert = lax.broadcasted_iota(jnp.int32, (n, count), 0)
    named = [expert == routes[k : k + 1, :] for k in range(TOPK)]
    member_of = functools.reduce(jnp.logical_or, named)
    earlier = lax.broadcasted_iota(jnp.int32, (count, count), 0) < lax.broadcasted_iota(
        jnp.int32, (count, count), 1
    )
    rank = jnp.dot(
        jnp.where(member_of, 1.0, 0.0).astype(jnp.bfloat16),
        jnp.where(earlier, 1.0, 0.0).astype(jnp.bfloat16),
        preferred_element_type=jnp.float32,
    )
    place = expert.astype(jnp.float32) * float(stride) + rank
    info[...] = jnp.zeros_like(info)
    for k in range(TOPK):
        info[k : k + 1, :] = jnp.sum(jnp.where(named[k], place, 0.0), 0, keepdims=True)
        info[TOPK + k : TOPK + k + 1, :] = rweights[k : k + 1, :]

    slot_of = one(is_relay)
    send_info = remote(info, info_in.at[slot_of], info_send, info_recv.at[slot_of], ep=far_relay)
    send_info.start()
    send_blocks = [
        remote(
            norm_v.at[c], block_in.at[slot_of, c], block_send, block_recv.at[slot_of, c],
            ep=far_relay,
        )
        for c in range(CHUNKS)
    ]
    for copy in send_blocks:
        copy.start()
    for copy in w_near:
        copy.start()
    for copy in own_weights:
        copy.start()

    base = half * rows

    def hits(table, k):
        slot = lax.broadcasted_iota(jnp.int32, (rows, count), 0) + base
        return slot.astype(jnp.float32) == table[k : k + 1, :]

    def pick(table):
        hit = functools.reduce(jnp.logical_or, [hits(table, k) for k in range(TOPK)])
        return jnp.where(hit, 1.0, 0.0).astype(jnp.bfloat16)

    def mixture(table, where):
        mix = sum(
            jnp.where(hits(table, k), table[TOPK + k : TOPK + k + 1, :], 0.0)
            for k in range(TOPK)
        ).T
        high = mix.astype(jnp.bfloat16)
        mix_hi[where] = high
        mix_lo[where] = (mix - high.astype(jnp.float32)).astype(jnp.bfloat16)

    own_table = info[...]
    sel[2] = pick(own_table)
    for c in range(CHUNKS):
        near_out[:, cols(c)] = jnp.dot(
            sel[2], norm_v[c], preferred_element_type=jnp.float32
        ).astype(jnp.bfloat16)
    own_rows = at(e * stride, stride)
    near_self = pltpu.make_async_copy(
        near_out.at[at(local * stride, stride), :], x_in.at[own_rows, :], near_recv
    )
    near_self.start()
    for j in range(1, half_count):
        remote(
            near_out.at[at(near_ep(j) * stride, stride), :], x_in.at[own_rows, :],
            near_send, near_recv, ep=half * half_count + near_ep(j),
        ).start()
    mixture(own_table, 2)

    def both_orders(first, size):
        for kv_head in range(kv_heads):
            lanes = slice(kv_head * 2 * HEAD_DIM, (kv_head + 1) * 2 * HEAD_DIM)
            both = kv_s[first : first + size, lanes]
            vk_s[first : first + size, lanes] = jnp.concatenate(
                [both[:, HEAD_DIM:], both[:, :HEAD_DIM]], 1
            )

    def got_halo():
        @pl.when(e == 0)
        def no_before():
            kv_s[0:WINDOW, :] = jnp.zeros((WINDOW, kv_s.shape[1]), kv_s.dtype)

        @pl.when(e > 0)
        def got_before():
            halo_after.wait_recv()

        @pl.when(e == n - 1)
        def no_after():
            kv_s[seq_rows + WINDOW : seq_rows + 2 * WINDOW, :] = jnp.zeros(
                (WINDOW, kv_s.shape[1]), kv_s.dtype
            )

        @pl.when(e < n - 1)
        def got_after():
            halo_before.wait_recv()

        both_orders(0, WINDOW)
        both_orders(seq_rows + WINDOW, WINDOW)

    loads[1].wait()
    both_orders(WINDOW, seq_rows)
    loads[2].wait()

    span = STEP_ROWS + 2 * WINDOW
    seq_total = seq_rows * n
    lower = lax.broadcasted_iota(jnp.int32, (STEP_ROWS, 2 * HEAD_DIM), 1) < HEAD_DIM

    def attend_step(start):
        start = pl.multiple_of(start, STEP_ROWS)
        row = lax.broadcasted_iota(jnp.int32, (STEP_ROWS, span), 0)
        column = lax.broadcasted_iota(jnp.int32, (STEP_ROWS, span), 1)
        key_pos = e * seq_rows + start - WINDOW + column
        allowed = (
            (column >= row) & (column <= row + 2 * WINDOW)
            & (key_pos >= 0) & (key_pos < seq_total)
        )
        for kv_head in range(kv_heads):
            lanes = slice(kv_head * 2 * HEAD_DIM, (kv_head + 1) * 2 * HEAD_DIM)
            kv = kv_s[pl.ds(start, span), lanes]
            vk = vk_s[pl.ds(start, span), lanes]
            for pair in range(fan // 2):
                head = kv_head * fan + 2 * pair
                places = slice(head * HEAD_DIM, (head + 2) * HEAD_DIM)
                q_pair = q_v[pl.ds(start, STEP_ROWS), places] * jnp.bfloat16(HEAD_DIM ** -0.5)
                results = []
                for odd in range(2):
                    q_one = jnp.where(lower != bool(odd), q_pair, jnp.zeros_like(q_pair))
                    key_side, value_side = (vk, kv) if odd else (kv, vk)
                    scores = lax.dot_general(
                        q_one, key_side, (((1,), (1,)), ((), ())),
                        preferred_element_type=jnp.float32,
                    )
                    scores = jnp.where(allowed, scores, NEG_FILL)
                    bound = sink[t * heads + head + odd]
                    top = jnp.maximum(jnp.max(scores, 1, keepdims=True), bound)
                    expo = jnp.exp(scores - top)
                    denom = jnp.sum(expo, 1, keepdims=True) + jnp.exp(bound - top)
                    value = jnp.dot(
                        expo.astype(jnp.bfloat16), value_side, preferred_element_type=jnp.float32
                    )
                    results.append(value / denom)
                att[pl.ds(start, STEP_ROWS), places] = jnp.where(
                    lower, results[0], results[1]
                ).astype(jnp.bfloat16)

    def attend_inner(first, last):
        def step(i, carry):
            attend_step(i * STEP_ROWS)
            return carry

        lax.fori_loop(first, last, step, 0)

    def attend_edges():
        def step(i, carry):
            attend_step(i * (seq_rows - STEP_ROWS))
            return carry

        lax.fori_loop(0, 2, step, 0)
        for k in range(tp):
            owner = rem(t + k, tp)
            block = att.at[at(owner * own_count, own_count), :]
            if k:
                remote(block, att_in.at[t], att_send, att_recv, tp=owner).start()
            else:
                pltpu.make_async_copy(block, att_in.at[t], att_recv).start()

    def relay_tables(s):
        arrived(info_in.at[s], info_recv.at[s])
        table = info_in[s]
        sel[s] = pick(table)
        mixture(table, s)

    def relay_forward(s, c):
        arrived(block_in.at[s, c], block_recv.at[s, c])
        relay_out[s, c] = jnp.dot(
            sel[s], block_in[s, c], preferred_element_type=jnp.float32
        ).astype(jnp.bfloat16)
        landing = x_in.at[at(far_source(s, 0) * stride, stride), cols(c)]
        for j in range(1, half_count):
            remote(
                relay_out.at[s, c, at(near_ep(j) * stride, stride), :], landing,
                pack_send, pack_recv.at[s], ep=half * half_count + near_ep(j),
            ).start()
        pltpu.make_async_copy(
            relay_out.at[s, c, at(local * stride, stride), :], landing, pack_recv.at[s]
        ).start()

    def on_relay(task, *args):
        pl.when(is_relay)(lambda: task(*args))

    def off_relay(task, *args):
        pl.when(jnp.logical_not(is_relay))(lambda: task(*args))

    def forward_weights(i):
        arrived(w_place(i, side), w_sem(i, side))
        for copy in w_fwd[i]:
            copy.start()

    def hidden_rows(start, size, slot):
        x = x_in[at(start, size), :]
        gate = jnp.dot(x, gate_s[slot], preferred_element_type=jnp.float32)
        up = jnp.dot(x, up_s[slot], preferred_element_type=jnp.float32)
        hid[at(start, size), pl.ds(slot * shard, shard)] = (
            gate / (1.0 + jnp.exp(-gate)) * up
        ).astype(jnp.bfloat16)

    def got_weights(item, slot):
        arrived(w_place(item, slot), w_sem(item, slot))

    def project():
        arrived(att_in, att_recv)
        loads[3].wait()
        total = jnp.zeros(mo_v.shape, jnp.float32)
        for c in range(CHUNKS):
            total = sum(
                jnp.dot(
                    att_in[k], ow_v[k * q_width : (k + 1) * q_width, cols(c)],
                    preferred_element_type=jnp.float32,
                )
                for k in range(tp)
            )
            mo_v[:, cols(c)] = total.astype(jnp.bfloat16)

    def results(s, c, direct=False):
        first = far_plane(s) * group
        res[c, at(first, group), :] = jnp.dot(
            hid[at(first, group), :], down_s[c], preferred_element_type=jnp.float32
        ).astype(jnp.bfloat16)
        landing = relay_in.at[s, c, at(local * stride, stride), :]
        for k in range(members):
            block = res.at[c, at(far_source(s, k) * stride, stride), :]
            near_plane = own_relay_plane if direct else plane
            if k:
                remote(
                    block, landing, back_far_send, relay_recv.at[s, c],
                    ep=near_plane * members + rem(member + k, members),
                ).start()
            else:
                keep = pltpu.make_async_copy(block, landing, relay_recv.at[s, c])
            if not k and direct:
                hand = remote(
                    block, landing, direct_send, relay_recv.at[s, c],
                    ep=own_relay_plane * members + member,
                )
                pl.when(is_relay)(keep.start)
                pl.when(jnp.logical_not(is_relay))(hand.start)
            elif not k:
                keep.start()

    def edge_block(s, c):
        return relay_in.at[s, c, at(rem(plane, 2) * group, group), :]

    def edge_forward(s, c):
        arrived(edge_block(s, c), relay_recv.at[s, c])
        remote(
            edge_block(s, c), edge_block(s, c), edge_send, relay_recv.at[s, c],
            ep=own_relay_plane * members + member,
        ).start()

    def near_results(c):
        first = half * rows
        res[c, at(first, rows), :] = jnp.dot(
            hid[at(first, rows), :], down_s[c], preferred_element_type=jnp.float32
        ).astype(jnp.bfloat16)
        landing = near_in.at[c, at(local * stride, stride), :]
        for j in range(1, half_count):
            target = half * half_count + near_ep(j)
            remote(
                res.at[c, at(target * stride, stride), :], landing,
                back_near_send, back_near_recv.at[c], ep=target,
            ).start()
        pltpu.make_async_copy(
            res.at[c, own_rows, :], landing, back_near_recv.at[c]
        ).start()

    def mixed(where, values):
        return jnp.dot(
            mix_hi[where], values, preferred_element_type=jnp.float32
        ) + jnp.dot(mix_lo[where], values, preferred_element_type=jnp.float32)

    def relay_merge(s, c):
        arrived(relay_in.at[s, c], relay_recv.at[s, c])
        merged[s, c] = mixed(s, relay_in[s, c]).astype(jnp.bfloat16)
        remote(
            merged.at[s, c], far_in.at[c], merged_send, far_recv.at[c],
            ep=far_source(s, 0),
        ).start()

    def finish(c):
        arrived(near_in.at[c], back_near_recv.at[c])
        total = mixed(2, near_in[c])
        arrived(far_in.at[c], far_recv.at[c])
        out_v[:, cols(c)] = (total + far_in[c].astype(jnp.float32)).astype(jnp.bfloat16)

    on_relay(relay_tables, 0)
    steps = seq_rows // STEP_ROWS
    quarter = max(steps // 4, 1)
    bounds = [1] + [min(1 + quarter * (i + 1), steps - 1) for i in range(4)]
    plan = [range(0, 2), range(2, 4), range(4, 6), range(6, CHUNKS)]
    for i in range(4):
        attend_inner(bounds[i], bounds[i + 1])
        for c in plan[i]:
            on_relay(relay_forward, 0, c)
    forward_weights(0)
    on_relay(relay_tables, 1)
    on_relay(relay_forward, 1, 0)
    got_halo()
    attend_edges()
    for c in range(1, 4):
        on_relay(relay_forward, 1, c)
    for slot in range(side):
        arrived(gate_s.at[pl.ds(0, 2)], w_near_recv.at[slot, 0])
    first_rows, last_rows = far_plane(0) * group, far_plane(1) * group
    arrived(x_in.at[at(first_rows, group), :], pack_recv.at[0])
    for slot in range(side):
        hidden_rows(first_rows, group, slot)
    for c in range(4, 6):
        on_relay(relay_forward, 1, c)
    arrived(x_in.at[at(half * rows, rows), :], near_recv)
    for slot in range(side):
        hidden_rows(half * rows, rows, slot)
    on_relay(relay_forward, 1, 6)
    forward_weights(1)
    hidden_rows(first_rows, group, side)
    for c in range(7, CHUNKS):
        on_relay(relay_forward, 1, c)
    hidden_rows(half * rows, rows, side)
    for slot in range(side + 1, tp):
        for item in range(2):
            got_weights(item, slot)
        hidden_rows(first_rows, group, slot)

    def got_down(c):
        for slot in range(tp):
            if slot < side and c == 0:
                arrived(gate_s.at[0], w_near_recv.at[slot, 1])
            if slot > side:
                got_weights(2 + c, slot)

    directs = ((0, 0), (0, 1), (1, 0), (1, 1))
    order = [(0, 0), (0, 1), (1, 0), (1, 1)] + [(s, c) for c in range(2, CHUNKS) for s in range(2)]
    merges, edges = list(order), [item for item in order if item not in directs]
    def last_arrived():
        arrived(x_in.at[at(last_rows, group), :], pack_recv.at[1])

    def last_hidden(*slots):
        for slot in slots:
            hidden_rows(last_rows, group, slot)

    def near_hidden():
        for slot in range(side + 1, tp):
            hidden_rows(half * rows, rows, slot)

    forward_weights(2)
    on_relay(last_arrived)
    on_relay(last_hidden, *range(side))
    got_down(0)
    results(0, 0, True)
    forward_weights(3)
    on_relay(last_hidden, *range(side, tp))
    off_relay(near_hidden)
    got_down(1)
    results(0, 1, True)
    off_relay(near_results, 0)
    off_relay(last_arrived)
    off_relay(last_hidden, *range(tp))
    results(1, 0, True)
    results(1, 1, True)
    on_relay(relay_merge, *merges.pop(0))
    on_relay(near_hidden)
    off_relay(near_results, 1)
    on_relay(relay_merge, *merges.pop(0))
    for c in range(2, CHUNKS):
        forward_weights(2 + c)
        got_down(c)
        results(0, c)
        results(1, c)
        for _ in range((0, 1, 2, 1, 2, 2)[min(c - 2, 5)]):
            off_relay(edge_forward, *edges.pop(0))
        for _ in range((1, 1, 2, 1, 2, 1)[min(c - 2, 5)]):
            on_relay(relay_merge, *merges.pop(0))
        on_relay(near_results, c - 2)
    for item in edges:
        off_relay(edge_forward, *item)
    for c in range(2, CHUNKS):
        off_relay(near_results, c)
    for c in range(CHUNKS - 2, CHUNKS):
        on_relay(near_results, c)
    while len(merges) > 4:
        on_relay(relay_merge, *merges.pop(0))
    project()
    for item in merges:
        on_relay(relay_merge, *item)
    for c in range(CHUNKS):
        finish(c)

    def sent(ref, sem):
        pltpu.make_async_copy(ref, ref, sem).wait()

    @pl.when(e < n - 1)
    def sent_after():
        halo_after.wait_send()

    @pl.when(e > 0)
    def sent_before():
        halo_before.wait_send()

    whole_shard = gate_s.at[pl.ds(0, 3)]
    sent(whole_shard, w_far_send)
    for k in range(1, side):
        sent(whole_shard, w_near_send.at[k])
        sent(whole_shard, w_fwd_send.at[k])
    send_info.wait_send()
    sent(norm_v, block_send)
    others = half_count - 1
    sent(near_out.at[pl.ds(0, others * stride), :], near_send)
    sent(att_in.at[pl.ds(0, tp - 1)], att_send)
    sent(near_in.at[:, pl.ds(0, others * stride), :], back_near_send)
    sent(relay_in.at[:, :, pl.ds(0, (members - 1) * stride), :], back_far_send)

    @pl.when(is_relay)
    def sent_relay():
        sent(relay_out.at[:, :, pl.ds(0, others * stride), :], pack_send)
        sent(merged, merged_send)

    @pl.when(jnp.logical_not(is_relay))
    def sent_edge():
        sent(relay_in.at[:, pl.ds(0, 2), pl.ds(0, stride), :], direct_send)
        sent(relay_in.at[:, pl.ds(0, CHUNKS - 2), pl.ds(0, group), :], edge_send)


def body(
    queries,
    keys_values,
    sink_logits,
    out_weight,
    expert_tokens,
    norm_gain,
    routes,
    route_weights,
    gate_weight,
    up_weight,
    down_weight,
):
    n, tp = lax.axis_size("ep"), lax.axis_size("tp")
    count, width = expert_tokens.shape
    cap = 3 * count * TOPK // (2 * n)
    stride = -(-cap // 16) * 16
    rows = n // 2 * stride
    wide = width // CHUNKS
    shard = gate_weight.shape[2]
    seq_rows, q_width = queries.shape
    kv_width = keys_values.shape[1]
    items = 2 + CHUNKS
    side = tp // 2
    bf16, f32 = jnp.bfloat16, jnp.float32
    dma = pltpu.SemaphoreType.DMA

    def vmem(*shape, dtype=bf16):
        return pltpu.VMEM(shape, dtype)

    scratch = [
        pltpu.SMEM(sink_logits.shape, f32),
        vmem(1, width, dtype=f32),
        vmem(TOPK, count, dtype=jnp.int32),
        vmem(TOPK, count, dtype=f32),
        vmem(count, width),
        vmem(CHUNKS, count, wide),
        vmem(8, count, dtype=f32),
        vmem(2, 8, count, dtype=f32),
        vmem(2, CHUNKS, count, wide),
        vmem(n * stride, width),
        vmem(rows, width),
        vmem(2, CHUNKS, rows, wide),
        vmem(3, rows, count),
        vmem(tp, width, shard),
        vmem(tp, width, shard),
        vmem(CHUNKS, tp * shard, wide),
        vmem(n * stride, tp * shard),
        vmem(CHUNKS, n * stride, wide),
        vmem(2, CHUNKS, rows, wide),
        vmem(2, CHUNKS, count, wide),
        vmem(CHUNKS, rows, wide),
        vmem(CHUNKS, count, wide),
        vmem(3, count, rows),
        vmem(3, count, rows),
        vmem(seq_rows, q_width),
        vmem(seq_rows + 2 * WINDOW, kv_width),
        vmem(seq_rows + 2 * WINDOW, kv_width),
        vmem(seq_rows, q_width),
        vmem(tp, seq_rows // tp, q_width),
        vmem(*out_weight.shape),
        dma((8,)),
        dma((side, 2)),
        dma((items, side)),
        dma((side,)),
        dma,
        dma((side,)),
        dma((2,)),
        dma((2,)),
        dma((2,)),
        dma,
        dma((2, CHUNKS)),
        dma,
        dma,
        dma,
        dma((2,)),
        dma,
        dma((CHUNKS,)),
        dma,
        dma,
        dma,
        dma,
        dma((2, CHUNKS)),
        dma,
        dma((CHUNKS,)),
        dma,
        dma,
    ]
    anywhere = pl.BlockSpec(memory_space=pl.ANY)
    small = pl.BlockSpec(memory_space=pltpu.VMEM)
    return pl.pallas_call(
        functools.partial(layer_kernel, n, tp, cap, stride),
        out_shape=(
            pltpu.VMEM((seq_rows // tp, width), bf16),
            pltpu.VMEM((count, width), bf16),
        ),
        in_specs=[anywhere] * 11,
        out_specs=(small, small),
        scratch_shapes=scratch,
        compiler_params=pltpu.CompilerParams(
            collective_id=0, has_side_effects=True, vmem_limit_bytes=62000000
        ),
        name="layer",
    )(
        sink_logits, queries, keys_values, out_weight, expert_tokens,
        norm_gain.reshape(1, width), routes.T, route_weights.T,
        gate_weight[0], up_weight[0], down_weight[0],
    )


def solution(mesh):
    return jax.shard_map(
        body,
        mesh=mesh,
        in_specs=(
            P("ep", "tp"),
            P("ep", "tp"),
            P(),
            P(),
            P(("ep", "tp"), None),
            P(),
            P(("ep", "tp"), None),
            P(("ep", "tp"), None),
            P("ep", None, "tp"),
            P("ep", None, "tp"),
            P("ep", "tp", None),
        ),
        out_specs=(P(("ep", "tp"), None), P(("ep", "tp"), None)),
        check_vma=False,
    )
```

```python
import functools

import jax
import jax.numpy as jnp
from jax import lax
from jax.experimental import pallas as pl
from jax.experimental.pallas import tpu as pltpu
from jax.sharding import PartitionSpec as P

HEAD_DIM = 64
WINDOW = 128
TOPK = 2
PLANES = 4
CHUNKS = 8
STEP_ROWS = 128
NEG_FILL = -1e30
MESH = pl.DeviceIdType.MESH


def div(a, b):
    return lax.div(a, jnp.int32(b))


def rem(a, b):
    return lax.rem(a, jnp.int32(b))


def layer_kernel(n, tp, cap, stride, *refs):
    (
        sink_hbm, q_hbm, kv_hbm, ow_hbm, tok_hbm, gain_hbm, routes_hbm, rweights_hbm,
        gate_hbm, up_hbm, down_hbm,
        mo_v, out_v,
        sink, gain, routes, rweights, tok_v, norm_v, info, info_in, block_in, x_in, near_out, relay_out, sel,
        gate_s, up_s, down_s, hid, res, relay_in, merged, near_in, far_in,
        mix_hi, mix_lo,
        q_v, kv_s, vk_s, att, att_in, ow_v,
        load_sem, w_near_recv, w_recv, w_near_send, w_far_send, w_fwd_send,
        halo_recv, halo_send, info_recv, info_send, block_recv, block_send,
        near_recv, near_send, pack_recv, pack_send,
        back_near_recv, back_near_send, back_far_send, direct_send, edge_send,
        relay_recv, merged_send, far_recv, att_recv, att_send,
    ) = refs
    count, width = tok_v.shape
    wide = width // CHUNKS
    half_count = n // 2
    members = n // PLANES
    rows = half_count * stride
    group = members * stride
    side = tp // 2
    shard = gate_s.shape[2]
    seq_rows, q_width = q_v.shape
    heads = q_width // HEAD_DIM
    kv_heads = kv_s.shape[1] // (2 * HEAD_DIM)
    fan = heads // kv_heads
    own_count = seq_rows // tp

    e = lax.axis_index("ep")
    t = lax.axis_index("tp")
    plane = div(e, members)
    member = rem(e, members)
    half = div(e, half_count)
    local = rem(e, half_count)
    other = 1 - half
    is_relay = jnp.logical_or(plane == 1, plane == 2)
    own_relay_plane = 1 + half
    far_relay = (1 + other) * members + member
    tp_base = t - rem(t, side)
    tp_far = rem(t + side, tp)

    def near_tp(k):
        return tp_base + rem(t - tp_base + k, side)

    def near_ep(j):
        return rem(local + j, half_count)

    def far_plane(s):
        return 1 + other if s else 3 * other

    def far_source(s, k):
        return far_plane(s) * members + rem(member + k, members)

    def at(start, size):
        return pl.ds(pl.multiple_of(start, 16), size)

    def cols(c):
        return pl.ds(c * wide, wide)

    def remote(src, dst, send, recv, **where):
        return pltpu.make_async_remote_copy(
            src_ref=src, dst_ref=dst, send_sem=send, recv_sem=recv,
            device_id=where, device_id_type=MESH,
        )

    def arrived(ref, sem):
        pltpu.make_async_copy(ref, ref, sem).wait()

    kv_own = kv_s.at[pl.ds(WINDOW, seq_rows), :]
    loads = [
        pltpu.make_async_copy(tok_hbm, tok_v, load_sem.at[0]),
        pltpu.make_async_copy(kv_hbm, kv_own, load_sem.at[1]),
        pltpu.make_async_copy(q_hbm, q_v, load_sem.at[2]),
        pltpu.make_async_copy(ow_hbm, ow_v, load_sem.at[3]),
        pltpu.make_async_copy(gain_hbm, gain, load_sem.at[4]),
        pltpu.make_async_copy(routes_hbm, routes, load_sem.at[5]),
        pltpu.make_async_copy(rweights_hbm, rweights, load_sem.at[6]),
        pltpu.make_async_copy(sink_hbm, sink, load_sem.at[7]),
    ]
    items = 2 + CHUNKS

    def w_source(item):
        if item == 0:
            return gate_hbm
        if item == 1:
            return up_hbm
        return down_hbm.at[:, cols(item - 2)]

    def w_place(item, slot):
        if item == 0:
            return gate_s.at[slot]
        if item == 1:
            return up_s.at[slot]
        return down_s.at[item - 2, pl.ds(slot * shard, shard), :]

    def w_sem(item, slot):
        if slot < side:
            return w_near_recv.at[slot, 0 if item < 2 else 1]
        return w_recv.at[item, slot - side]

    own_weights = [
        pltpu.make_async_copy(w_source(i), w_place(i, 0), w_sem(i, 0)) for i in range(items)
    ]
    barrier = pltpu.get_barrier_semaphore()

    def greet(**where):
        pl.semaphore_signal(barrier, inc=1, device_id=where, device_id_type=MESH)

    for j in range(1, half_count):
        greet(ep=half * half_count + near_ep(j))
    for k in range(1, tp):
        greet(tp=rem(t + k, tp))

    @pl.when(e > 0)
    def greet_before():
        greet(ep=e - 1)

    @pl.when(e < n - 1)
    def greet_after():
        greet(ep=e + 1)

    @pl.when(is_relay)
    def greet_sources():
        for s in range(2):
            greet(ep=far_source(s, 0))

    @pl.when(jnp.logical_not(is_relay))
    def greet_relay():
        greet(ep=far_relay)

    for copy in loads:
        copy.start()

    def one(flag):
        return jnp.where(flag, 1, 0).astype(jnp.int32)

    pl.semaphore_wait(
        barrier, half_count - 1 + tp - 1 + one(e > 0) + one(e < n - 1) + 1 + one(is_relay)
    )

    halo_after = remote(
        kv_hbm.at[pl.ds(seq_rows - WINDOW, WINDOW), :], kv_s.at[pl.ds(0, WINDOW), :],
        halo_send.at[0], halo_recv.at[0], ep=rem(e + 1, n),
    )
    halo_before = remote(
        kv_hbm.at[pl.ds(0, WINDOW), :], kv_s.at[pl.ds(seq_rows + WINDOW, WINDOW), :],
        halo_send.at[1], halo_recv.at[1], ep=rem(e + n - 1, n),
    )

    @pl.when(e < n - 1)
    def send_after():
        halo_after.start()

    @pl.when(e > 0)
    def send_before():
        halo_before.start()

    w_far = [
        remote(w_source(i), w_place(i, side), w_far_send, w_sem(i, side), tp=tp_far)
        for i in range(items)
    ]
    w_near = [
        remote(
            w_source(i), w_place(i, (side - k) % side), w_near_send.at[k],
            w_sem(i, (side - k) % side), tp=near_tp(k),
        )
        for i in range(items)
        for k in range(1, side)
    ]
    w_fwd = {
        i: [
            remote(
                w_place(i, side), w_place(i, side + (side - k) % side), w_fwd_send.at[k],
                w_sem(i, side + (side - k) % side), tp=near_tp(k),
            )
            for k in range(1, side)
        ]
        for i in range(items)
    }
    for copy in w_far:
        copy.start()

    loads[0].wait()
    for copy in loads[4:]:
        copy.wait()
    tokens = tok_v[...].astype(jnp.float32)
    centred = tokens - jnp.mean(tokens, -1, keepdims=True)
    scale = lax.rsqrt(jnp.mean(centred * centred, -1, keepdims=True) + 1e-06)
    normed = (centred * scale * gain[...]).astype(jnp.bfloat16)
    for c in range(CHUNKS):
        norm_v[c] = normed[:, c * wide : (c + 1) * wide]

    expert = lax.broadcasted_iota(jnp.int32, (n, count), 0)
    named = [expert == routes[k : k + 1, :] for k in range(TOPK)]
    member_of = functools.reduce(jnp.logical_or, named)
    earlier = lax.broadcasted_iota(jnp.int32, (count, count), 0) < lax.broadcasted_iota(
        jnp.int32, (count, count), 1
    )
    rank = jnp.dot(
        jnp.where(member_of, 1.0, 0.0).astype(jnp.bfloat16),
        jnp.where(earlier, 1.0, 0.0).astype(jnp.bfloat16),
        preferred_element_type=jnp.float32,
    )
    place = expert.astype(jnp.float32) * float(stride) + rank
    info[...] = jnp.zeros_like(info)
    for k in range(TOPK):
        info[k : k + 1, :] = jnp.sum(jnp.where(named[k], place, 0.0), 0, keepdims=True)
        info[TOPK + k : TOPK + k + 1, :] = rweights[k : k + 1, :]

    slot_of = one(is_relay)
    send_info = remote(info, info_in.at[slot_of], info_send, info_recv.at[slot_of], ep=far_relay)
    send_info.start()
    send_blocks = [
        remote(
            norm_v.at[c], block_in.at[slot_of, c], block_send, block_recv.at[slot_of, c],
            ep=far_relay,
        )
        for c in range(CHUNKS)
    ]
    for copy in send_blocks:
        copy.start()
    for copy in w_near:
        copy.start()
    for copy in own_weights:
        copy.start()

    base = half * rows

    def hits(table, k):
        slot = lax.broadcasted_iota(jnp.int32, (rows, count), 0) + base
        return slot.astype(jnp.float32) == table[k : k + 1, :]

    def pick(table):
        hit = functools.reduce(jnp.logical_or, [hits(table, k) for k in range(TOPK)])
        return jnp.where(hit, 1.0, 0.0).astype(jnp.bfloat16)

    def mixture(table, where):
        mix = sum(
            jnp.where(hits(table, k), table[TOPK + k : TOPK + k + 1, :], 0.0)
            for k in range(TOPK)
        ).T
        high = mix.astype(jnp.bfloat16)
        mix_hi[where] = high
        mix_lo[where] = (mix - high.astype(jnp.float32)).astype(jnp.bfloat16)

    own_table = info[...]
    sel[2] = pick(own_table)
    for c in range(CHUNKS):
        near_out[:, cols(c)] = jnp.dot(
            sel[2], norm_v[c], preferred_element_type=jnp.float32
        ).astype(jnp.bfloat16)
    own_rows = at(e * stride, stride)
    near_self = pltpu.make_async_copy(
        near_out.at[at(local * stride, stride), :], x_in.at[own_rows, :], near_recv
    )
    near_self.start()
    for j in range(1, half_count):
        remote(
            near_out.at[at(near_ep(j) * stride, stride), :], x_in.at[own_rows, :],
            near_send, near_recv, ep=half * half_count + near_ep(j),
        ).start()
    mixture(own_table, 2)

    def both_orders(first, size):
        for kv_head in range(kv_heads):
            lanes = slice(kv_head * 2 * HEAD_DIM, (kv_head + 1) * 2 * HEAD_DIM)
            both = kv_s[first : first + size, lanes]
            vk_s[first : first + size, lanes] = jnp.concatenate(
                [both[:, HEAD_DIM:], both[:, :HEAD_DIM]], 1
            )

    def got_halo():
        @pl.when(e == 0)
        def no_before():
            kv_s[0:WINDOW, :] = jnp.zeros((WINDOW, kv_s.shape[1]), kv_s.dtype)

        @pl.when(e > 0)
        def got_before():
            halo_after.wait_recv()

        @pl.when(e == n - 1)
        def no_after():
            kv_s[seq_rows + WINDOW : seq_rows + 2 * WINDOW, :] = jnp.zeros(
                (WINDOW, kv_s.shape[1]), kv_s.dtype
            )

        @pl.when(e < n - 1)
        def got_after():
            halo_before.wait_recv()

        both_orders(0, WINDOW)
        both_orders(seq_rows + WINDOW, WINDOW)

    loads[1].wait()
    both_orders(WINDOW, seq_rows)
    loads[2].wait()

    span = STEP_ROWS + 2 * WINDOW
    seq_total = seq_rows * n
    lower = lax.broadcasted_iota(jnp.int32, (STEP_ROWS, 2 * HEAD_DIM), 1) < HEAD_DIM

    def attend_step(start):
        start = pl.multiple_of(start, STEP_ROWS)
        row = lax.broadcasted_iota(jnp.int32, (STEP_ROWS, span), 0)
        column = lax.broadcasted_iota(jnp.int32, (STEP_ROWS, span), 1)
        key_pos = e * seq_rows + start - WINDOW + column
        allowed = (
            (column >= row) & (column <= row + 2 * WINDOW)
            & (key_pos >= 0) & (key_pos < seq_total)
        )
        for kv_head in range(kv_heads):
            lanes = slice(kv_head * 2 * HEAD_DIM, (kv_head + 1) * 2 * HEAD_DIM)
            kv = kv_s[pl.ds(start, span), lanes]
            vk = vk_s[pl.ds(start, span), lanes]
            for pair in range(fan // 2):
                head = kv_head * fan + 2 * pair
                places = slice(head * HEAD_DIM, (head + 2) * HEAD_DIM)
                q_pair = q_v[pl.ds(start, STEP_ROWS), places] * jnp.bfloat16(HEAD_DIM ** -0.5)
                results = []
                for odd in range(2):
                    q_one = jnp.where(lower != bool(odd), q_pair, jnp.zeros_like(q_pair))
                    key_side, value_side = (vk, kv) if odd else (kv, vk)
                    scores = lax.dot_general(
                        q_one, key_side, (((1,), (1,)), ((), ())),
                        preferred_element_type=jnp.float32,
                    )
                    scores = jnp.where(allowed, scores, NEG_FILL)
                    bound = sink[t * heads + head + odd]
                    top = jnp.maximum(jnp.max(scores, 1, keepdims=True), bound)
                    expo = jnp.exp(scores - top)
                    denom = jnp.sum(expo, 1, keepdims=True) + jnp.exp(bound - top)
                    value = jnp.dot(
                        expo.astype(jnp.bfloat16), value_side, preferred_element_type=jnp.float32
                    )
                    results.append(value / denom)
                att[pl.ds(start, STEP_ROWS), places] = jnp.where(
                    lower, results[0], results[1]
                ).astype(jnp.bfloat16)

    def attend_inner(first, last):
        def step(i, carry):
            attend_step(i * STEP_ROWS)
            return carry

        lax.fori_loop(first, last, step, 0)

    def attend_edges():
        def step(i, carry):
            attend_step(i * (seq_rows - STEP_ROWS))
            return carry

        lax.fori_loop(0, 2, step, 0)
        for k in range(tp):
            owner = rem(t + k, tp)
            block = att.at[at(owner * own_count, own_count), :]
            if k:
                remote(block, att_in.at[t], att_send, att_recv, tp=owner).start()
            else:
                pltpu.make_async_copy(block, att_in.at[t], att_recv).start()

    def relay_tables(s):
        arrived(info_in.at[s], info_recv.at[s])
        table = info_in[s]
        sel[s] = pick(table)
        mixture(table, s)

    def relay_forward(s, c):
        arrived(block_in.at[s, c], block_recv.at[s, c])
        relay_out[s, c] = jnp.dot(
            sel[s], block_in[s, c], preferred_element_type=jnp.float32
        ).astype(jnp.bfloat16)
        landing = x_in.at[at(far_source(s, 0) * stride, stride), cols(c)]
        for j in range(1, half_count):
            remote(
                relay_out.at[s, c, at(near_ep(j) * stride, stride), :], landing,
                pack_send, pack_recv.at[s], ep=half * half_count + near_ep(j),
            ).start()
        pltpu.make_async_copy(
            relay_out.at[s, c, at(local * stride, stride), :], landing, pack_recv.at[s]
        ).start()

    def on_relay(task, *args):
        pl.when(is_relay)(lambda: task(*args))

    def off_relay(task, *args):
        pl.when(jnp.logical_not(is_relay))(lambda: task(*args))

    def forward_weights(i):
        arrived(w_place(i, side), w_sem(i, side))
        for copy in w_fwd[i]:
            copy.start()

    def hidden_rows(start, size, slot):
        x = x_in[at(start, size), :]
        gate = jnp.dot(x, gate_s[slot], preferred_element_type=jnp.float32)
        up = jnp.dot(x, up_s[slot], preferred_element_type=jnp.float32)
        hid[at(start, size), pl.ds(slot * shard, shard)] = (
            gate / (1.0 + jnp.exp(-gate)) * up
        ).astype(jnp.bfloat16)

    def got_weights(item, slot):
        arrived(w_place(item, slot), w_sem(item, slot))

    def project():
        arrived(att_in, att_recv)
        loads[3].wait()
        total = jnp.zeros(mo_v.shape, jnp.float32)
        for c in range(CHUNKS):
            total = sum(
                jnp.dot(
                    att_in[k], ow_v[k * q_width : (k + 1) * q_width, cols(c)],
                    preferred_element_type=jnp.float32,
                )
                for k in range(tp)
            )
            mo_v[:, cols(c)] = total.astype(jnp.bfloat16)

    def results(s, c, direct=False):
        first = far_plane(s) * group
        res[c, at(first, group), :] = jnp.dot(
            hid[at(first, group), :], down_s[c], preferred_element_type=jnp.float32
        ).astype(jnp.bfloat16)
        landing = relay_in.at[s, c, at(local * stride, stride), :]
        for k in range(members):
            block = res.at[c, at(far_source(s, k) * stride, stride), :]
            near_plane = own_relay_plane if direct else plane
            if k:
                remote(
                    block, landing, back_far_send, relay_recv.at[s, c],
                    ep=near_plane * members + rem(member + k, members),
                ).start()
            else:
                keep = pltpu.make_async_copy(block, landing, relay_recv.at[s, c])
            if not k and direct:
                hand = remote(
                    block, landing, direct_send, relay_recv.at[s, c],
                    ep=own_relay_plane * members + member,
                )
                pl.when(is_relay)(keep.start)
                pl.when(jnp.logical_not(is_relay))(hand.start)
            elif not k:
                keep.start()

    def edge_block(s, c):
        return relay_in.at[s, c, at(rem(plane, 2) * group, group), :]

    def edge_forward(s, c):
        arrived(edge_block(s, c), relay_recv.at[s, c])
        remote(
            edge_block(s, c), edge_block(s, c), edge_send, relay_recv.at[s, c],
            ep=own_relay_plane * members + member,
        ).start()

    def near_results(c):
        first = half * rows
        res[c, at(first, rows), :] = jnp.dot(
            hid[at(first, rows), :], down_s[c], preferred_element_type=jnp.float32
        ).astype(jnp.bfloat16)
        landing = near_in.at[c, at(local * stride, stride), :]
        for j in range(1, half_count):
            target = half * half_count + near_ep(j)
            remote(
                res.at[c, at(target * stride, stride), :], landing,
                back_near_send, back_near_recv.at[c], ep=target,
            ).start()
        pltpu.make_async_copy(
            res.at[c, own_rows, :], landing, back_near_recv.at[c]
        ).start()

    def mixed(where, values):
        return jnp.dot(
            mix_hi[where], values, preferred_element_type=jnp.float32
        ) + jnp.dot(mix_lo[where], values, preferred_element_type=jnp.float32)

    def relay_merge(s, c):
        arrived(relay_in.at[s, c], relay_recv.at[s, c])
        merged[s, c] = mixed(s, relay_in[s, c]).astype(jnp.bfloat16)
        remote(
            merged.at[s, c], far_in.at[c], merged_send, far_recv.at[c],
            ep=far_source(s, 0),
        ).start()

    def finish(c):
        arrived(near_in.at[c], back_near_recv.at[c])
        total = mixed(2, near_in[c])
        arrived(far_in.at[c], far_recv.at[c])
        out_v[:, cols(c)] = (total + far_in[c].astype(jnp.float32)).astype(jnp.bfloat16)

    on_relay(relay_tables, 0)
    steps = seq_rows // STEP_ROWS
    quarter = max(steps // 4, 1)
    bounds = [1] + [min(1 + quarter * (i + 1), steps - 1) for i in range(4)]
    plan = [range(0, 2), range(2, 4), range(4, 6), range(6, CHUNKS)]
    for i in range(4):
        attend_inner(bounds[i], bounds[i + 1])
        for c in plan[i]:
            on_relay(relay_forward, 0, c)
    forward_weights(0)
    on_relay(relay_tables, 1)
    on_relay(relay_forward, 1, 0)
    got_halo()
    attend_edges()
    for c in range(1, 4):
        on_relay(relay_forward, 1, c)
    for slot in range(side):
        arrived(gate_s.at[pl.ds(0, 2)], w_near_recv.at[slot, 0])
    first_rows, last_rows = far_plane(0) * group, far_plane(1) * group
    arrived(x_in.at[at(first_rows, group), :], pack_recv.at[0])
    for slot in range(side):
        hidden_rows(first_rows, group, slot)
    for c in range(4, 6):
        on_relay(relay_forward, 1, c)
    arrived(x_in.at[at(half * rows, rows), :], near_recv)
    for slot in range(side):
        hidden_rows(half * rows, rows, slot)
    on_relay(relay_forward, 1, 6)
    forward_weights(1)
    hidden_rows(first_rows, group, side)
    for c in range(7, CHUNKS):
        on_relay(relay_forward, 1, c)
    hidden_rows(half * rows, rows, side)
    for slot in range(side + 1, tp):
        for item in range(2):
            got_weights(item, slot)
        hidden_rows(first_rows, group, slot)

    def got_down(c):
        for slot in range(tp):
            if slot < side and c == 0:
                arrived(gate_s.at[0], w_near_recv.at[slot, 1])
            if slot > side:
                got_weights(2 + c, slot)

    directs = tuple((s, c) for c in range(3) for s in range(2))
    order = [(0, 0), (0, 1), (1, 0), (1, 1)] + [(s, c) for c in range(2, CHUNKS) for s in range(2)]
    merges, edges = list(order), [item for item in order if item not in directs]
    def last_arrived():
        arrived(x_in.at[at(last_rows, group), :], pack_recv.at[1])

    def last_hidden(*slots):
        for slot in slots:
            hidden_rows(last_rows, group, slot)

    def near_hidden():
        for slot in range(side + 1, tp):
            hidden_rows(half * rows, rows, slot)

    forward_weights(2)
    on_relay(last_arrived)
    on_relay(last_hidden, *range(side))
    got_down(0)
    results(0, 0, True)
    forward_weights(3)
    on_relay(last_hidden, *range(side, tp))
    off_relay(near_hidden)
    got_down(1)
    results(0, 1, True)
    off_relay(near_results, 0)
    off_relay(last_arrived)
    off_relay(last_hidden, *range(tp))
    results(1, 0, True)
    results(1, 1, True)
    on_relay(relay_merge, *merges.pop(0))
    on_relay(near_hidden)
    off_relay(near_results, 1)
    on_relay(relay_merge, *merges.pop(0))
    for c in range(2, CHUNKS):
        forward_weights(2 + c)
        got_down(c)
        results(0, c, (0, c) in directs)
        results(1, c, (1, c) in directs)
        for _ in range((0, 0, 1, 2, 2, 2)[min(c - 2, 5)]):
            off_relay(edge_forward, *edges.pop(0))
        for _ in range((1, 1, 2, 1, 2, 1)[min(c - 2, 5)]):
            on_relay(relay_merge, *merges.pop(0))
        on_relay(near_results, c - 2)
    for item in edges:
        off_relay(edge_forward, *item)
    for c in range(2, CHUNKS):
        off_relay(near_results, c)
    for c in range(CHUNKS - 2, CHUNKS):
        on_relay(near_results, c)
    while len(merges) > 4:
        on_relay(relay_merge, *merges.pop(0))
    project()
    for item in merges:
        on_relay(relay_merge, *item)
    for c in range(CHUNKS):
        finish(c)

    def sent(ref, sem):
        pltpu.make_async_copy(ref, ref, sem).wait()

    @pl.when(e < n - 1)
    def sent_after():
        halo_after.wait_send()

    @pl.when(e > 0)
    def sent_before():
        halo_before.wait_send()

    whole_shard = gate_s.at[pl.ds(0, 3)]
    sent(whole_shard, w_far_send)
    for k in range(1, side):
        sent(whole_shard, w_near_send.at[k])
        sent(whole_shard, w_fwd_send.at[k])
    send_info.wait_send()
    sent(norm_v, block_send)
    others = half_count - 1
    sent(near_out.at[pl.ds(0, others * stride), :], near_send)
    sent(att_in.at[pl.ds(0, tp - 1)], att_send)
    sent(near_in.at[:, pl.ds(0, others * stride), :], back_near_send)
    sent(relay_in.at[:, :, pl.ds(0, (members - 1) * stride), :], back_far_send)

    @pl.when(is_relay)
    def sent_relay():
        sent(relay_out.at[:, :, pl.ds(0, others * stride), :], pack_send)
        sent(merged, merged_send)

    @pl.when(jnp.logical_not(is_relay))
    def sent_edge():
        sent(relay_in.at[:, pl.ds(0, 3), pl.ds(0, stride), :], direct_send)
        sent(relay_in.at[:, pl.ds(0, CHUNKS - 3), pl.ds(0, group), :], edge_send)


def body(
    queries,
    keys_values,
    sink_logits,
    out_weight,
    expert_tokens,
    norm_gain,
    routes,
    route_weights,
    gate_weight,
    up_weight,
    down_weight,
):
    n, tp = lax.axis_size("ep"), lax.axis_size("tp")
    count, width = expert_tokens.shape
    cap = 3 * count * TOPK // (2 * n)
    stride = -(-cap // 16) * 16
    rows = n // 2 * stride
    wide = width // CHUNKS
    shard = gate_weight.shape[2]
    seq_rows, q_width = queries.shape
    kv_width = keys_values.shape[1]
    items = 2 + CHUNKS
    side = tp // 2
    bf16, f32 = jnp.bfloat16, jnp.float32
    dma = pltpu.SemaphoreType.DMA

    def vmem(*shape, dtype=bf16):
        return pltpu.VMEM(shape, dtype)

    scratch = [
        pltpu.SMEM(sink_logits.shape, f32),
        vmem(1, width, dtype=f32),
        vmem(TOPK, count, dtype=jnp.int32),
        vmem(TOPK, count, dtype=f32),
        vmem(count, width),
        vmem(CHUNKS, count, wide),
        vmem(8, count, dtype=f32),
        vmem(2, 8, count, dtype=f32),
        vmem(2, CHUNKS, count, wide),
        vmem(n * stride, width),
        vmem(rows, width),
        vmem(2, CHUNKS, rows, wide),
        vmem(3, rows, count),
        vmem(tp, width, shard),
        vmem(tp, width, shard),
        vmem(CHUNKS, tp * shard, wide),
        vmem(n * stride, tp * shard),
        vmem(CHUNKS, n * stride, wide),
        vmem(2, CHUNKS, rows, wide),
        vmem(2, CHUNKS, count, wide),
        vmem(CHUNKS, rows, wide),
        vmem(CHUNKS, count, wide),
        vmem(3, count, rows),
        vmem(3, count, rows),
        vmem(seq_rows, q_width),
        vmem(seq_rows + 2 * WINDOW, kv_width),
        vmem(seq_rows + 2 * WINDOW, kv_width),
        vmem(seq_rows, q_width),
        vmem(tp, seq_rows // tp, q_width),
        vmem(*out_weight.shape),
        dma((8,)),
        dma((side, 2)),
        dma((items, side)),
        dma((side,)),
        dma,
        dma((side,)),
        dma((2,)),
        dma((2,)),
        dma((2,)),
        dma,
        dma((2, CHUNKS)),
        dma,
        dma,
        dma,
        dma((2,)),
        dma,
        dma((CHUNKS,)),
        dma,
        dma,
        dma,
        dma,
        dma((2, CHUNKS)),
        dma,
        dma((CHUNKS,)),
        dma,
        dma,
    ]
    anywhere = pl.BlockSpec(memory_space=pl.ANY)
    small = pl.BlockSpec(memory_space=pltpu.VMEM)
    return pl.pallas_call(
        functools.partial(layer_kernel, n, tp, cap, stride),
        out_shape=(
            pltpu.VMEM((seq_rows // tp, width), bf16),
            pltpu.VMEM((count, width), bf16),
        ),
        in_specs=[anywhere] * 11,
        out_specs=(small, small),
        scratch_shapes=scratch,
        compiler_params=pltpu.CompilerParams(
            collective_id=0, has_side_effects=True, vmem_limit_bytes=62000000
        ),
        name="layer",
    )(
        sink_logits, queries, keys_values, out_weight, expert_tokens,
        norm_gain.reshape(1, width), routes.T, route_weights.T,
        gate_weight[0], up_weight[0], down_weight[0],
    )


def solution(mesh):
    return jax.shard_map(
        body,
        mesh=mesh,
        in_specs=(
            P("ep", "tp"),
            P("ep", "tp"),
            P(),
            P(),
            P(("ep", "tp"), None),
            P(),
            P(("ep", "tp"), None),
            P(("ep", "tp"), None),
            P("ep", None, "tp"),
            P("ep", None, "tp"),
            P("ep", "tp", None),
        ),
        out_specs=(P(("ep", "tp"), None), P(("ep", "tp"), None)),
        check_vma=False,
    )
```
